128 devices in a mesh: sp: 32 (over z, y, core), tp: 4 (over x).
Axes of the slice: x: 4, y: 4, z: 4, core: 2. Of those that a mesh axis runs over, the one named last changes fastest.
Arguments:
- tokens: bfloat16 [32768, 4096], P('sp', 'tp'), may hold values from -16 to 16
- norm_gain: float32 [4096], replicated, may hold values from 0.1 to 1.9
- w_pool_in: bfloat16 [4096, 2048], P('sp', 'tp'), may hold values from -0.09375 to 0.09375
- w_query: bfloat16 [4096, 2048], P('sp', 'tp'), may hold values from -0.09375 to 0.09375
- w_key: bfloat16 [4096, 256], P('sp', 'tp'), may hold values from -0.09375 to 0.09375
- w_value: bfloat16 [4096, 256], P('sp', 'tp'), may hold values from -0.09375 to 0.09375
- pool_map: bfloat16 [4, 512, 512], P('tp'), may hold values from -0.25 to 0.25
- pool_scale: float32 [2048], P('tp'), may hold values from 0.3 to 3
- q_gain: float32 [64], replicated, may hold values from 0.1 to 1.9
- k_gain: float32 [64], replicated, may hold values from 0.1 to 1.9
- sinks: float32 [32], P('tp'), may hold values from 0 to 4
- w_out: bfloat16 [4096, 4096], P('tp', 'sp'), may hold values from -0.09375 to 0.09375
Outputs:
- layer_out: bfloat16 [32768, 4096], P(('sp', 'tp'))
The draws below stay inside these ranges and needn't reach their ends.
All inputs are finite; a program needn't handle non-finite values.
Results may differ from the reference program's by a relative error of at most 0.012.
Values may be sent and summed in bfloat16 or wider, within the bound.
A program may use at most 128 MiB of HBM per device.

```python
import math
import jax
import jax.numpy as jnp
from jax import lax

D = 4096
HEAD_DIM = 64
GROUP = 8
GROUPS = 4
WINDOW = 128
GROUP_WIDTH = 512
Q_HEADS = 32
BRANCH_WIDTH = 2048
MIX = 4096
TOKENS = 32768
N_TP = 4


def draw_tokens(key, part):
    first_key, second_key = jax.random.split(jax.random.fold_in(key, 11), 2)
    base_rows = jnp.clip(jax.random.normal(first_key, (TOKENS, D), jnp.float32), -5.0, 5.0)
    row_scale = jnp.exp(jax.random.uniform(second_key, (TOKENS, 1), jnp.float32, math.log(0.3), math.log(3.0)))
    return (base_rows * row_scale).astype(jnp.bfloat16)


def shard_levels(key, extent, pieces, least, high):
    def one(dim, shards_of):
        steps = jax.random.uniform(jax.random.fold_in(jax.random.fold_in(key, 6), dim), (shards_of,), jnp.float32, least / len(pieces), high / len(pieces))
        return jnp.repeat(jnp.exp(steps), extent[dim] // shards_of).reshape((-1,) + (1,) * (len(extent) - dim - 1))

    level = one(*pieces[0])
    for cut in pieces[1:]:
        level = level * one(*cut)
    return level


def gaussian(own_key, dims, scale, bound, cuts=(), held_as=jnp.bfloat16):
    drawn = jax.random.normal(own_key, dims, jnp.float32) * scale
    if len(cuts) > 0:
        drawn = shard_levels(own_key, dims, cuts, -0.22, 0.18) * drawn
    return jnp.clip(drawn, min=-bound, max=bound).astype(held_as)


def setup_inputs(seed: int = 0) -> dict:
    splits = jax.random.split(jax.random.key(seed), 13)
    return {
        "tokens": draw_tokens(jax.random.fold_in(splits[12], 71), 0),
        "norm_gain": jnp.clip(1.0 + 0.18 * jax.random.normal(splits[1], (D,), jnp.float32), 0.1, 1.9),
        "w_pool_in": gaussian(splits[2], (D, BRANCH_WIDTH), D ** -0.5, 0.09375, ((0, 32), (1, 4))),
        "w_query": gaussian(splits[3], (D, BRANCH_WIDTH), D ** -0.5, 0.09375, ((0, 32), (1, 4))),
        "w_key": gaussian(splits[4], (D, GROUPS * HEAD_DIM), D ** -0.5, 0.09375, ((0, 32), (1, 4))),
        "w_value": gaussian(splits[5], (D, GROUPS * HEAD_DIM), D ** -0.5, 0.09375, ((0, 32), (1, 4))),
        "pool_map": gaussian(splits[6], (GROUPS, GROUP_WIDTH, GROUP_WIDTH), GROUP_WIDTH ** -0.5, 0.25, ((0, 4),)),
        "pool_scale": jnp.clip(jnp.exp(math.log(3.0) - 2.3025851 * jax.random.uniform(splits[7], (BRANCH_WIDTH,), jnp.float32) ** shard_levels(splits[7], (BRANCH_WIDTH,), ((0, 4),), -0.2, 0.2)), 0.3, 3.0),
        "q_gain": jnp.clip(1.0 + 0.18 * jax.random.normal(splits[8], (HEAD_DIM,), jnp.float32), 0.1, 1.9),
        "k_gain": jnp.clip(1.0 + 0.18 * jax.random.normal(splits[9], (HEAD_DIM,), jnp.float32), 0.1, 1.9),
        "sinks": jnp.clip(4.0 * jax.random.uniform(splits[10], (Q_HEADS,), jnp.float32) ** shard_levels(splits[10], (Q_HEADS,), ((0, 4),), -0.2, 0.2), 0.0, 4.0),
        "w_out": gaussian(splits[11], (MIX, D), MIX ** -0.5, 0.09375, ((0, 4), (1, 32))),
    }


epsilon = 1e-06

def rms_scale(values):
    return values * lax.rsqrt(lax.optimization_barrier(jnp.mean(values * values, axis=-1, keepdims=True)) + epsilon)

def reference(tokens, norm_gain, w_pool_in, w_query, w_key, w_value, pool_map, pool_scale, q_gain, k_gain, sinks, w_out):
    widened = tokens.astype(jnp.float32)
    normed = (rms_scale(widened) * norm_gain).astype(jnp.bfloat16)
    pool_in = jnp.dot(normed, w_pool_in, preferred_element_type=jnp.float32).astype(jnp.bfloat16)
    query_rows = jnp.dot(normed, w_query, preferred_element_type=jnp.float32).astype(jnp.bfloat16)
    key_rows = jnp.dot(normed, w_key, preferred_element_type=jnp.float32).astype(jnp.bfloat16)
    value_rows = jnp.dot(normed, w_value, preferred_element_type=jnp.float32).astype(jnp.bfloat16)
    query_float = lax.optimization_barrier(query_rows).astype(jnp.float32).reshape(TOKENS, Q_HEADS, HEAD_DIM)
    query_normed = (rms_scale(query_float) * q_gain).astype(jnp.bfloat16)
    key_float = lax.optimization_barrier(key_rows).astype(jnp.float32).reshape(TOKENS, GROUPS, HEAD_DIM)
    key_normed = (rms_scale(key_float) * k_gain).astype(jnp.bfloat16)
    value_heads = value_rows.reshape(TOKENS, GROUPS, HEAD_DIM)
    positions = jnp.arange(TOKENS, dtype=jnp.int32)
    pool_float = pool_in.astype(jnp.float32).reshape(TOKENS, GROUPS, GROUP_WIDTH)
    padded = jnp.pad(pool_float, ((15, 0), (0, 0), (0, 0)))
    blocks = TOKENS // WINDOW
    key_padded = jnp.concatenate([jnp.zeros((WINDOW, GROUPS, HEAD_DIM), jnp.bfloat16), key_normed], axis=0)
    value_padded = jnp.concatenate([jnp.zeros((WINDOW, GROUPS, HEAD_DIM), jnp.bfloat16), value_heads], axis=0)
    query_pos = jnp.arange(WINDOW, dtype=jnp.int32)[:, None] + WINDOW
    key_pos = jnp.arange(2 * WINDOW, dtype=jnp.int32)[None, :]
    distance = query_pos - key_pos
    in_band = (distance >= 0) & (distance < WINDOW)
    key_global = jnp.arange(blocks, dtype=jnp.int32)[:, None] * WINDOW - WINDOW + jnp.arange(2 * WINDOW, dtype=jnp.int32)[None, :]
    allowed = in_band[None] & (key_global >= 0)[:, None, :]
    branches = []
    for group_index in range(GROUPS):
        span_width = 2 ** (group_index + 1)
        running = jnp.zeros((TOKENS, GROUP_WIDTH), jnp.float32)
        for offset in range(span_width):
            running = running + padded[15 - offset:15 - offset + TOKENS, group_index]
        counts = jnp.minimum(positions.astype(jnp.float32) + 1.0, float(span_width))
        pool_diff = (running / counts[:, None] - pool_float[:, group_index]).astype(jnp.bfloat16)
        mapped = jnp.dot(pool_diff, pool_map[group_index], preferred_element_type=jnp.float32)
        mapped = mapped * pool_scale[group_index * GROUP_WIDTH:(group_index + 1) * GROUP_WIDTH]
        pool_branch = rms_scale(mapped)
        head_first = group_index * GROUP
        query_blocks = query_normed[:, head_first:head_first + GROUP].reshape(blocks, WINDOW, GROUP, HEAD_DIM).astype(jnp.float32)
        key_pairs = jnp.concatenate([key_padded[:TOKENS, group_index].reshape(blocks, WINDOW, HEAD_DIM), key_padded[WINDOW:, group_index].reshape(blocks, WINDOW, HEAD_DIM)], axis=1).astype(jnp.float32)
        value_pairs = jnp.concatenate([value_padded[:TOKENS, group_index].reshape(blocks, WINDOW, HEAD_DIM), value_padded[WINDOW:, group_index].reshape(blocks, WINDOW, HEAD_DIM)], axis=1).astype(jnp.float32)
        scores = jnp.einsum('nqgd,nkd->ngqk', query_blocks, key_pairs) * HEAD_DIM ** (-0.5)
        head_ids = head_first + jnp.arange(GROUP, dtype=jnp.int32) + 1
        slopes = jnp.exp2(-8.0 * head_ids.astype(jnp.float32) / Q_HEADS)
        logits = scores - slopes[None, :, None, None] * distance.astype(jnp.float32)[None, None]
        exp_scores = jnp.exp(jnp.where(allowed[:, None], logits, -jnp.inf))
        sink_logits = sinks[head_first:head_first + GROUP]
        denominator = lax.optimization_barrier(jnp.sum(exp_scores, axis=-1)) + jnp.exp(sink_logits)[None, :, None]
        weights_bf = (exp_scores / denominator[..., None]).astype(jnp.bfloat16)
        attended = jnp.einsum('ngqk,nkd->nqgd', weights_bf.astype(jnp.float32), value_pairs)
        attn_branch = rms_scale(attended.reshape(TOKENS, GROUP_WIDTH))
        branches.append(jnp.stack([pool_branch, attn_branch], axis=1))
    mixed_rows = jnp.stack(branches, axis=1).reshape(TOKENS, MIX).astype(jnp.bfloat16)
    block_width = MIX // N_TP
    summed = jnp.zeros((TOKENS, D), jnp.float32)
    for part_index in range(N_TP):
        row_start = part_index * block_width
        partial_term = jnp.dot(mixed_rows[:, row_start:row_start + block_width], w_out[row_start:row_start + block_width], preferred_element_type=jnp.float32).astype(jnp.bfloat16)
        summed = summed + lax.optimization_barrier(partial_term).astype(jnp.float32)
    return summed.astype(jnp.bfloat16)
```

```python
import jax
import jax.numpy as jnp
from jax import lax
from jax.experimental import pallas as pl
from jax.experimental.pallas import tpu as pltpu
from jax.sharding import PartitionSpec as P

MESH = pl.DeviceIdType.MESH
F32 = jnp.float32
BF16 = jnp.bfloat16
EPS = 1e-6
N_COPIES = 96


def mod4(v):
    return lax.rem(v, 4)


def kernel(
    tokens, wp, wq, wkv, wo, pmap, prm_in, gain,
    own_out, recv_out,
    W1, W2, TOK, ST1, ST2, ST3, PM, PRM, KV, PB, QB, ACC, SS, MIX, BIAS, BLK, SENDB, OWNB,
    lsem, ssem, rsem, osend, orecv, oloc, hsend, hrecv,
):
    sp = lax.axis_index("sp")
    x = lax.axis_index("tp")
    c = lax.rem(sp, 2)
    y = mod4(lax.div(sp, 2))
    z = lax.div(sp, 8)
    f = y + c * (z - y)
    s = z + c * (y - z)
    par = lax.rem(x, 2)
    flip1 = x + 1 - 2 * par
    flip3 = 3 - x
    p = (1 - c) * flip1 + c * flip3
    n = (1 - c) * flip3 + c * flip1
    x2 = mod4(x + 2)
    dx = mod4(x + 1 + 2 * c)

    def sp_of(c_, f_, s_):
        y_ = (1 - c_) * f_ + c_ * s_
        z_ = (1 - c_) * s_ + c_ * f_
        return (z_ * 4 + y_) * 2 + c_

    fu, fd = mod4(f + 1), mod4(f + 3)
    su, sd, s2 = mod4(s + 1), mod4(s + 3), mod4(s + 2)
    dev_fu, dev_fd = (sp_of(c, fu, s), x), (sp_of(c, fd, s), x)
    dev_su, dev_sd = (sp_of(c, f, su), x), (sp_of(c, f, sd), x)
    dev_sib = (sp + 1 - 2 * c, x)
    dev_dx, dev_p, dev_n, dev_x2 = (sp, dx), (sp, p), (sp, n), (sp, x2)
    cs, ss_, sf_ = 1 - c, f, s
    ssu, ssd, ss2 = mod4(ss_ + 1), mod4(ss_ + 3), mod4(ss_ + 2)

    pending = []

    def send(src, dst, dev):
        k = len(pending)
        d = pltpu.make_async_remote_copy(
            src_ref=src, dst_ref=dst, send_sem=ssem.at[k], recv_sem=rsem.at[k],
            device_id=dev, device_id_type=MESH,
        )
        d.start()
        pending.append(d)
        return d

    def recv(*ds):
        for d in ds:
            d.wait_recv()

    loc = []

    def local(src, dst):
        d = pltpu.make_async_copy(src, dst, lsem.at[len(loc)])
        d.start()
        loc.append(d)
        return d

    own1 = W1.at[0, c, s, f]
    l0 = local(wp, own1.at[:, pl.ds(0, 512)])
    l1 = local(wq, own1.at[:, pl.ds(512, 512)])
    l2 = local(wkv, own1.at[:, pl.ds(1024, 128)])
    l3 = local(wo, W2.at[c, s, f, 0])
    l4 = local(tokens.at[pl.ds(x * 256, 256)], TOK.at[0, x])
    l5 = local(tokens.at[pl.ds(p * 256, 256)], TOK.at[1, x])
    l6 = local(pmap, PM.at[0])
    l7 = local(prm_in, PRM.at[0])

    l0.wait()
    l1.wait()
    l2.wait()
    x_w1 = send(own1, ST1, dev_dx)
    a1 = [send(own1, own1, dev_fu), send(own1, own1, dev_fd)]
    tn = [
        send(tokens.at[pl.ds(n * 256, 256)], TOK.at[0, x], dev_n),
        send(tokens.at[pl.ds(x2 * 256, 256)], TOK.at[1, x], dev_n),
    ]
    tp_ = [
        send(tokens.at[pl.ds(p * 256, 256)], TOK.at[0, x], dev_p),
        send(tokens.at[pl.ds(x * 256, 256)], TOK.at[1, x], dev_p),
    ]
    prm_c = send(prm_in, PRM.at[1], dev_x2)
    l3.wait()
    x_w2 = send(W2.at[c, s, f, 0], ST2, dev_dx)
    l6.wait()
    half = pl.ds(c * 256, 256)
    x_pm = send(PM.at[0, half], ST3, dev_dx)

    lane_i = lax.broadcasted_iota(jnp.int32, (512, 512), 1)
    row_i = lax.broadcasted_iota(jnp.int32, (512, 512), 0)
    BLK[...] = jnp.where(
        lax.shift_right_logical(lane_i, 6) == lax.shift_right_logical(row_i, 6), 1.0, 0.0
    ).astype(BF16)
    SS[...] = jnp.zeros_like(SS)

    recv(x_w1)
    f_w1 = send(ST1, W1.at[1, c, s, f], dev_dx)

    def step_b1(g, a):
        recv(*a)
        return [
            send(W1.at[g, c, s, fd, pl.ds(0, 64)], W1.at[g, c, s, fd, pl.ds(0, 64)], dev_fu),
            send(W1.at[g, c, s, fu, pl.ds(64, 64)], W1.at[g, c, s, fu, pl.ds(64, 64)], dev_fd),
        ]

    def step_c1(g, b):
        recv(*b)
        plane = W1.at[g, c, s]
        return [send(plane, plane, dev_su), send(plane, plane, dev_sd)], [send(plane, plane, dev_sib)]

    def step_d1(g, cc, sib):
        recv(*cc)
        lo, hi = W1.at[g, c, sd], W1.at[g, c, su]
        d = [
            send(lo.at[pl.ds(0, 2)], lo.at[pl.ds(0, 2)], dev_su),
            send(hi.at[pl.ds(2, 2)], hi.at[pl.ds(2, 2)], dev_sd),
        ]
        sib += [send(lo, lo, dev_sib), send(hi, hi, dev_sib)]
        return d

    def step_e1(g, d, sib):
        recv(*d)
        far = W1.at[g, c, s2]
        sib.append(send(far, far, dev_sib))

    b1 = step_b1(0, a1)
    c1, sib1 = step_c1(0, b1)
    recv(f_w1)
    oth1 = W1.at[1, c, s, f]
    a1o = [send(oth1, oth1, dev_fu), send(oth1, oth1, dev_fd)]

    def scale_slab(j):
        g = gain[:, pl.ds(pl.multiple_of(j * 1024, 1024), 1024)]

        def body(k, carry):
            slot, r = lax.div(k, 4), pl.ds(lax.rem(k, 4) * 64, 64)
            t = TOK[slot, j, r, :].astype(F32)
            sq = t * t
            tot = sq[:, 0:128]
            for m in range(1, 8):
                tot += sq[:, m * 128 : (m + 1) * 128]
            SS[slot, r, :] += tot
            TOK[slot, j, r, :] = (t * g).astype(BF16)
            return carry

        lax.fori_loop(0, 8, body, 0)

    l4.wait()
    l5.wait()
    scale_slab(x)

    recv(*tn)
    tf = [
        send(TOK.at[0, n], TOK.at[1, n], dev_p),
        send(TOK.at[1, n], TOK.at[0, n], dev_p),
    ]
    b1o = step_b1(1, a1o)
    recv(x_w2)
    f_w2 = send(ST2, W2.at[c, s, f, 1], dev_dx)
    recv(x_pm)
    f_pm = send(ST3, PM.at[1, half], dev_dx)
    c1o, sib1o = step_c1(1, b1o)
    recv(f_w2)
    own2 = W2.at[c, s, f]
    a2 = [send(own2, own2, dev_fu), send(own2, own2, dev_fd)]

    recv(*tp_)
    scale_slab(p)

    l7.wait()
    recv(prm_c)
    key_i = jnp.bitwise_and(lane_i, 255)
    dist = 128 + jnp.bitwise_and(row_i, 127) - key_i
    band = (dist >= 0) & (dist < 128)
    head_in = 2 * lax.shift_right_logical(row_i, 7) + lax.shift_right_logical(lane_i, 8) + 1
    for gi, g in ((0, x), (1, x2)):
        slope = jnp.exp2(-0.25 * (g * 8 + head_in).astype(F32))
        BIAS[gi] = jnp.where(band, -slope * dist.astype(F32), -1e30)

    d1 = step_d1(0, c1, sib1)
    recv(*a2)
    b2 = [
        send(W2.at[c, s, fd, 0], W2.at[c, s, fd, 0], dev_fu),
        send(W2.at[c, s, fu, 1], W2.at[c, s, fu, 1], dev_fd),
    ]
    recv(f_pm)
    sib_pm = send(PM.at[1, half], PM.at[1, half], dev_sib)
    for d in tf:
        d.wait_send()
    scale_slab(n)
    recv(*b2)
    d1o = step_d1(1, c1o, sib1o)

    def half_plane(s_, k):
        return W2.at[c, s_, pl.ds(2 * k, 2)]

    def c2_send(k_up, k_dn):
        u, d = half_plane(s, k_up), half_plane(s, k_dn)
        return [send(u, u, dev_su), send(d, d, dev_sd)]

    c2a = c2_send(0, 1)
    c2b = c2_send(1, 0)
    plane2 = W2.at[c, s]
    sib2_own = [send(plane2, plane2, dev_sib)]

    def matmul(gi, jz):
        parts = []
        for yy in range(4):
            parts.append(W1[gi, 0, jz, yy])
            parts.append(W1[gi, 1, yy, jz])
        rhs = jnp.concatenate(parts, axis=0)
        lhs = TOK[:, jz].reshape(512, 1024)
        ACC[...] += jnp.dot(lhs, rhs, preferred_element_type=F32)

    def matmuls(gi, order):
        ACC[...] = jnp.zeros_like(ACC)

        def body(t, carry):
            matmul(gi, order(t))
            return carry

        return body

    def post(gi):
        def body(k, carry):
            slot, r = lax.div(k, 2), lax.rem(k, 2)
            rows = pl.ds(pl.multiple_of(k * 128, 128), 128)
            tot = jnp.sum(SS[slot, pl.ds(r * 128, 128), :], axis=-1, keepdims=True)
            a = ACC[rows, :] * lax.rsqrt(tot * (1.0 / 4096) + EPS)
            PB[gi, slot, pl.ds(pl.multiple_of(16 + r * 128, 16), 128), :] = a[:, 0:512].astype(BF16)
            qf = a[:, 512:1024].astype(BF16).astype(F32)
            sq = qf * qf
            hi = sq.astype(BF16)
            lo = (sq - hi.astype(F32)).astype(BF16)
            ssq = jnp.dot(hi, BLK[...], preferred_element_type=F32) + jnp.dot(
                lo, BLK[...], preferred_element_type=F32
            )
            qg = jnp.concatenate([PRM[0, 8 + j : 9 + j, :] for j in range(4)], axis=1)
            QB[gi, rows, :] = (qf * lax.rsqrt(ssq * (1.0 / 64) + EPS) * qg).astype(BF16)
            kv = a[:, 1024:1152].astype(BF16).astype(F32)
            is_key = lax.broadcasted_iota(jnp.int32, (128, 128), 1) < 64
            ksq = jnp.sum(jnp.where(is_key, kv * kv, 0.0), axis=-1, keepdims=True)
            kn = kv * lax.rsqrt(ksq * (1.0 / 64) + EPS) * PRM[0, 12:13, :]
            KV[gi, slot, pl.ds(pl.multiple_of(128 + r * 128, 128), 128), :] = jnp.where(
                is_key, kn, kv
            ).astype(BF16)
            return carry

        lax.fori_loop(0, 4, body, 0)

    def holder(q, c_):
        inner = lax.rem(lax.div(q + 1, 2), 2)
        even = lax.div(q, 2) * 2 + par
        odd = inner * (2 - par) + (1 - inner) * 3 * par
        return (1 - c_) * even + c_ * odd

    quarters = (x, p)

    def halo_next(gi, i):
        q = quarters[i]
        qn = mod4(q + 1)
        spn = sp + lax.div(q + 1, 4)
        xn = holder(qn, lax.rem(spn, 2))
        slot = jnp.where(xn == qn, 0, 1)
        gn = jnp.where(xn == x, gi, 1 - gi)
        here = (spn == sp) & (xn == x)
        away = jnp.logical_not(here) & (spn < 32)
        spn_ok = jnp.where(spn < 32, spn, 0)
        copies = [
            pltpu.make_async_remote_copy(
                src_ref=src, dst_ref=dst, send_sem=hsend.at[gi, i, k], recv_sem=hrecv.at[gn, slot, k],
                device_id=(spn_ok, xn), device_id_type=MESH,
            )
            for k, (src, dst) in enumerate(
                (
                    (KV.at[gi, i, pl.ds(256, 128)], KV.at[gn, slot, pl.ds(0, 128)]),
                    (PB.at[gi, i, pl.ds(256, 16)], PB.at[gn, slot, pl.ds(0, 16)]),
                )
            )
        ]
        return here, away, copies

    def halo_send(gi):
        for i in range(2):
            here, away, copies = halo_next(gi, i)

            @pl.when(away)
            def _():
                for d in copies:
                    d.start()

            @pl.when(here)
            def _():
                KV[gi, 1 - i, pl.ds(0, 128), :] = KV[gi, i, pl.ds(256, 128), :]
                PB[gi, 1 - i, pl.ds(0, 16), :] = PB[gi, i, pl.ds(256, 16), :]

    def halo_sent(gi):
        for i in range(2):
            _, away, copies = halo_next(gi, i)

            @pl.when(away)
            def _():
                for d in copies:
                    d.wait_send()

    def halo_wait(gi):
        for i in range(2):
            q = quarters[i]
            first = (sp == 0) & (q == 0)
            qp = mod4(q + 3)
            back = jnp.where(q == 0, 1, 0)
            spp = sp - back
            xp = holder(qp, lax.rem(spp + 2, 2))
            here = (back == 0) & (xp == x)

            @pl.when(first)
            def _():
                KV[gi, i, pl.ds(0, 128), :] = jnp.zeros((128, 128), BF16)
                PB[gi, i, pl.ds(0, 16), :] = jnp.zeros((16, 512), BF16)

            @pl.when(jnp.logical_not(first) & jnp.logical_not(here))
            def _():
                for k, dst in enumerate((KV.at[gi, i, pl.ds(0, 128)], PB.at[gi, i, pl.ds(0, 16)])):
                    pltpu.make_async_copy(dst, dst, hrecv.at[gi, i, k]).wait()

    def pool(gi, g):
        span = lax.shift_left(jnp.int32(2), g)
        for i in range(2):
            pf = PB[gi, i].astype(F32)
            t2 = pf + pltpu.roll(pf, 1, 0)
            t4 = t2 + pltpu.roll(t2, 2, 0)
            t8 = t4 + pltpu.roll(t4, 4, 0)
            t16 = t8 + pltpu.roll(t8, 8, 0)
            run = jnp.where(g == 0, t2, jnp.where(g == 1, t4, jnp.where(g == 2, t8, t16)))[16:]
            pos = sp * 1024 + quarters[i] * 256 + lax.broadcasted_iota(jnp.int32, (256, 1), 0)
            count = jnp.minimum(pos + 1, span).astype(F32)
            diff = (run * (1.0 / count) - pf[16:]).astype(BF16)
            m = jnp.dot(diff, PM[gi], preferred_element_type=F32)
            m = m * jnp.concatenate([PRM[gi, j : j + 1, :] for j in range(4)], axis=1)
            m = m * lax.rsqrt(jnp.mean(m * m, axis=-1, keepdims=True) + EPS)
            MIX[gi, i * 256 : (i + 1) * 256, 0:512] = m.astype(BF16)

    def attend(gi):
        es = jnp.exp(PRM[gi, 4:8, :])
        es = jnp.concatenate(
            [jnp.broadcast_to(es[j : j + 1], (128, 128)) for j in range(4)], axis=0
        )

        def body(k, carry):
            slot, r = lax.div(k, 2), lax.rem(k, 2)
            rows = pl.ds(pl.multiple_of(k * 128, 128), 128)
            kv = KV[gi, slot, pl.ds(pl.multiple_of(r * 128, 128), 256), :].astype(F32)
            low = lax.broadcasted_iota(jnp.int32, (256, 128), 1) < 64
            ke = jnp.where(low, kv, 0.0)
            vo = jnp.where(low, 0.0, kv)
            ko = pltpu.roll(ke, 64, 1)
            ve = pltpu.roll(vo, 64, 1)
            q_here = (1 - slot) * x + slot * p
            missing = jnp.where((sp == 0) & (q_here == 0) & (r == 0), 128, 0)
            there = lax.broadcasted_iota(jnp.int32, (256, 128), 0) >= missing
            oe = jnp.where(low & there, 1.0, 0.0)
            oo = jnp.where(jnp.logical_not(low) & there, 1.0, 0.0)
            keys = jnp.concatenate([ke, ko], axis=0).astype(BF16)
            values = jnp.concatenate(
                [jnp.concatenate([ve, oe], axis=1), jnp.concatenate([vo, oo], axis=1)], axis=0
            ).astype(BF16)
            q = QB[gi, rows, :]
            q = jnp.concatenate([q[:, j * 128 : (j + 1) * 128] for j in range(4)], axis=0)
            sc = lax.dot_general(q, keys, (((1,), (1,)), ((), ())), preferred_element_type=F32)
            e = jnp.exp(sc + BIAS[gi]).astype(BF16)
            o = jnp.dot(e, values, preferred_element_type=F32)
            att = o[:, 0:128] / (o[:, 128:256] + es)
            parts = [att[j * 128 : (j + 1) * 128] for j in range(4)]
            sq = parts[0] * parts[0]
            for j in range(1, 4):
                sq += parts[j] * parts[j]
            r_ = lax.rsqrt(jnp.sum(sq, axis=-1, keepdims=True) * (1.0 / 512) + EPS)
            for j in range(4):
                MIX[gi, rows, 512 + j * 128 : 640 + j * 128] = (parts[j] * r_).astype(BF16)
            return carry

        lax.fori_loop(0, 4, body, 0)

    step_e1(0, d1, sib1)
    recv(*sib1)
    order = lambda t: jnp.where(t == 0, x, jnp.where(t == 1, p, jnp.where(t == 2, n, x2)))
    body0 = matmuls(0, order)
    lax.fori_loop(0, 3, body0, 0)
    recv(*tf)
    scale_slab(x2)
    lax.fori_loop(3, 4, body0, 0)
    post(0)
    halo_send(0)
    step_e1(1, d1o, sib1o)
    recv(*sib1o)
    body1 = matmuls(1, order)
    lax.fori_loop(0, 4, body1, 0)
    post(1)
    halo_send(1)

    recv(sib_pm)
    halo_wait(0)
    attend(0)
    pool(0, x)
    halo_wait(1)
    attend(1)
    pool(1, x2)

    def unit(u, cc, s_, k):
        rhs = []
        for g in range(2):
            rhs.append(
                jnp.concatenate([W2[cc, s_, 2 * k, g], W2[cc, s_, 2 * k + 1, g]], axis=1)
            )
        o = jnp.dot(MIX[0], rhs[0], preferred_element_type=F32)
        o += jnp.dot(MIX[1], rhs[1], preferred_element_type=F32)
        ob = o.astype(BF16)
        for e in range(2):
            idx = 2 * u + e
            f_ = 2 * k + e
            col = pl.ds(pl.multiple_of(sp_of(cc, f_, s_) * 128, 128), 128)
            OWNB[idx] = ob[0:256, e * 128 : (e + 1) * 128]
            SENDB[idx] = ob[256:512, e * 128 : (e + 1) * 128]
            out_copy(idx, col).start()
            pltpu.make_async_copy(OWNB.at[idx], own_out.at[:, col], oloc.at[idx]).start()

    def out_copy(idx, col):
        return pltpu.make_async_remote_copy(
            src_ref=SENDB.at[idx], dst_ref=recv_out.at[:, col], send_sem=osend.at[idx],
            recv_sem=orecv.at[idx], device_id=dev_p, device_id_type=MESH,
        )

    def pair(stage, mine, sA, kA, sB, kB):
        cc = c if mine else cs

        def body(t, carry):
            unit(stage * 4 + (0 if mine else 2) + t, cc, sA + t * (sB - sA), kA + t * (kB - kA))
            return carry

        lax.fori_loop(0, 2, body, 0)

    pair(0, True, s, 0, s, 1)
    recv(*sib2_own)
    pair(0, False, ss_, 0, ss_, 1)

    recv(*c2a)
    u0, d0 = half_plane(sd, 0), half_plane(su, 1)
    d2 = [send(u0, u0, dev_su), send(d0, d0, dev_sd)]
    sib2_a = [send(u0, u0, dev_sib), send(d0, d0, dev_sib)]
    pair(1, True, sd, 0, su, 1)
    recv(*sib2_a)
    pair(1, False, ssd, 0, ssu, 1)

    recv(*c2b)
    u1, d1_ = half_plane(sd, 1), half_plane(su, 0)
    sib2_b = [send(u1, u1, dev_sib), send(d1_, d1_, dev_sib)]
    pair(2, True, sd, 1, su, 0)
    recv(*sib2_b)
    pair(2, False, ssd, 1, ssu, 0)

    recv(*d2)
    u2, d2_ = half_plane(s2, 0), half_plane(s2, 1)
    sib2_c = [send(u2, u2, dev_sib), send(d2_, d2_, dev_sib)]
    pair(3, True, s2, 0, s2, 1)
    recv(*sib2_c)
    pair(3, False, ss2, 0, ss2, 1)

    tf_ids = {id(d) for d in tf}
    for d in pending:
        if id(d) not in tf_ids:
            d.wait_send()
    halo_sent(0)
    halo_sent(1)

    def drain(idx, carry):
        col = pl.ds(pl.multiple_of(idx * 128, 128), 128)
        d = out_copy(idx, col)
        d.wait_send()
        d.wait_recv()
        pltpu.make_async_copy(OWNB.at[idx], own_out.at[:, col], oloc.at[idx]).wait()
        return carry

    lax.fori_loop(0, 32, drain, 0)


def local_program(
    tokens, norm_gain, w_pool_in, w_query, w_key, w_value, pool_map, pool_scale,
    q_gain, k_gain, sinks, w_out,
):
    wkv = jnp.concatenate([w_key, w_value], axis=1)
    prm = jnp.concatenate(
        [
            pool_scale,
            jnp.repeat(sinks, 64),
            jnp.tile(q_gain * 0.125, 8),
            k_gain,
            jnp.ones((64,), F32),
            jnp.zeros((3 * 128,), F32),
        ]
    ).reshape(16, 128)
    any_ = pl.BlockSpec(memory_space=pl.ANY)
    vmem = pl.BlockSpec(memory_space=pltpu.VMEM)
    dma = pltpu.SemaphoreType.DMA
    own, got = pl.pallas_call(
        kernel,
        out_shape=[jax.ShapeDtypeStruct((256, 4096), BF16)] * 2,
        in_specs=[any_] * 7 + [vmem],
        out_specs=[any_, any_],
        scratch_shapes=[
            pltpu.VMEM((2, 2, 4, 4, 128, 1152), BF16),
            pltpu.VMEM((2, 4, 4, 2, 1024, 128), BF16),
            pltpu.VMEM((2, 4, 256, 1024), BF16),
            pltpu.VMEM((128, 1152), BF16),
            pltpu.VMEM((1024, 128), BF16),
            pltpu.VMEM((256, 512), BF16),
            pltpu.VMEM((2, 512, 512), BF16),
            pltpu.VMEM((2, 16, 128), F32),
            pltpu.VMEM((2, 2, 384, 128), BF16),
            pltpu.VMEM((2, 2, 272, 512), BF16),
            pltpu.VMEM((2, 512, 512), BF16),
            pltpu.VMEM((512, 1152), F32),
            pltpu.VMEM((2, 256, 128), F32),
            pltpu.VMEM((2, 512, 1024), BF16),
            pltpu.VMEM((2, 512, 512), F32),
            pltpu.VMEM((512, 512), BF16),
            pltpu.VMEM((32, 256, 128), BF16),
            pltpu.VMEM((32, 256, 128), BF16),
            dma((8,)),
            dma((N_COPIES,)),
            dma((N_COPIES,)),
            dma((32,)),
            dma((32,)),
            dma((32,)),
            dma((2, 2, 2)),
            dma((2, 2, 2)),
        ],
        compiler_params=pltpu.CompilerParams(
            has_side_effects=True, vmem_limit_bytes=66_000_000
        ),
        name="mixer",
    )(tokens, w_pool_in, w_query, wkv, w_out, pool_map.reshape(512, 512), prm, norm_gain.reshape(1, 4096))
    return (own.astype(F32) + got.astype(F32)).astype(BF16)


def solution(mesh):
    in_specs = (
        P("sp", "tp"), P(), P("sp", "tp"), P("sp", "tp"), P("sp", "tp"), P("sp", "tp"),
        P("tp", None, None), P("tp"), P(), P(), P("tp"), P("tp", "sp"),
    )
    out_specs = P(("sp", "tp"), None)
    return jax.shard_map(local_program, mesh=mesh, in_specs=in_specs, out_specs=out_specs, check_vma=False)
```

```python
import jax
import jax.numpy as jnp
from jax import lax
from jax.experimental import pallas as pl
from jax.experimental.pallas import tpu as pltpu
from jax.sharding import PartitionSpec as P

MESH = pl.DeviceIdType.MESH
F32 = jnp.float32
BF16 = jnp.bfloat16
EPS = 1e-6
N_COPIES = 128


def mod4(v):
    return lax.rem(v, 4)


def kernel(
    tokens, wp, wq, wk_t, wv_t, wo, pmap, scale_in, sinks_in, q_gain, k_gain, gain,
    out,
    W1, W2, TOK, ST1, ST2, ST3, PM, SCALE, SINK, KVT, KV, PB, QB, ACC, SS, MIX, BIAS, BLK, SENDB, OWNB, RECVB, RLK, RLP,
    lsem, ssem, rsem, osend, orecv, oloc, hsend, hrecv, rlsend, rlrecv,
):
    sp = lax.axis_index("sp")
    x = lax.axis_index("tp")
    c = lax.rem(sp, 2)
    y = mod4(lax.div(sp, 2))
    z = lax.div(sp, 8)
    f = y + c * (z - y)
    s = z + c * (y - z)
    par = lax.rem(x, 2)
    flip1 = x + 1 - 2 * par
    flip3 = 3 - x
    p = (1 - c) * flip1 + c * flip3
    n = (1 - c) * flip3 + c * flip1
    x2 = mod4(x + 2)
    dx = mod4(x + 1 + 2 * c)

    def sp_of(c_, f_, s_):
        y_ = (1 - c_) * f_ + c_ * s_
        z_ = (1 - c_) * s_ + c_ * f_
        return (z_ * 4 + y_) * 2 + c_

    fu, fd = mod4(f + 1), mod4(f + 3)
    su, sd, s2 = mod4(s + 1), mod4(s + 3), mod4(s + 2)
    dev_fu, dev_fd = (sp_of(c, fu, s), x), (sp_of(c, fd, s), x)
    dev_su, dev_sd = (sp_of(c, f, su), x), (sp_of(c, f, sd), x)
    dev_sib = (sp + 1 - 2 * c, x)
    dev_dx, dev_p, dev_n, dev_x2 = (sp, dx), (sp, p), (sp, n), (sp, x2)
    cs, ss_, sf_ = 1 - c, f, s
    ssu, ssd, ss2 = mod4(ss_ + 1), mod4(ss_ + 3), mod4(ss_ + 2)

    pending = []

    def send(src, dst, dev):
        k = len(pending)
        d = pltpu.make_async_remote_copy(
            src_ref=src, dst_ref=dst, send_sem=ssem.at[k], recv_sem=rsem.at[k],
            device_id=dev, device_id_type=MESH,
        )
        d.start()
        pending.append(d)
        return d

    def recv(*ds):
        for d in ds:
            d.wait_recv()

    loc = []

    def local(src, dst):
        d = pltpu.make_async_copy(src, dst, lsem.at[len(loc)])
        d.start()
        loc.append(d)
        return d

    own1 = W1.at[0, c, s, f]
    l0 = local(wp, own1.at[:, pl.ds(0, 512)])
    l1 = local(wq, own1.at[:, pl.ds(512, 512)])
    l2 = local(wk_t, KVT.at[pl.ds(0, 64)])
    l7 = local(wv_t, KVT.at[pl.ds(64, 64)])
    l3 = local(wo, W2.at[c, s, f, 0])
    l4 = local(tokens.at[pl.ds(x * 256, 256)], TOK.at[0, x])
    l5 = local(tokens.at[pl.ds(p * 256, 256)], TOK.at[1, x])
    l6 = local(pmap, PM.at[0])

    def holder(q, c_):
        inner = lax.rem(lax.div(q + 1, 2), 2)
        even = lax.div(q, 2) * 2 + par
        odd = inner * (2 - par) + (1 - inner) * 3 * par
        return (1 - c_) * even + c_ * odd

    quarters = (x, p)

    def halo_to(i):
        q = quarters[i]
        qn = mod4(q + 1)
        spn = sp + lax.div(q + 1, 4)
        xn = holder(qn, lax.rem(spn, 2))
        here = (spn == sp) & (xn == x)
        away = jnp.logical_not(here) & (spn < 32)
        passed = away & (c == 1) & (q == 3)
        return qn, jnp.where(spn < 32, spn, 0), xn, here, away & jnp.logical_not(passed), passed

    def halo_from(i):
        q = quarters[i]
        first = (sp == 0) & (q == 0)
        back = jnp.where(q == 0, 1, 0)
        relayed = (back == 1) & (c == 0)
        spp = jnp.where(first, sp, sp - back - jnp.where(relayed, 1, 0))
        xp = holder(mod4(q + 3), lax.rem(sp - back + 2, 2))
        here = (back == 0) & (xp == x)
        return first, jnp.logical_not(first) & jnp.logical_not(here), spp, xp

    relay = (c == 0) & ((x == 0) | (x == 3)) & (sp < 30)
    relay_dev = (jnp.where(relay, sp + 2, 0), par)
    relay_slot = jnp.where(par == 0, 0, 1)

    barrier = pltpu.get_barrier_semaphore()

    def greet(dev):
        pl.semaphore_signal(barrier, inc=1, device_id=dev, device_id_type=MESH)

    for dev in (dev_fu, dev_fd, dev_su, dev_sd, dev_sib, dev_p, dev_n, dev_x2):
        greet(dev)
    @pl.when(relay)
    def _():
        greet(relay_dev)

    for i in range(2):
        _, spn, xn, _, away, _ = halo_to(i)

        @pl.when(away)
        def _():
            greet((spn, xn))

        _, apart, spp, xp = halo_from(i)

        @pl.when(apart)
        def _():
            greet((spp, xp))

    lane_i = lax.broadcasted_iota(jnp.int32, (512, 512), 1)
    row_i = lax.broadcasted_iota(jnp.int32, (512, 512), 0)
    l2.wait()
    l7.wait()
    W1[0, c, s, f, :, pl.ds(1024, 128)] = KVT[...].astype(F32).T.astype(BF16)
    BLK[...] = jnp.where(
        lax.shift_right_logical(lane_i, 6) == lax.shift_right_logical(row_i, 6), 1.0, 0.0
    ).astype(BF16)
    SS[...] = jnp.zeros_like(SS)
    key_i = jnp.bitwise_and(lane_i, 255)
    dist = 128 + jnp.bitwise_and(row_i, 127) - key_i
    band = (dist >= 0) & (dist < 128)
    head_in = 2 * lax.shift_right_logical(row_i, 7) + lax.shift_right_logical(lane_i, 8) + 1
    for gi, g in ((0, x), (1, x2)):
        slope = jnp.exp2(-0.25 * (g * 8 + head_in).astype(F32))
        BIAS[gi] = jnp.where(band, -slope * dist.astype(F32), -1e30)

    peers = 8 + jnp.where(relay, 1, 0)
    for i in range(2):
        peers += jnp.where(halo_to(i)[4], 1, 0) + jnp.where(halo_from(i)[1], 1, 0)
    pl.semaphore_wait(barrier, peers)

    l0.wait()
    l1.wait()
    l3.wait()
    def halves(src, dst, dev, first):
        return [
            send(src.at[pl.ds(r, 64)], dst.at[pl.ds(r, 64)], dev) for r in (first, 64 - first)
        ]

    def step_a1(g):
        piece = W1.at[g, c, s, f]
        up, down = halves(piece, piece, dev_fu, 0), halves(piece, piece, dev_fd, 64)
        return [up[0], down[0]], [up[1], down[1]]

    def step_b1(g, a):
        recv(*a[0])
        lo, hi = W1.at[g, c, s, fd, pl.ds(0, 64)], W1.at[g, c, s, fu, pl.ds(64, 64)]
        return [send(lo, lo, dev_fu), send(hi, hi, dev_fd)]

    def step_c1(g, a, b):
        recv(*a[1], *b)
        plane = W1.at[g, c, s]
        lo, hi = plane.at[pl.ds(0, 2)], plane.at[pl.ds(2, 2)]
        first = [send(lo, lo, dev_su), send(hi, hi, dev_sd)]
        second = [send(hi, hi, dev_su), send(lo, lo, dev_sd)]
        return first, second, [send(plane, plane, dev_sib)]

    def step_d1(g, cc):
        recv(*cc[0])
        lo, hi = W1.at[g, c, sd, pl.ds(0, 2)], W1.at[g, c, su, pl.ds(2, 2)]
        return [send(lo, lo, dev_su), send(hi, hi, dev_sd)]

    def share1(g, s_):
        piece = W1.at[g, c, s_]
        return send(piece, piece, dev_sib)

    def step_a2(g):
        piece = W2.at[c, s, f, g]
        return [send(piece, piece, dev_fu), send(piece, piece, dev_fd)]

    def step_b2(g, a):
        recv(*a)
        lo, hi = W2.at[c, s, fd, g, pl.ds(0, 512)], W2.at[c, s, fu, g, pl.ds(512, 512)]
        return [send(lo, lo, dev_fu), send(hi, hi, dev_fd)]

    x_w1 = halves(own1, ST1, dev_dx, 0)
    a1 = step_a1(0)
    a2 = step_a2(0)
    x_w2 = send(W2.at[c, s, f, 0], ST2, dev_dx)

    f_w1 = []
    b1 = None
    for k in range(2):
        recv(x_w1[k])
        part = pl.ds(64 * k, 64)
        f_w1.append(send(ST1.at[part], W1.at[1, c, s, f, part], dev_dx))
        if k == 0:
            b1 = step_b1(0, a1)
    c1a, c1b, sib1 = step_c1(0, a1, b1)
    recv(x_w2)
    f_w2 = send(ST2, W2.at[c, s, f, 1], dev_dx)
    tn = [
        send(tokens.at[pl.ds(n * 256, 256)], TOK.at[0, x], dev_n),
        send(tokens.at[pl.ds(x2 * 256, 256)], TOK.at[1, x], dev_n),
    ]
    sc_c = [send(scale_in, SCALE, dev_x2), send(sinks_in, SINK, dev_x2)]

    recv(*f_w1)
    a1o = step_a1(1)

    def scale_slab(j):
        g = gain[:, pl.ds(pl.multiple_of(j * 1024, 1024), 1024)]

        def body(k, carry):
            slot, r = lax.div(k, 4), pl.ds(lax.rem(k, 4) * 64, 64)
            t = TOK[slot, j, r, :].astype(F32)
            sq = t * t
            tot = sq[:, 0:128]
            for m in range(1, 8):
                tot += sq[:, m * 128 : (m + 1) * 128]
            SS[slot, r, :] += tot
            TOK[slot, j, r, :] = (t * g).astype(BF16)
            return carry

        lax.fori_loop(0, 8, body, 0)

    l4.wait()
    l5.wait()
    scale_slab(x)
    b1o = step_b1(1, a1o)
    recv(f_w2)
    a2o = step_a2(1)
    b2 = step_b2(0, a2)
    d1 = step_d1(0, (c1a, c1b))
    c1oa, c1ob, sib1o = step_c1(1, a1o, b1o)
    tp_ = [
        send(tokens.at[pl.ds(p * 256, 256)], TOK.at[0, x], dev_p),
        send(tokens.at[pl.ds(x * 256, 256)], TOK.at[1, x], dev_p),
    ]
    recv(*c1b)
    sib1 += [share1(0, sd), share1(0, su)]
    recv(*tn)
    tf = [
        send(TOK.at[0, n], TOK.at[1, n], dev_p),
        send(TOK.at[1, n], TOK.at[0, n], dev_p),
    ]
    l6.wait()
    half = pl.ds(c * 256, 256)
    x_pm = send(PM.at[0, half], ST3, dev_dx)
    b2o = step_b2(1, a2o)

    def half_plane(s_, k):
        return W2.at[c, s_, pl.ds(2 * k, 2)]

    def c2_send(k_up, k_dn):
        u, d = half_plane(s, k_up), half_plane(s, k_dn)
        return [send(u, u, dev_su), send(d, d, dev_sd)]

    def matmul(gi, jz):
        parts = []
        for yy in range(4):
            parts.append(W1[gi, 0, jz, yy])
            parts.append(W1[gi, 1, yy, jz])
        rhs = jnp.concatenate(parts, axis=0)
        lhs = TOK[:, jz].reshape(512, 1024)
        ACC[...] += jnp.dot(lhs, rhs, preferred_element_type=F32)

    def matmul_slab(gi, jz):
        lax.fori_loop(0, 1, lambda t, carry: (matmul(gi, jz), carry)[1], 0)

    def matmul_planes(gi, cc, sA, sB, count):
        def body(t, carry):
            s_ = sA + t * (sB - sA)
            rhs = jnp.concatenate([W1[gi, cc, s_, k] for k in range(4)], axis=0)
            lhs = []
            for k in range(4):
                off = ((1 - cc) * k + cc * s_) * 256 + cc * 128
                col = pl.ds(pl.multiple_of(off, 128), 128)
                lhs.append(TOK[:, (1 - cc) * s_ + cc * k, :, col].reshape(512, 128))
            lhs = jnp.concatenate(lhs, axis=1)
            ACC[...] += jnp.dot(lhs, rhs, preferred_element_type=F32)
            return carry

        lax.fori_loop(0, count, body, 0)

    def post(gi):
        def body(k, carry):
            slot, r = lax.div(k, 2), lax.rem(k, 2)
            rows = pl.ds(pl.multiple_of(k * 128, 128), 128)
            tot = jnp.sum(SS[slot, pl.ds(r * 128, 128), :], axis=-1, keepdims=True)
            a = ACC[rows, :] * lax.rsqrt(tot * (1.0 / 4096) + EPS)
            PB[gi, slot, pl.ds(pl.multiple_of(16 + r * 128, 16), 128), :] = a[:, 0:512].astype(BF16)
            qf = a[:, 512:1024].astype(BF16).astype(F32)
            sq = qf * qf
            hi = sq.astype(BF16)
            lo = (sq - hi.astype(F32)).astype(BF16)
            ssq = jnp.dot(hi, BLK[...], preferred_element_type=F32) + jnp.dot(
                lo, BLK[...], preferred_element_type=F32
            )
            qg = jnp.concatenate([q_gain[...]] * 8, axis=1) * 0.125
            QB[gi, rows, :] = (qf * lax.rsqrt(ssq * (1.0 / 64) + EPS) * qg).astype(BF16)
            kv = a[:, 1024:1152].astype(BF16).astype(F32)
            is_key = lax.broadcasted_iota(jnp.int32, (128, 128), 1) < 64
            ksq = jnp.sum(jnp.where(is_key, kv * kv, 0.0), axis=-1, keepdims=True)
            kn = kv * lax.rsqrt(ksq * (1.0 / 64) + EPS) * jnp.concatenate([k_gain[...]] * 2, axis=1)
            KV[gi, slot, pl.ds(pl.multiple_of(128 + r * 128, 128), 128), :] = jnp.where(
                is_key, kn, kv
            ).astype(BF16)
            return carry

        lax.fori_loop(0, 4, body, 0)

    def halo_next(gi, i):
        qn, spn, xn, here, away, passed = halo_to(i)
        slot = jnp.where(xn == qn, 0, 1)
        gn = jnp.where(xn == x, gi, 1 - gi)
        tails = (KV.at[gi, i, pl.ds(256, 128)], PB.at[gi, i, pl.ds(256, 16)])
        copies = [
            pltpu.make_async_remote_copy(
                src_ref=src, dst_ref=dst, send_sem=hsend.at[gi, i, k], recv_sem=hrecv.at[gn, slot, k],
                device_id=(spn, xn), device_id_type=MESH,
            )
            for k, (src, dst) in enumerate(
                zip(tails, (KV.at[gn, slot, pl.ds(0, 128)], PB.at[gn, slot, pl.ds(0, 16)]))
            )
        ]
        passes = [
            pltpu.make_async_remote_copy(
                src_ref=src, dst_ref=dst, send_sem=hsend.at[gi, i, k], recv_sem=rlrecv.at[gi, k],
                device_id=dev_sib, device_id_type=MESH,
            )
            for k, (src, dst) in enumerate(zip(tails, (RLK.at[gi], RLP.at[gi])))
        ]
        return here, away, copies, passed, passes

    def halo_send(gi):
        for i in range(2):
            here, away, copies, passed, passes = halo_next(gi, i)

            @pl.when(passed)
            def _():
                for d in passes:
                    d.start()

            @pl.when(away)
            def _():
                for d in copies:
                    d.start()

            @pl.when(here)
            def _():
                KV[gi, 1 - i, pl.ds(0, 128), :] = KV[gi, i, pl.ds(256, 128), :]
                PB[gi, 1 - i, pl.ds(0, 16), :] = PB[gi, i, pl.ds(256, 16), :]

    def halo_sent(gi):
        for i in range(2):
            _, away, copies, passed, passes = halo_next(gi, i)

            @pl.when(passed)
            def _():
                for d in passes:
                    d.wait_send()

            @pl.when(away)
            def _():
                for d in copies:
                    d.wait_send()

    def relay_copies(gi):
        gn = jnp.where(par == x, gi, 1 - gi)
        return [
            pltpu.make_async_remote_copy(
                src_ref=src, dst_ref=dst, send_sem=rlsend.at[gi, k],
                recv_sem=hrecv.at[gn, relay_slot, k], device_id=relay_dev, device_id_type=MESH,
            )
            for k, (src, dst) in enumerate(
                (
                    (RLK.at[gi], KV.at[gn, relay_slot, pl.ds(0, 128)]),
                    (RLP.at[gi], PB.at[gn, relay_slot, pl.ds(0, 16)]),
                )
            )
        ]

    def halo_relay(gi):
        @pl.when(relay)
        def _():
            for k, dst in enumerate((RLK.at[gi], RLP.at[gi])):
                pltpu.make_async_copy(dst, dst, rlrecv.at[gi, k]).wait()
            for d in relay_copies(gi):
                d.start()

    def relay_sent(gi):
        @pl.when(relay)
        def _():
            for d in relay_copies(gi):
                d.wait_send()

    def halo_wait(gi):
        for i in range(2):
            first, apart, _, _ = halo_from(i)

            @pl.when(first)
            def _():
                KV[gi, i, pl.ds(0, 128), :] = jnp.zeros((128, 128), BF16)
                PB[gi, i, pl.ds(0, 16), :] = jnp.zeros((16, 512), BF16)

            @pl.when(apart)
            def _():
                for k, dst in enumerate((KV.at[gi, i, pl.ds(0, 128)], PB.at[gi, i, pl.ds(0, 16)])):
                    pltpu.make_async_copy(dst, dst, hrecv.at[gi, i, k]).wait()

    def pool(gi, g):
        span = lax.shift_left(jnp.int32(2), g)
        for i in range(2):
            pf = PB[gi, i].astype(F32)
            t2 = pf + pltpu.roll(pf, 1, 0)
            t4 = t2 + pltpu.roll(t2, 2, 0)
            t8 = t4 + pltpu.roll(t4, 4, 0)
            t16 = t8 + pltpu.roll(t8, 8, 0)
            run = jnp.where(g == 0, t2, jnp.where(g == 1, t4, jnp.where(g == 2, t8, t16)))[16:]
            pos = sp * 1024 + quarters[i] * 256 + lax.broadcasted_iota(jnp.int32, (256, 1), 0)
            count = jnp.minimum(pos + 1, span).astype(F32)
            diff = (run * (1.0 / count) - pf[16:]).astype(BF16)
            m = jnp.dot(diff, PM[gi], preferred_element_type=F32)
            m = m * (scale_in if gi == 0 else SCALE)[...]
            m = m * lax.rsqrt(jnp.mean(m * m, axis=-1, keepdims=True) + EPS)
            MIX[gi, i * 256 : (i + 1) * 256, 0:512] = m.astype(BF16)

    def attend(gi, r):
        sink = jnp.exp((sinks_in if gi == 0 else SINK)[...])
        left = lax.broadcasted_iota(jnp.int32, (1, 128), 1) < 64
        es = jnp.concatenate(
            [
                jnp.broadcast_to(
                    jnp.where(left, sink[:, 2 * j : 2 * j + 1], sink[:, 2 * j + 1 : 2 * j + 2]),
                    (128, 128),
                )
                for j in range(4)
            ],
            axis=0,
        )

        def body(k, carry):
            slot = k
            rows = pl.ds(pl.multiple_of(k * 256 + r * 128, 128), 128)
            kv = KV[gi, slot, pl.ds(r * 128, 256), :].astype(F32)
            low = lax.broadcasted_iota(jnp.int32, (256, 128), 1) < 64
            ke = jnp.where(low, kv, 0.0)
            vo = jnp.where(low, 0.0, kv)
            ko = pltpu.roll(ke, 64, 1)
            ve = pltpu.roll(vo, 64, 1)
            q_here = (1 - slot) * x + slot * p
            missing = jnp.where((sp == 0) & (q_here == 0), 128, 0) if r == 0 else 0
            there = lax.broadcasted_iota(jnp.int32, (256, 128), 0) >= missing
            oe = jnp.where(low & there, 1.0, 0.0)
            oo = jnp.where(jnp.logical_not(low) & there, 1.0, 0.0)
            keys = jnp.concatenate([ke, ko], axis=0).astype(BF16)
            values = jnp.concatenate(
                [jnp.concatenate([ve, oe], axis=1), jnp.concatenate([vo, oo], axis=1)], axis=0
            ).astype(BF16)
            q = QB[gi, rows, :]
            q = jnp.concatenate([q[:, j * 128 : (j + 1) * 128] for j in range(4)], axis=0)
            sc = lax.dot_general(q, keys, (((1,), (1,)), ((), ())), preferred_element_type=F32)
            e = jnp.exp(sc + BIAS[gi]).astype(BF16)
            o = jnp.dot(e, values, preferred_element_type=F32)
            att = o[:, 0:128] / (o[:, 128:256] + es)
            parts = [att[j * 128 : (j + 1) * 128] for j in range(4)]
            sq = parts[0] * parts[0]
            for j in range(1, 4):
                sq += parts[j] * parts[j]
            r_ = lax.rsqrt(jnp.sum(sq, axis=-1, keepdims=True) * (1.0 / 512) + EPS)
            for j in range(4):
                MIX[gi, rows, 512 + j * 128 : 640 + j * 128] = (parts[j] * r_).astype(BF16)
            return carry

        lax.fori_loop(0, 2, body, 0)

    recv(*d1)
    sib1.append(share1(0, s2))
    ACC[...] = jnp.zeros_like(ACC)
    recv(*sib1)
    matmul_slab(0, x)
    recv(*tp_)
    scale_slab(p)
    matmul_slab(0, p)
    d1o = step_d1(1, (c1oa, c1ob))
    recv(*b2, *b2o)
    c2a = c2_send(0, 1)
    c2b = c2_send(1, 0)
    plane2 = W2.at[c, s]
    sib2_own = [send(plane2, plane2, dev_sib)]
    for d in tf:
        d.wait_send()
    scale_slab(n)
    matmul_slab(0, n)
    recv(*tf)
    scale_slab(x2)
    matmul_slab(0, x2)
    post(0)
    halo_send(0)
    recv(*c1ob)
    sib1o += [share1(1, sd), share1(1, su)]
    recv(x_pm)
    f_pm = send(ST3, PM.at[1, half], dev_dx)
    ACC[...] = jnp.zeros_like(ACC)
    matmul_planes(1, c, s, s, 1)
    matmul_planes(1, c, sd, su, 2)
    recv(*sib1o)
    matmul_planes(1, cs, ss_, ss_, 1)
    matmul_planes(1, cs, ssd, ssu, 2)
    halo_relay(0)
    attend(0, 1)
    recv(*d1o)
    sib1o_far = share1(1, s2)
    matmul_planes(1, c, s2, s2, 1)
    recv(sib1o_far)
    matmul_planes(1, cs, ss2, ss2, 1)
    post(1)
    halo_send(1)

    recv(*sc_c)
    attend(1, 1)
    halo_relay(1)
    recv(f_pm)
    sib_pm = send(PM.at[1, half], PM.at[1, half], dev_sib)
    halo_wait(0)
    attend(0, 0)
    pool(0, x)
    halo_wait(1)
    attend(1, 0)
    recv(sib_pm)
    pool(1, x2)
    recv(*c2a)
    u0, d0 = half_plane(sd, 0), half_plane(su, 1)
    d2 = [[send(u0.at[k], u0.at[k], dev_su), send(d0.at[k], d0.at[k], dev_sd)] for k in range(2)]
    sib2_a = [send(u0, u0, dev_sib), send(d0, d0, dev_sib)]

    def unit(u, cc, s_, fs):
        rhs = []
        for g in range(2):
            rhs.append(jnp.concatenate([W2[cc, s_, fs[0], g], W2[cc, s_, fs[1], g]], axis=1))
        o = jnp.dot(MIX[0], rhs[0], preferred_element_type=F32)
        o += jnp.dot(MIX[1], rhs[1], preferred_element_type=F32)
        ob = o.astype(BF16)
        for e in range(2):
            idx = 2 * u + e
            OWNB[idx] = ob[0:256, e * 128 : (e + 1) * 128]
            SENDB[idx] = ob[256:512, e * 128 : (e + 1) * 128]
            out_copy(idx).start()

    def out_copy(idx):
        return pltpu.make_async_remote_copy(
            src_ref=SENDB.at[idx], dst_ref=RECVB.at[idx], send_sem=osend.at[idx],
            recv_sem=orecv.at[idx], device_id=dev_p, device_id_type=MESH,
        )

    def total(u, cc, s_, fs):
        for e in range(2):
            idx = 2 * u + e
            col = pl.ds(pl.multiple_of(sp_of(cc, fs[e], s_) * 128, 128), 128)
            out_copy(idx).wait_recv()
            OWNB[idx] = (OWNB[idx].astype(F32) + RECVB[idx].astype(F32)).astype(BF16)
            pltpu.make_async_copy(OWNB.at[idx], out.at[:, col], oloc.at[idx]).start()

    def pair(stage, mine, sA, kA, sB, kB, act=unit):
        cc = c if mine else cs

        def body(t, carry):
            k = kA + t * (kB - kA)
            act(stage * 4 + (0 if mine else 2) + t, cc, sA + t * (sB - sA), (2 * k, 2 * k + 1))
            return carry

        lax.fori_loop(0, 2, body, 0)

    pair(0, True, s, 0, s, 1)
    recv(*sib2_own)
    pair(0, False, ss_, 0, ss_, 1)

    pair(1, True, sd, 0, su, 1)
    recv(*sib2_a)
    pair(1, False, ssd, 0, ssu, 1)
    recv(*c2b)
    u1, d1_ = half_plane(sd, 1), half_plane(su, 0)
    sib2_b = [send(u1, u1, dev_sib), send(d1_, d1_, dev_sib)]
    pair(2, True, sd, 1, su, 0)
    recv(*sib2_b)
    pair(2, False, ssd, 1, ssu, 0)

    pair(0, True, s, 0, s, 1, total)
    pair(0, False, ss_, 0, ss_, 1, total)
    for k in range(2):
        recv(*d2[k])
        far = [W2.at[c, s2, k], W2.at[c, s2, 2 + k]]
        sib2_c = [send(r, r, dev_sib) for r in far]
        unit(12 + 2 * k, c, s2, (k, 2 + k))
        recv(*sib2_c)
        unit(13 + 2 * k, cs, ss2, (k, 2 + k))
        if k == 0:
            pair(1, True, sd, 0, su, 1, total)
            pair(1, False, ssd, 0, ssu, 1, total)

    pair(2, True, sd, 1, su, 0, total)
    pair(2, False, ssd, 1, ssu, 0, total)
    for k in range(2):
        total(12 + 2 * k, c, s2, (k, 2 + k))
        total(13 + 2 * k, cs, ss2, (k, 2 + k))

    tf_ids = {id(d) for d in tf}
    for d in pending:
        if id(d) not in tf_ids:
            d.wait_send()
    for gi in range(2):
        halo_sent(gi)
        relay_sent(gi)

    def drain(idx, carry):
        out_copy(idx).wait_send()
        col = pl.ds(pl.multiple_of(idx * 128, 128), 128)
        pltpu.make_async_copy(OWNB.at[idx], out.at[:, col], oloc.at[idx]).wait()
        return carry

    lax.fori_loop(0, 32, drain, 0)


def local_program(
    tokens, norm_gain, w_pool_in, w_query, w_key, w_value, pool_map, pool_scale,
    q_gain, k_gain, sinks, w_out,
):
    any_ = pl.BlockSpec(memory_space=pl.ANY)
    vmem = pl.BlockSpec(memory_space=pltpu.VMEM)
    dma = pltpu.SemaphoreType.DMA
    return pl.pallas_call(
        kernel,
        out_shape=jax.ShapeDtypeStruct((256, 4096), BF16),
        in_specs=[any_] * 7 + [vmem] * 5,
        out_specs=any_,
        scratch_shapes=[
            pltpu.VMEM((2, 2, 4, 4, 128, 1152), BF16),
            pltpu.VMEM((2, 4, 4, 2, 1024, 128), BF16),
            pltpu.VMEM((2, 4, 256, 1024), BF16),
            pltpu.VMEM((128, 1152), BF16),
            pltpu.VMEM((1024, 128), BF16),
            pltpu.VMEM((256, 512), BF16),
            pltpu.VMEM((2, 512, 512), BF16),
            pltpu.VMEM((1, 512), F32),
            pltpu.VMEM((1, 8), F32),
            pltpu.VMEM((128, 128), BF16),
            pltpu.VMEM((2, 2, 384, 128), BF16),
            pltpu.VMEM((2, 2, 272, 512), BF16),
            pltpu.VMEM((2, 512, 512), BF16),
            pltpu.VMEM((512, 1152), F32),
            pltpu.VMEM((2, 256, 128), F32),
            pltpu.VMEM((2, 512, 1024), BF16),
            pltpu.VMEM((2, 512, 512), F32),
            pltpu.VMEM((512, 512), BF16),
            pltpu.VMEM((32, 256, 128), BF16),
            pltpu.VMEM((32, 256, 128), BF16),
            pltpu.VMEM((32, 256, 128), BF16),
            pltpu.VMEM((2, 128, 128), BF16),
            pltpu.VMEM((2, 16, 512), BF16),
            dma((8,)),
            dma((N_COPIES,)),
            dma((N_COPIES,)),
            dma((32,)),
            dma((32,)),
            dma((32,)),
            dma((2, 2, 2)),
            dma((2, 2, 2)),
            dma((2, 2)),
            dma((2, 2)),
        ],
        compiler_params=pltpu.CompilerParams(
            collective_id=0, has_side_effects=True, vmem_limit_bytes=66_000_000
        ),
        name="mixer",
    )(
        tokens, w_pool_in, w_query, w_key.T, w_value.T, w_out, pool_map.reshape(512, 512),
        pool_scale.reshape(1, 512), sinks.reshape(1, 8), q_gain.reshape(1, 64),
        k_gain.reshape(1, 64), norm_gain.reshape(1, 4096),
    )


def solution(mesh):
    in_specs = (
        P("sp", "tp"), P(), P("sp", "tp"), P("sp", "tp"), P("sp", "tp"), P("sp", "tp"),
        P("tp", None, None), P("tp"), P(), P(), P("tp"), P("tp", "sp"),
    )
    out_specs = P(("sp", "tp"), None)
    return jax.shard_map(local_program, mesh=mesh, in_specs=in_specs, out_specs=out_specs, check_vma=False)
```

```python
import jax
import jax.numpy as jnp
from jax import lax
from jax.experimental import pallas as pl
from jax.experimental.pallas import tpu as pltpu
from jax.sharding import PartitionSpec as P

MESH = pl.DeviceIdType.MESH
F32 = jnp.float32
BF16 = jnp.bfloat16
EPS = 1e-6
N_GROUPS = 41


def mod4(v):
    return lax.rem(v, 4)


def kernel(
    tokens, wp, wq, wk_t, wv_t, wo, pmap, scale_in, sinks_in, q_gain, k_gain, gain,
    out,
    W1, W2, TOK, ST1, ST2, ST3, PM, SCALE, SINK, KVT, KV, PB, QB, ACC, SS, MIX, BIAS, BLK, SENDB, OWNB, RECVB, RLK, RLP,
    lsem, ssem, rsem, osend, orecv, oloc, hsend, hrecv, rlsend, rlrecv,
):
    sp = lax.axis_index("sp")
    x = lax.axis_index("tp")
    c = lax.rem(sp, 2)
    y = mod4(lax.div(sp, 2))
    z = lax.div(sp, 8)
    f = y + c * (z - y)
    s = z + c * (y - z)
    par = lax.rem(x, 2)
    flip1 = x + 1 - 2 * par
    flip3 = 3 - x
    p = (1 - c) * flip1 + c * flip3
    n = (1 - c) * flip3 + c * flip1
    x2 = mod4(x + 2)
    dx = mod4(x + 1 + 2 * c)

    def sp_of(c_, f_, s_):
        y_ = (1 - c_) * f_ + c_ * s_
        z_ = (1 - c_) * s_ + c_ * f_
        return (z_ * 4 + y_) * 2 + c_

    fu, fd = mod4(f + 1), mod4(f + 3)
    su, sd, s2 = mod4(s + 1), mod4(s + 3), mod4(s + 2)
    dev_fu, dev_fd = (sp_of(c, fu, s), x), (sp_of(c, fd, s), x)
    dev_su, dev_sd = (sp_of(c, f, su), x), (sp_of(c, f, sd), x)
    dev_sib = (sp + 1 - 2 * c, x)
    dev_dx, dev_p, dev_n, dev_x2 = (sp, dx), (sp, p), (sp, n), (sp, x2)
    cs, ss_, sf_ = 1 - c, f, s
    ssu, ssd, ss2 = mod4(ss_ + 1), mod4(ss_ + 3), mod4(ss_ + 2)

    groups = []
    W1_SENT, W2_SENT, TOK_SENT, TF_SENT, OTHER_SENT = range(5)

    def group(whole):
        groups.append(whole)
        return len(groups) - 1

    def send(src, dst, dev, to, sent):
        pltpu.make_async_remote_copy(
            src_ref=src, dst_ref=dst, send_sem=ssem.at[sent], recv_sem=rsem.at[to],
            device_id=dev, device_id_type=MESH,
        ).start()

    def wait(whole, sem):
        pltpu.make_async_copy(whole, whole, sem).wait()

    def recv(*gs):
        for g in gs:
            wait(groups[g], rsem.at[g])

    loc = []

    def local(src, dst):
        d = pltpu.make_async_copy(src, dst, lsem.at[len(loc)])
        d.start()
        loc.append(d)
        return d

    own1 = W1.at[0, c, s, f]
    l0 = local(wp, own1.at[:, pl.ds(0, 512)])
    l1 = local(wq, own1.at[:, pl.ds(512, 512)])
    l2 = local(wk_t, KVT.at[pl.ds(0, 64)])
    l7 = local(wv_t, KVT.at[pl.ds(64, 64)])
    l3 = local(wo, W2.at[c, s, f, 0])
    l4 = local(tokens.at[pl.ds(x * 256, 256)], TOK.at[0, x])
    l5 = local(tokens.at[pl.ds(p * 256, 256)], TOK.at[1, x])
    l6 = local(pmap, PM.at[0])

    def holder(q, c_):
        inner = lax.rem(lax.div(q + 1, 2), 2)
        even = lax.div(q, 2) * 2 + par
        odd = inner * (2 - par) + (1 - inner) * 3 * par
        return (1 - c_) * even + c_ * odd

    quarters = (x, p)

    def halo_to(i):
        q = quarters[i]
        qn = mod4(q + 1)
        spn = sp + lax.div(q + 1, 4)
        xn = holder(qn, lax.rem(spn, 2))
        here = (spn == sp) & (xn == x)
        away = jnp.logical_not(here) & (spn < 32)
        passed = away & (c == 1) & (q == 3)
        return qn, jnp.where(spn < 32, spn, 0), xn, here, away & jnp.logical_not(passed), passed

    def halo_from(i):
        q = quarters[i]
        first = (sp == 0) & (q == 0)
        back = jnp.where(q == 0, 1, 0)
        relayed = (back == 1) & (c == 0)
        spp = jnp.where(first, sp, sp - back - jnp.where(relayed, 1, 0))
        xp = holder(mod4(q + 3), lax.rem(sp - back + 2, 2))
        here = (back == 0) & (xp == x)
        return first, jnp.logical_not(first) & jnp.logical_not(here), spp, xp

    relay = (c == 0) & ((x == 0) | (x == 3)) & (sp < 30)
    relay_dev = (jnp.where(relay, sp + 2, 0), par)
    relay_slot = jnp.where(par == 0, 0, 1)

    barrier = pltpu.get_barrier_semaphore()

    def greet(dev):
        pl.semaphore_signal(barrier, inc=1, device_id=dev, device_id_type=MESH)

    for dev in (dev_fu, dev_fd, dev_su, dev_sd, dev_sib, dev_p, dev_n, dev_x2):
        greet(dev)
    @pl.when(relay)
    def _():
        greet(relay_dev)

    for i in range(2):
        _, spn, xn, _, away, _ = halo_to(i)

        @pl.when(away)
        def _():
            greet((spn, xn))

        _, apart, spp, xp = halo_from(i)

        @pl.when(apart)
        def _():
            greet((spp, xp))

    lane_i = lax.broadcasted_iota(jnp.int32, (512, 512), 1)
    row_i = lax.broadcasted_iota(jnp.int32, (512, 512), 0)
    l2.wait()
    l7.wait()
    W1[0, c, s, f, :, pl.ds(1024, 128)] = KVT[...].astype(F32).T.astype(BF16)
    BLK[...] = jnp.where(
        lax.shift_right_logical(lane_i, 6) == lax.shift_right_logical(row_i, 6), 1.0, 0.0
    ).astype(BF16)
    SS[...] = jnp.zeros_like(SS)
    key_i = jnp.bitwise_and(lane_i, 255)
    dist = 128 + jnp.bitwise_and(row_i, 127) - key_i
    band = (dist >= 0) & (dist < 128)
    head_in = 2 * lax.shift_right_logical(row_i, 7) + lax.shift_right_logical(lane_i, 8) + 1
    for gi, g in ((0, x), (1, x2)):
        slope = jnp.exp2(-0.25 * (g * 8 + head_in).astype(F32))
        BIAS[gi] = jnp.where(band, -slope * dist.astype(F32), -1e30)

    peers = 8 + jnp.where(relay, 1, 0)
    for i in range(2):
        peers += jnp.where(halo_to(i)[4], 1, 0) + jnp.where(halo_from(i)[1], 1, 0)
    pl.semaphore_wait(barrier, peers)

    l0.wait()
    l1.wait()
    l3.wait()
    shard1, shard2 = W1.at[0, 0, 0, 0], W2.at[0, 0, 0]

    def send1(piece, dev, to):
        send(piece, piece, dev, to, W1_SENT)

    def send2(piece, dev, to):
        send(piece, piece, dev, to, W2_SENT)

    def step_a1(g):
        piece = W1.at[g, c, s, f]
        to = group(shard1), group(shard1)
        for k in range(2):
            send1(piece.at[pl.ds(64 * k, 64)], dev_fu, to[k])
            send1(piece.at[pl.ds(64 - 64 * k, 64)], dev_fd, to[k])
        return to

    def step_b1(g, a):
        recv(a[0])
        to = group(shard1)
        send1(W1.at[g, c, s, fd, pl.ds(0, 64)], dev_fu, to)
        send1(W1.at[g, c, s, fu, pl.ds(64, 64)], dev_fd, to)
        return to

    def step_c1(g, a, b, shared):
        recv(a[1], b)
        plane = W1.at[g, c, s]
        to = group(W1.at[0, 0, 0]), group(W1.at[0, 0, 0])
        for k in range(2):
            send1(plane.at[pl.ds(2 * k, 2)], dev_su, to[k])
            send1(plane.at[pl.ds(2 - 2 * k, 2)], dev_sd, to[k])
        send1(plane, dev_sib, shared)
        return to

    def step_d1(g, cc):
        recv(cc[0])
        to = group(W1.at[0, 0, 0])
        send1(W1.at[g, c, sd, pl.ds(0, 2)], dev_su, to)
        send1(W1.at[g, c, su, pl.ds(2, 2)], dev_sd, to)
        return to

    def share1(g, s_, to):
        send1(W1.at[g, c, s_], dev_sib, to)

    def step_a2(g):
        to = group(shard2)
        for dev in (dev_fu, dev_fd):
            send2(W2.at[c, s, f, g], dev, to)
        return to

    def step_b2(g, a):
        recv(a)
        to = group(shard2.at[0])
        send2(W2.at[c, s, fd, g, pl.ds(0, 512)], dev_fu, to)
        send2(W2.at[c, s, fu, g, pl.ds(512, 512)], dev_fd, to)
        return to

    x_w1 = [group(shard1.at[pl.ds(0, 64)]) for _ in range(2)]
    for k in range(2):
        part = pl.ds(64 * k, 64)
        send(own1.at[part], ST1.at[part], dev_dx, x_w1[k], W1_SENT)
    a1 = step_a1(0)
    a2 = step_a2(0)
    x_w2 = group(shard2.at[0])
    send(W2.at[c, s, f, 0], ST2, dev_dx, x_w2, W2_SENT)

    f_w1 = group(shard1)
    for k in range(2):
        recv(x_w1[k])
        part = pl.ds(64 * k, 64)
        send(ST1.at[part], W1.at[1, c, s, f, part], dev_dx, f_w1, W1_SENT)
        if k == 0:
            b1 = step_b1(0, a1)
    sib1 = group(W1.at[0, 0])
    c1a, c1b = step_c1(0, a1, b1, sib1)
    recv(x_w2)
    f_w2 = group(shard2.at[0])
    send(ST2, W2.at[c, s, f, 1], dev_dx, f_w2, W2_SENT)
    two_slabs = TOK.at[0, pl.ds(0, 2)]
    tn = group(two_slabs)
    send(tokens.at[pl.ds(n * 256, 256)], TOK.at[0, x], dev_n, tn, TOK_SENT)
    send(tokens.at[pl.ds(x2 * 256, 256)], TOK.at[1, x], dev_n, tn, TOK_SENT)
    sc_c, sk_c = group(SCALE), group(SINK)
    send(scale_in, SCALE, dev_x2, sc_c, OTHER_SENT)
    send(sinks_in, SINK, dev_x2, sk_c, OTHER_SENT + 1)

    recv(f_w1)
    a1o = step_a1(1)

    def scale_slab(j):
        g = gain[:, pl.ds(pl.multiple_of(j * 1024, 1024), 1024)]

        def body(k, carry):
            slot, r = lax.div(k, 4), pl.ds(lax.rem(k, 4) * 64, 64)
            t = TOK[slot, j, r, :].astype(F32)
            sq = t * t
            tot = sq[:, 0:128]
            for m in range(1, 8):
                tot += sq[:, m * 128 : (m + 1) * 128]
            SS[slot, r, :] += tot
            TOK[slot, j, r, :] = (t * g).astype(BF16)
            return carry

        lax.fori_loop(0, 8, body, 0)

    l4.wait()
    l5.wait()
    scale_slab(x)
    b1o = step_b1(1, a1o)
    recv(f_w2)
    a2o = step_a2(1)
    b2 = step_b2(0, a2)
    d1 = step_d1(0, (c1a, c1b))
    sib1o = group(W1.at[0, 0, pl.ds(0, 3)])
    c1o = step_c1(1, a1o, b1o, sib1o)
    tp_ = group(two_slabs)
    send(tokens.at[pl.ds(p * 256, 256)], TOK.at[0, x], dev_p, tp_, TOK_SENT)
    send(tokens.at[pl.ds(x * 256, 256)], TOK.at[1, x], dev_p, tp_, TOK_SENT)
    recv(c1b)
    share1(0, sd, sib1)
    share1(0, su, sib1)
    recv(tn)
    tf = group(two_slabs)
    send(TOK.at[0, n], TOK.at[1, n], dev_p, tf, TF_SENT)
    send(TOK.at[1, n], TOK.at[0, n], dev_p, tf, TF_SENT)
    l6.wait()
    half = pl.ds(c * 256, 256)
    x_pm = group(ST3)
    send(PM.at[0, half], ST3, dev_dx, x_pm, OTHER_SENT + 2)
    b2o = step_b2(1, a2o)

    def half_plane(s_, k):
        return W2.at[c, s_, pl.ds(2 * k, 2)]

    def c2_send(k_up, k_dn):
        to = group(W2.at[0, 0])
        send2(half_plane(s, k_up), dev_su, to)
        send2(half_plane(s, k_dn), dev_sd, to)
        return to

    def matmul(gi, jz):
        parts = []
        for yy in range(4):
            parts.append(W1[gi, 0, jz, yy])
            parts.append(W1[gi, 1, yy, jz])
        rhs = jnp.concatenate(parts, axis=0)
        lhs = TOK[:, jz].reshape(512, 1024)
        ACC[...] += jnp.dot(lhs, rhs, preferred_element_type=F32)

    def matmul_slab(gi, jz):
        lax.fori_loop(0, 1, lambda t, carry: (matmul(gi, jz), carry)[1], 0)

    def matmul_planes(gi, cc, sA, sB, count):
        def body(t, carry):
            s_ = sA + t * (sB - sA)
            rhs = jnp.concatenate([W1[gi, cc, s_, k] for k in range(4)], axis=0)
            lhs = []
            for k in range(4):
                off = ((1 - cc) * k + cc * s_) * 256 + cc * 128
                col = pl.ds(pl.multiple_of(off, 128), 128)
                lhs.append(TOK[:, (1 - cc) * s_ + cc * k, :, col].reshape(512, 128))
            lhs = jnp.concatenate(lhs, axis=1)
            ACC[...] += jnp.dot(lhs, rhs, preferred_element_type=F32)
            return carry

        lax.fori_loop(0, count, body, 0)

    def post(gi):
        def body(k, carry):
            slot, r = lax.div(k, 2), lax.rem(k, 2)
            rows = pl.ds(pl.multiple_of(k * 128, 128), 128)
            tot = jnp.sum(SS[slot, pl.ds(r * 128, 128), :], axis=-1, keepdims=True)
            a = ACC[rows, :] * lax.rsqrt(tot * (1.0 / 4096) + EPS)
            PB[gi, slot, pl.ds(pl.multiple_of(16 + r * 128, 16), 128), :] = a[:, 0:512].astype(BF16)
            qf = a[:, 512:1024].astype(BF16).astype(F32)
            sq = qf * qf
            hi = sq.astype(BF16)
            lo = (sq - hi.astype(F32)).astype(BF16)
            ssq = jnp.dot(hi, BLK[...], preferred_element_type=F32) + jnp.dot(
                lo, BLK[...], preferred_element_type=F32
            )
            qg = jnp.concatenate([q_gain[...]] * 8, axis=1) * 0.125
            QB[gi, rows, :] = (qf * lax.rsqrt(ssq * (1.0 / 64) + EPS) * qg).astype(BF16)
            kv = a[:, 1024:1152].astype(BF16).astype(F32)
            is_key = lax.broadcasted_iota(jnp.int32, (128, 128), 1) < 64
            ksq = jnp.sum(jnp.where(is_key, kv * kv, 0.0), axis=-1, keepdims=True)
            kn = kv * lax.rsqrt(ksq * (1.0 / 64) + EPS) * jnp.concatenate([k_gain[...]] * 2, axis=1)
            KV[gi, slot, pl.ds(pl.multiple_of(128 + r * 128, 128), 128), :] = jnp.where(
                is_key, kn, kv
            ).astype(BF16)
            return carry

        lax.fori_loop(0, 4, body, 0)

    def halo_next(gi, i):
        qn, spn, xn, here, away, passed = halo_to(i)
        slot = jnp.where(xn == qn, 0, 1)
        gn = jnp.where(xn == x, gi, 1 - gi)
        tails = (KV.at[gi, i, pl.ds(256, 128)], PB.at[gi, i, pl.ds(256, 16)])
        copies = [
            pltpu.make_async_remote_copy(
                src_ref=src, dst_ref=dst, send_sem=hsend.at[gi, i, k], recv_sem=hrecv.at[gn, slot, k],
                device_id=(spn, xn), device_id_type=MESH,
            )
            for k, (src, dst) in enumerate(
                zip(tails, (KV.at[gn, slot, pl.ds(0, 128)], PB.at[gn, slot, pl.ds(0, 16)]))
            )
        ]
        passes = [
            pltpu.make_async_remote_copy(
                src_ref=src, dst_ref=dst, send_sem=hsend.at[gi, i, k], recv_sem=rlrecv.at[gi, k],
                device_id=dev_sib, device_id_type=MESH,
            )
            for k, (src, dst) in enumerate(zip(tails, (RLK.at[gi], RLP.at[gi])))
        ]
        return here, away, copies, passed, passes

    def halo_send(gi):
        for i in range(2):
            here, away, copies, passed, passes = halo_next(gi, i)

            @pl.when(passed)
            def _():
                for d in passes:
                    d.start()

            @pl.when(away)
            def _():
                for d in copies:
                    d.start()

            @pl.when(here)
            def _():
                KV[gi, 1 - i, pl.ds(0, 128), :] = KV[gi, i, pl.ds(256, 128), :]
                PB[gi, 1 - i, pl.ds(0, 16), :] = PB[gi, i, pl.ds(256, 16), :]

    def halo_sent(gi):
        for i in range(2):
            _, away, copies, passed, passes = halo_next(gi, i)

            @pl.when(passed)
            def _():
                for d in passes:
                    d.wait_send()

            @pl.when(away)
            def _():
                for d in copies:
                    d.wait_send()

    def relay_copies(gi):
        gn = jnp.where(par == x, gi, 1 - gi)
        return [
            pltpu.make_async_remote_copy(
                src_ref=src, dst_ref=dst, send_sem=rlsend.at[gi, k],
                recv_sem=hrecv.at[gn, relay_slot, k], device_id=relay_dev, device_id_type=MESH,
            )
            for k, (src, dst) in enumerate(
                (
                    (RLK.at[gi], KV.at[gn, relay_slot, pl.ds(0, 128)]),
                    (RLP.at[gi], PB.at[gn, relay_slot, pl.ds(0, 16)]),
                )
            )
        ]

    def halo_relay(gi):
        @pl.when(relay)
        def _():
            for k, dst in enumerate((RLK.at[gi], RLP.at[gi])):
                pltpu.make_async_copy(dst, dst, rlrecv.at[gi, k]).wait()
            for d in relay_copies(gi):
                d.start()

    def relay_sent(gi):
        @pl.when(relay)
        def _():
            for d in relay_copies(gi):
                d.wait_send()

    def halo_wait(gi):
        for i in range(2):
            first, apart, _, _ = halo_from(i)

            @pl.when(first)
            def _():
                KV[gi, i, pl.ds(0, 128), :] = jnp.zeros((128, 128), BF16)
                PB[gi, i, pl.ds(0, 16), :] = jnp.zeros((16, 512), BF16)

            @pl.when(apart)
            def _():
                for k, dst in enumerate((KV.at[gi, i, pl.ds(0, 128)], PB.at[gi, i, pl.ds(0, 16)])):
                    pltpu.make_async_copy(dst, dst, hrecv.at[gi, i, k]).wait()

    def pool(gi, g):
        span = lax.shift_left(jnp.int32(2), g)
        for i in range(2):
            pf = PB[gi, i].astype(F32)
            t2 = pf + pltpu.roll(pf, 1, 0)
            t4 = t2 + pltpu.roll(t2, 2, 0)
            t8 = t4 + pltpu.roll(t4, 4, 0)
            t16 = t8 + pltpu.roll(t8, 8, 0)
            run = jnp.where(g == 0, t2, jnp.where(g == 1, t4, jnp.where(g == 2, t8, t16)))[16:]
            pos = sp * 1024 + quarters[i] * 256 + lax.broadcasted_iota(jnp.int32, (256, 1), 0)
            count = jnp.minimum(pos + 1, span).astype(F32)
            diff = (run * (1.0 / count) - pf[16:]).astype(BF16)
            m = jnp.dot(diff, PM[gi], preferred_element_type=F32)
            m = m * (scale_in if gi == 0 else SCALE)[...]
            m = m * lax.rsqrt(jnp.mean(m * m, axis=-1, keepdims=True) + EPS)
            MIX[gi, i * 256 : (i + 1) * 256, 0:512] = m.astype(BF16)

    def attend(gi, r):
        sink = jnp.exp((sinks_in if gi == 0 else SINK)[...])
        left = lax.broadcasted_iota(jnp.int32, (1, 128), 1) < 64
        es = jnp.concatenate(
            [
                jnp.broadcast_to(
                    jnp.where(left, sink[:, 2 * j : 2 * j + 1], sink[:, 2 * j + 1 : 2 * j + 2]),
                    (128, 128),
                )
                for j in range(4)
            ],
            axis=0,
        )

        def body(k, carry):
            slot = k
            rows = pl.ds(pl.multiple_of(k * 256 + r * 128, 128), 128)
            kv = KV[gi, slot, pl.ds(r * 128, 256), :].astype(F32)
            low = lax.broadcasted_iota(jnp.int32, (256, 128), 1) < 64
            ke = jnp.where(low, kv, 0.0)
            vo = jnp.where(low, 0.0, kv)
            ko = pltpu.roll(ke, 64, 1)
            ve = pltpu.roll(vo, 64, 1)
            q_here = (1 - slot) * x + slot * p
            missing = jnp.where((sp == 0) & (q_here == 0), 128, 0) if r == 0 else 0
            there = lax.broadcasted_iota(jnp.int32, (256, 128), 0) >= missing
            oe = jnp.where(low & there, 1.0, 0.0)
            oo = jnp.where(jnp.logical_not(low) & there, 1.0, 0.0)
            keys = jnp.concatenate([ke, ko], axis=0).astype(BF16)
            values = jnp.concatenate(
                [jnp.concatenate([ve, oe], axis=1), jnp.concatenate([vo, oo], axis=1)], axis=0
            ).astype(BF16)
            q = QB[gi, rows, :]
            q = jnp.concatenate([q[:, j * 128 : (j + 1) * 128] for j in range(4)], axis=0)
            sc = lax.dot_general(q, keys, (((1,), (1,)), ((), ())), preferred_element_type=F32)
            e = jnp.exp(sc + BIAS[gi]).astype(BF16)
            o = jnp.dot(e, values, preferred_element_type=F32)
            att = o[:, 0:128] / (o[:, 128:256] + es)
            parts = [att[j * 128 : (j + 1) * 128] for j in range(4)]
            sq = parts[0] * parts[0]
            for j in range(1, 4):
                sq += parts[j] * parts[j]
            r_ = lax.rsqrt(jnp.sum(sq, axis=-1, keepdims=True) * (1.0 / 512) + EPS)
            for j in range(4):
                MIX[gi, rows, 512 + j * 128 : 640 + j * 128] = (parts[j] * r_).astype(BF16)
            return carry

        lax.fori_loop(0, 2, body, 0)

    recv(d1)
    share1(0, s2, sib1)
    ACC[...] = jnp.zeros_like(ACC)
    recv(sib1)
    matmul_slab(0, x)
    recv(tp_)
    scale_slab(p)
    matmul_slab(0, p)
    d1o = step_d1(1, c1o)
    recv(b2, b2o)
    c2a = c2_send(0, 1)
    c2b = c2_send(1, 0)
    sib2_own = group(W2.at[0, 0])
    send2(W2.at[c, s], dev_sib, sib2_own)
    wait(two_slabs, ssem.at[TF_SENT])
    scale_slab(n)
    matmul_slab(0, n)
    recv(tf)
    scale_slab(x2)
    matmul_slab(0, x2)
    post(0)
    halo_send(0)
    recv(c1o[1])
    share1(1, sd, sib1o)
    share1(1, su, sib1o)
    recv(x_pm)
    f_pm = group(ST3)
    send(ST3, PM.at[1, half], dev_dx, f_pm, OTHER_SENT + 3)
    ACC[...] = jnp.zeros_like(ACC)
    matmul_planes(1, c, s, s, 1)
    matmul_planes(1, c, sd, su, 2)
    recv(sib1o)
    matmul_planes(1, cs, ss_, ss_, 1)
    matmul_planes(1, cs, ssd, ssu, 2)
    halo_relay(0)
    attend(0, 1)
    recv(d1o)
    sib1o_far = group(W1.at[0, 0, 0])
    share1(1, s2, sib1o_far)
    matmul_planes(1, c, s2, s2, 1)
    recv(sib1o_far)
    matmul_planes(1, cs, ss2, ss2, 1)
    post(1)
    halo_send(1)

    recv(sc_c, sk_c)
    attend(1, 1)
    halo_relay(1)
    recv(f_pm)
    sib_pm = group(ST3)
    send(PM.at[1, half], PM.at[1, half], dev_sib, sib_pm, OTHER_SENT + 4)
    recv(c2a)
    u0, d0 = half_plane(sd, 0), half_plane(su, 1)
    d2 = [group(W2.at[0, 0, pl.ds(0, 2)]) for _ in range(2)]
    for k in range(2):
        send2(u0.at[k], dev_su, d2[k])
        send2(d0.at[k], dev_sd, d2[k])
    sib2_a = group(W2.at[0, 0])
    send2(u0, dev_sib, sib2_a)
    send2(d0, dev_sib, sib2_a)
    halo_wait(0)
    attend(0, 0)
    pool(0, x)
    halo_wait(1)
    attend(1, 0)
    recv(sib_pm)
    pool(1, x2)

    def unit(u, cc, s_, fs):
        rhs = []
        for g in range(2):
            rhs.append(jnp.concatenate([W2[cc, s_, fs[0], g], W2[cc, s_, fs[1], g]], axis=1))
        o = jnp.dot(MIX[0], rhs[0], preferred_element_type=F32)
        o += jnp.dot(MIX[1], rhs[1], preferred_element_type=F32)
        ob = o.astype(BF16)
        for e in range(2):
            idx = 2 * u + e
            OWNB[idx] = ob[0:256, e * 128 : (e + 1) * 128]
            SENDB[idx] = ob[256:512, e * 128 : (e + 1) * 128]
            pltpu.make_async_remote_copy(
                src_ref=SENDB.at[idx], dst_ref=RECVB.at[idx], send_sem=osend, recv_sem=orecv.at[u],
                device_id=dev_p, device_id_type=MESH,
            ).start()

    def total(u, cc, s_, fs):
        wait(RECVB.at[pl.ds(2 * u, 2)], orecv.at[u])
        for e in range(2):
            idx = 2 * u + e
            col = pl.ds(pl.multiple_of(sp_of(cc, fs[e], s_) * 128, 128), 128)
            OWNB[idx] = (OWNB[idx].astype(F32) + RECVB[idx].astype(F32)).astype(BF16)
            pltpu.make_async_copy(OWNB.at[idx], out.at[:, col], oloc).start()

    def pair(stage, mine, sA, kA, sB, kB, act=unit):
        cc = c if mine else cs

        def body(t, carry):
            k = kA + t * (kB - kA)
            act(stage * 4 + (0 if mine else 2) + t, cc, sA + t * (sB - sA), (2 * k, 2 * k + 1))
            return carry

        lax.fori_loop(0, 2, body, 0)

    def far_unit(u, cc, s_, k, act):
        def body(t, carry):
            act(u, cc, s_, (t, 2 + t))
            return carry

        lax.fori_loop(k, k + 1, body, 0)

    pair(0, True, s, 0, s, 1)
    recv(sib2_own)
    pair(0, False, ss_, 0, ss_, 1)
    pair(1, True, sd, 0, su, 1)
    recv(c2b)
    sib2_b = group(W2.at[0, 0])
    send2(half_plane(sd, 1), dev_sib, sib2_b)
    send2(half_plane(su, 0), dev_sib, sib2_b)
    recv(sib2_a)
    pair(1, False, ssd, 0, ssu, 1)
    pair(2, True, sd, 1, su, 0)
    pair(0, True, s, 0, s, 1, total)
    pair(0, False, ss_, 0, ss_, 1, total)
    recv(sib2_b)
    pair(2, False, ssd, 1, ssu, 0)

    for k in range(2):
        recv(d2[k])
        sib2_c = group(W2.at[0, 0, pl.ds(0, 2)])
        send2(W2.at[c, s2, k], dev_sib, sib2_c)
        send2(W2.at[c, s2, 2 + k], dev_sib, sib2_c)
        far_unit(12 + 2 * k, c, s2, k, unit)
        recv(sib2_c)
        far_unit(13 + 2 * k, cs, ss2, k, unit)
        if k == 0:
            pair(1, True, sd, 0, su, 1, total)
            pair(1, False, ssd, 0, ssu, 1, total)
            pair(2, True, sd, 1, su, 0, total)
            pair(2, False, ssd, 1, ssu, 0, total)

    wait(W1, ssem.at[W1_SENT])
    wait(W2, ssem.at[W2_SENT])
    wait(TOK.at[0], ssem.at[TOK_SENT])
    for k, whole in enumerate((SCALE, SINK, ST3, ST3, ST3)):
        wait(whole, ssem.at[OTHER_SENT + k])
    for gi in range(2):
        halo_sent(gi)
        relay_sent(gi)
    wait(SENDB, osend)
    for k in range(2):
        far_unit(12 + 2 * k, c, s2, k, total)
        far_unit(13 + 2 * k, cs, ss2, k, total)
    wait(OWNB, oloc)
    assert len(groups) == N_GROUPS, len(groups)


def local_program(
    tokens, norm_gain, w_pool_in, w_query, w_key, w_value, pool_map, pool_scale,
    q_gain, k_gain, sinks, w_out,
):
    any_ = pl.BlockSpec(memory_space=pl.ANY)
    vmem = pl.BlockSpec(memory_space=pltpu.VMEM)
    dma = pltpu.SemaphoreType.DMA
    return pl.pallas_call(
        kernel,
        out_shape=jax.ShapeDtypeStruct((256, 4096), BF16),
        in_specs=[any_] * 7 + [vmem] * 5,
        out_specs=any_,
        scratch_shapes=[
            pltpu.VMEM((2, 2, 4, 4, 128, 1152), BF16),
            pltpu.VMEM((2, 4, 4, 2, 1024, 128), BF16),
            pltpu.VMEM((2, 4, 256, 1024), BF16),
            pltpu.VMEM((128, 1152), BF16),
            pltpu.VMEM((1024, 128), BF16),
            pltpu.VMEM((256, 512), BF16),
            pltpu.VMEM((2, 512, 512), BF16),
            pltpu.VMEM((1, 512), F32),
            pltpu.VMEM((1, 8), F32),
            pltpu.VMEM((128, 128), BF16),
            pltpu.VMEM((2, 2, 384, 128), BF16),
            pltpu.VMEM((2, 2, 272, 512), BF16),
            pltpu.VMEM((2, 512, 512), BF16),
            pltpu.VMEM((512, 1152), F32),
            pltpu.VMEM((2, 256, 128), F32),
            pltpu.VMEM((2, 512, 1024), BF16),
            pltpu.VMEM((2, 512, 512), F32),
            pltpu.VMEM((512, 512), BF16),
            pltpu.VMEM((32, 256, 128), BF16),
            pltpu.VMEM((32, 256, 128), BF16),
            pltpu.VMEM((32, 256, 128), BF16),
            pltpu.VMEM((2, 128, 128), BF16),
            pltpu.VMEM((2, 16, 512), BF16),
            dma((8,)),
            dma((9,)),
            dma((N_GROUPS,)),
            dma(()),
            dma((16,)),
            dma(()),
            dma((2, 2, 2)),
            dma((2, 2, 2)),
            dma((2, 2)),
            dma((2, 2)),
        ],
        compiler_params=pltpu.CompilerParams(
            collective_id=0, has_side_effects=True, vmem_limit_bytes=66_000_000
        ),
        name="mixer",
    )(
        tokens, w_pool_in, w_query, w_key.T, w_value.T, w_out, pool_map.reshape(512, 512),
        pool_scale.reshape(1, 512), sinks.reshape(1, 8), q_gain.reshape(1, 64),
        k_gain.reshape(1, 64), norm_gain.reshape(1, 4096),
    )


def solution(mesh):
    in_specs = (
        P("sp", "tp"), P(), P("sp", "tp"), P("sp", "tp"), P("sp", "tp"), P("sp", "tp"),
        P("tp", None, None), P("tp"), P(), P(), P("tp"), P("tp", "sp"),
    )
    out_specs = P(("sp", "tp"), None)
    return jax.shard_map(local_program, mesh=mesh, in_specs=in_specs, out_specs=out_specs, check_vma=False)
```

```python
import jax
import jax.numpy as jnp
from jax import lax
from jax.experimental import pallas as pl
from jax.experimental.pallas import tpu as pltpu
from jax.sharding import PartitionSpec as P

MESH = pl.DeviceIdType.MESH
F32 = jnp.float32
BF16 = jnp.bfloat16
EPS = 1e-6
N_GROUPS = 41


def mod4(v):
    return lax.rem(v, 4)


def kernel(
    tokens, wp, wq, wk_t, wv_t, wo, pmap, scale_in, sinks_in, q_gain, k_gain, gain,
    out,
    W1, W2, TOK, ST1, ST2, ST3, PM, SCALE, SINK, KVT, KV, PB, QB, ACC, SS, MIX, BIAS, BLK, SENDB, OWNB, RECVB, RLK, RLP,
    lsem, ssem, rsem, osend, orecv, oloc, hsend, hrecv, rlsend, rlrecv,
):
    sp = lax.axis_index("sp")
    x = lax.axis_index("tp")
    c = lax.rem(sp, 2)
    y = mod4(lax.div(sp, 2))
    z = lax.div(sp, 8)
    f = y + c * (z - y)
    s = z + c * (y - z)
    par = lax.rem(x, 2)
    flip1 = x + 1 - 2 * par
    flip3 = 3 - x
    p = (1 - c) * flip1 + c * flip3
    n = (1 - c) * flip3 + c * flip1
    x2 = mod4(x + 2)
    dx = mod4(x + 1 + 2 * c)

    def sp_of(c_, f_, s_):
        y_ = (1 - c_) * f_ + c_ * s_
        z_ = (1 - c_) * s_ + c_ * f_
        return (z_ * 4 + y_) * 2 + c_

    fu, fd = mod4(f + 1), mod4(f + 3)
    su, sd, s2 = mod4(s + 1), mod4(s + 3), mod4(s + 2)
    dev_fu, dev_fd = (sp_of(c, fu, s), x), (sp_of(c, fd, s), x)
    dev_su, dev_sd = (sp_of(c, f, su), x), (sp_of(c, f, sd), x)
    dev_sib = (sp + 1 - 2 * c, x)
    dev_dx, dev_p, dev_n, dev_x2 = (sp, dx), (sp, p), (sp, n), (sp, x2)
    cs, ss_, sf_ = 1 - c, f, s
    ssu, ssd, ss2 = mod4(ss_ + 1), mod4(ss_ + 3), mod4(ss_ + 2)

    groups = []
    W1_SENT, W2_SENT, TOK_SENT, TF_SENT, OTHER_SENT = range(5)

    def group(whole):
        groups.append(whole)
        return len(groups) - 1

    def send(src, dst, dev, to, sent):
        pltpu.make_async_remote_copy(
            src_ref=src, dst_ref=dst, send_sem=ssem.at[sent], recv_sem=rsem.at[to],
            device_id=dev, device_id_type=MESH,
        ).start()

    def wait(whole, sem):
        pltpu.make_async_copy(whole, whole, sem).wait()

    def recv(*gs):
        for g in gs:
            wait(groups[g], rsem.at[g])

    loc = []

    def local(src, dst):
        d = pltpu.make_async_copy(src, dst, lsem.at[len(loc)])
        d.start()
        loc.append(d)
        return d

    own1 = W1.at[0, c, s, f]
    l0 = local(wp, own1.at[:, pl.ds(0, 512)])
    l1 = local(wq, own1.at[:, pl.ds(512, 512)])
    l2 = local(wk_t, KVT.at[pl.ds(0, 64)])
    l7 = local(wv_t, KVT.at[pl.ds(64, 64)])
    l3 = local(wo, W2.at[c, s, f, 0])
    l4 = local(tokens.at[pl.ds(x * 256, 256)], TOK.at[0, x])
    l5 = local(tokens.at[pl.ds(p * 256, 256)], TOK.at[1, x])
    l6 = local(pmap, PM.at[0])

    def holder(q, c_):
        inner = lax.rem(lax.div(q + 1, 2), 2)
        even = lax.div(q, 2) * 2 + par
        odd = inner * (2 - par) + (1 - inner) * 3 * par
        return (1 - c_) * even + c_ * odd

    quarters = (x, p)

    def halo_to(i):
        q = quarters[i]
        qn = mod4(q + 1)
        spn = sp + lax.div(q + 1, 4)
        xn = holder(qn, lax.rem(spn, 2))
        here = (spn == sp) & (xn == x)
        away = jnp.logical_not(here) & (spn < 32)
        passed = away & (c == 1) & (q == 3)
        return qn, jnp.where(spn < 32, spn, 0), xn, here, away & jnp.logical_not(passed), passed

    def halo_from(i):
        q = quarters[i]
        first = (sp == 0) & (q == 0)
        back = jnp.where(q == 0, 1, 0)
        relayed = (back == 1) & (c == 0)
        spp = jnp.where(first, sp, sp - back - jnp.where(relayed, 1, 0))
        xp = holder(mod4(q + 3), lax.rem(sp - back + 2, 2))
        here = (back == 0) & (xp == x)
        return first, jnp.logical_not(first) & jnp.logical_not(here), spp, xp

    relay = (c == 0) & ((x == 0) | (x == 3)) & (sp < 30)
    relay_dev = (jnp.where(relay, sp + 2, 0), par)
    relay_slot = jnp.where(par == 0, 0, 1)

    barrier = pltpu.get_barrier_semaphore()

    def greet(dev):
        pl.semaphore_signal(barrier, inc=1, device_id=dev, device_id_type=MESH)

    for dev in (dev_fu, dev_fd, dev_su, dev_sd, dev_sib, dev_p, dev_n, dev_x2):
        greet(dev)
    @pl.when(relay)
    def _():
        greet(relay_dev)

    for i in range(2):
        _, spn, xn, _, away, _ = halo_to(i)

        @pl.when(away)
        def _():
            greet((spn, xn))

        _, apart, spp, xp = halo_from(i)

        @pl.when(apart)
        def _():
            greet((spp, xp))

    lane_i = lax.broadcasted_iota(jnp.int32, (512, 512), 1)
    row_i = lax.broadcasted_iota(jnp.int32, (512, 512), 0)
    l2.wait()
    l7.wait()
    W1[0, c, s, f, :, pl.ds(1024, 128)] = KVT[...].astype(F32).T.astype(BF16)
    BLK[...] = jnp.where(
        lax.shift_right_logical(lane_i, 6) == lax.shift_right_logical(row_i, 6), 1.0, 0.0
    ).astype(BF16)
    SS[...] = jnp.zeros_like(SS)
    key_i = jnp.bitwise_and(lane_i, 255)
    dist = 128 + jnp.bitwise_and(row_i, 127) - key_i
    band = (dist >= 0) & (dist < 128)
    head_in = 2 * lax.shift_right_logical(row_i, 7) + lax.shift_right_logical(lane_i, 8) + 1
    for gi, g in ((0, x), (1, x2)):
        slope = jnp.exp2(-0.25 * (g * 8 + head_in).astype(F32))
        BIAS[gi] = jnp.where(band, -slope * dist.astype(F32), -1e30)

    peers = 8 + jnp.where(relay, 1, 0)
    for i in range(2):
        peers += jnp.where(halo_to(i)[4], 1, 0) + jnp.where(halo_from(i)[1], 1, 0)
    pl.semaphore_wait(barrier, peers)

    l0.wait()
    l1.wait()
    l3.wait()
    shard1, shard2 = W1.at[0, 0, 0, 0], W2.at[0, 0, 0]

    def send1(piece, dev, to):
        send(piece, piece, dev, to, W1_SENT)

    def send2(piece, dev, to):
        send(piece, piece, dev, to, W2_SENT)

    def step_a1(g):
        piece = W1.at[g, c, s, f]
        to = group(shard1), group(shard1)
        for k in range(2):
            send1(piece.at[pl.ds(64 * k, 64)], dev_fu, to[k])
            send1(piece.at[pl.ds(64 - 64 * k, 64)], dev_fd, to[k])
        return to

    def step_b1(g, a):
        recv(a[0])
        to = group(shard1)
        send1(W1.at[g, c, s, fd, pl.ds(0, 64)], dev_fu, to)
        send1(W1.at[g, c, s, fu, pl.ds(64, 64)], dev_fd, to)
        return to

    def step_c1(g, a, b, shared):
        recv(a[1], b)
        plane = W1.at[g, c, s]
        to = group(W1.at[0, 0, 0]), group(W1.at[0, 0, 0])
        for k in range(2):
            send1(plane.at[pl.ds(2 * k, 2)], dev_su, to[k])
            send1(plane.at[pl.ds(2 - 2 * k, 2)], dev_sd, to[k])
        send1(plane, dev_sib, shared)
        return to

    def step_d1(g, cc):
        recv(cc[0])
        to = group(W1.at[0, 0, 0])
        send1(W1.at[g, c, sd, pl.ds(0, 2)], dev_su, to)
        send1(W1.at[g, c, su, pl.ds(2, 2)], dev_sd, to)
        return to

    def share1(g, s_, to):
        send1(W1.at[g, c, s_], dev_sib, to)

    def step_a2(g):
        to = group(shard2)
        for dev in (dev_fu, dev_fd):
            send2(W2.at[c, s, f, g], dev, to)
        return to

    def step_b2(g, a):
        recv(a)
        to = group(shard2.at[0])
        send2(W2.at[c, s, fd, g, pl.ds(0, 512)], dev_fu, to)
        send2(W2.at[c, s, fu, g, pl.ds(512, 512)], dev_fd, to)
        return to

    x_w1 = [group(shard1.at[pl.ds(0, 64)]) for _ in range(2)]
    for k in range(2):
        part = pl.ds(64 * k, 64)
        send(own1.at[part], ST1.at[part], dev_dx, x_w1[k], W1_SENT)
    a1 = step_a1(0)
    a2 = step_a2(0)
    f_w1 = group(shard1)
    for k in range(2):
        recv(x_w1[k])
        part = pl.ds(64 * k, 64)
        send(ST1.at[part], W1.at[1, c, s, f, part], dev_dx, f_w1, W1_SENT)
        if k == 0:
            b1 = step_b1(0, a1)
    two_slabs = TOK.at[0, pl.ds(0, 2)]
    tn = group(two_slabs)
    send(tokens.at[pl.ds(n * 256, 256)], TOK.at[0, x], dev_n, tn, TOK_SENT)
    send(tokens.at[pl.ds(x2 * 256, 256)], TOK.at[1, x], dev_n, tn, TOK_SENT)
    sc_c, sk_c = group(SCALE), group(SINK)
    send(scale_in, SCALE, dev_x2, sc_c, OTHER_SENT)
    send(sinks_in, SINK, dev_x2, sk_c, OTHER_SENT + 1)

    b2 = step_b2(0, a2)
    sib1 = group(W1.at[0, 0])
    c1a, c1b = step_c1(0, a1, b1, sib1)
    recv(f_w1)
    a1o = step_a1(1)

    def scale_slab(j):
        g = gain[:, pl.ds(pl.multiple_of(j * 1024, 1024), 1024)]

        def body(k, carry):
            slot, r = lax.div(k, 4), pl.ds(lax.rem(k, 4) * 64, 64)
            t = TOK[slot, j, r, :].astype(F32)
            sq = t * t
            tot = sq[:, 0:128]
            for m in range(1, 8):
                tot += sq[:, m * 128 : (m + 1) * 128]
            SS[slot, r, :] += tot
            TOK[slot, j, r, :] = (t * g).astype(BF16)
            return carry

        lax.fori_loop(0, 8, body, 0)

    l4.wait()
    l5.wait()
    scale_slab(x)
    b1o = step_b1(1, a1o)
    tp_ = group(two_slabs)
    send(tokens.at[pl.ds(p * 256, 256)], TOK.at[0, x], dev_p, tp_, TOK_SENT)
    send(tokens.at[pl.ds(x * 256, 256)], TOK.at[1, x], dev_p, tp_, TOK_SENT)
    recv(tn)
    tf = group(two_slabs)
    send(TOK.at[0, n], TOK.at[1, n], dev_p, tf, TF_SENT)
    send(TOK.at[1, n], TOK.at[0, n], dev_p, tf, TF_SENT)
    d1 = step_d1(0, (c1a, c1b))
    sib1o = group(W1.at[0, 0, pl.ds(0, 3)])
    c1o = step_c1(1, a1o, b1o, sib1o)
    recv(c1b)
    share1(0, sd, sib1)
    share1(0, su, sib1)

    def half_plane(s_, k):
        return W2.at[c, s_, pl.ds(2 * k, 2)]

    def c2_send(g):
        to = c2a, c2b
        for k in range(2):
            send2(W2.at[c, s, pl.ds(2 * k, 2), g], dev_su, to[k])
            send2(W2.at[c, s, pl.ds(2 - 2 * k, 2), g], dev_sd, to[k])

    def matmul(lhs, rhs, first):
        o = jnp.dot(lhs, rhs, preferred_element_type=F32)
        if first:
            ACC[...] = o
        else:
            ACC[...] += o

    def matmul_slab(gi, jz, first=False):
        def body(t, carry):
            parts = []
            for yy in range(4):
                parts.append(W1[gi, 0, jz, yy])
                parts.append(W1[gi, 1, yy, jz])
            matmul(TOK[:, jz].reshape(512, 1024), jnp.concatenate(parts, axis=0), first)
            return carry

        lax.fori_loop(0, 1, body, 0)

    def matmul_planes(gi, cc, planes, first=False):
        def body(t, carry):
            lhs, rhs = [], []
            for s_ in planes:
                for k in range(4):
                    rhs.append(W1[gi, cc, s_, k])
                    off = ((1 - cc) * k + cc * s_) * 256 + cc * 128
                    col = pl.ds(pl.multiple_of(off, 128), 128)
                    lhs.append(TOK[:, (1 - cc) * s_ + cc * k, :, col].reshape(512, 128))
            matmul(jnp.concatenate(lhs, axis=1), jnp.concatenate(rhs, axis=0), first)
            return carry

        lax.fori_loop(0, 1, body, 0)

    def post(gi):
        def body(k, carry):
            slot, r = lax.div(k, 2), lax.rem(k, 2)
            rows = pl.ds(pl.multiple_of(k * 128, 128), 128)
            tot = jnp.sum(SS[slot, pl.ds(r * 128, 128), :], axis=-1, keepdims=True)
            a = ACC[rows, :] * lax.rsqrt(tot * (1.0 / 4096) + EPS)
            PB[gi, slot, pl.ds(pl.multiple_of(16 + r * 128, 16), 128), :] = a[:, 0:512].astype(BF16)
            qf = a[:, 512:1024].astype(BF16).astype(F32)
            sq = qf * qf
            hi = sq.astype(BF16)
            lo = (sq - hi.astype(F32)).astype(BF16)
            ssq = jnp.dot(hi, BLK[...], preferred_element_type=F32) + jnp.dot(
                lo, BLK[...], preferred_element_type=F32
            )
            qg = jnp.concatenate([q_gain[...]] * 8, axis=1) * 0.125
            QB[gi, rows, :] = (qf * lax.rsqrt(ssq * (1.0 / 64) + EPS) * qg).astype(BF16)
            kv = a[:, 1024:1152].astype(BF16).astype(F32)
            is_key = lax.broadcasted_iota(jnp.int32, (128, 128), 1) < 64
            ksq = jnp.sum(jnp.where(is_key, kv * kv, 0.0), axis=-1, keepdims=True)
            kn = kv * lax.rsqrt(ksq * (1.0 / 64) + EPS) * jnp.concatenate([k_gain[...]] * 2, axis=1)
            KV[gi, slot, pl.ds(pl.multiple_of(128 + r * 128, 128), 128), :] = jnp.where(
                is_key, kn, kv
            ).astype(BF16)
            return carry

        lax.fori_loop(0, 4, body, 0)

    def halo_next(gi, i):
        qn, spn, xn, here, away, passed = halo_to(i)
        slot = jnp.where(xn == qn, 0, 1)
        gn = jnp.where(xn == x, gi, 1 - gi)
        tails = (KV.at[gi, i, pl.ds(256, 128)], PB.at[gi, i, pl.ds(256, 16)])
        copies = [
            pltpu.make_async_remote_copy(
                src_ref=src, dst_ref=dst, send_sem=hsend.at[gi, i, k], recv_sem=hrecv.at[gn, slot, k],
                device_id=(spn, xn), device_id_type=MESH,
            )
            for k, (src, dst) in enumerate(
                zip(tails, (KV.at[gn, slot, pl.ds(0, 128)], PB.at[gn, slot, pl.ds(0, 16)]))
            )
        ]
        passes = [
            pltpu.make_async_remote_copy(
                src_ref=src, dst_ref=dst, send_sem=hsend.at[gi, i, k], recv_sem=rlrecv.at[gi, k],
                device_id=dev_sib, device_id_type=MESH,
            )
            for k, (src, dst) in enumerate(zip(tails, (RLK.at[gi], RLP.at[gi])))
        ]
        return here, away, copies, passed, passes

    def halo_send(gi):
        for i in range(2):
            here, away, copies, passed, passes = halo_next(gi, i)

            @pl.when(passed)
            def _():
                for d in passes:
                    d.start()

            @pl.when(away)
            def _():
                for d in copies:
                    d.start()

            @pl.when(here)
            def _():
                KV[gi, 1 - i, pl.ds(0, 128), :] = KV[gi, i, pl.ds(256, 128), :]
                PB[gi, 1 - i, pl.ds(0, 16), :] = PB[gi, i, pl.ds(256, 16), :]

    def halo_sent(gi):
        for i in range(2):
            _, away, copies, passed, passes = halo_next(gi, i)

            @pl.when(passed)
            def _():
                for d in passes:
                    d.wait_send()

            @pl.when(away)
            def _():
                for d in copies:
                    d.wait_send()

    def relay_copies(gi):
        gn = jnp.where(par == x, gi, 1 - gi)
        return [
            pltpu.make_async_remote_copy(
                src_ref=src, dst_ref=dst, send_sem=rlsend.at[gi, k],
                recv_sem=hrecv.at[gn, relay_slot, k], device_id=relay_dev, device_id_type=MESH,
            )
            for k, (src, dst) in enumerate(
                (
                    (RLK.at[gi], KV.at[gn, relay_slot, pl.ds(0, 128)]),
                    (RLP.at[gi], PB.at[gn, relay_slot, pl.ds(0, 16)]),
                )
            )
        ]

    def halo_relay(gi):
        @pl.when(relay)
        def _():
            for k, dst in enumerate((RLK.at[gi], RLP.at[gi])):
                pltpu.make_async_copy(dst, dst, rlrecv.at[gi, k]).wait()
            for d in relay_copies(gi):
                d.start()

    def relay_sent(gi):
        @pl.when(relay)
        def _():
            for d in relay_copies(gi):
                d.wait_send()

    def halo_wait(gi):
        for i in range(2):
            first, apart, _, _ = halo_from(i)

            @pl.when(first)
            def _():
                KV[gi, i, pl.ds(0, 128), :] = jnp.zeros((128, 128), BF16)
                PB[gi, i, pl.ds(0, 16), :] = jnp.zeros((16, 512), BF16)

            @pl.when(apart)
            def _():
                for k, dst in enumerate((KV.at[gi, i, pl.ds(0, 128)], PB.at[gi, i, pl.ds(0, 16)])):
                    pltpu.make_async_copy(dst, dst, hrecv.at[gi, i, k]).wait()

    def pool(gi, g):
        span = lax.shift_left(jnp.int32(2), g)
        for i in range(2):
            pf = PB[gi, i].astype(F32)
            t2 = pf + pltpu.roll(pf, 1, 0)
            t4 = t2 + pltpu.roll(t2, 2, 0)
            t8 = t4 + pltpu.roll(t4, 4, 0)
            t16 = t8 + pltpu.roll(t8, 8, 0)
            run = jnp.where(g == 0, t2, jnp.where(g == 1, t4, jnp.where(g == 2, t8, t16)))[16:]
            pos = sp * 1024 + quarters[i] * 256 + lax.broadcasted_iota(jnp.int32, (256, 1), 0)
            count = jnp.minimum(pos + 1, span).astype(F32)
            diff = (run * (1.0 / count) - pf[16:]).astype(BF16)
            m = jnp.dot(diff, PM[gi], preferred_element_type=F32)
            m = m * (scale_in if gi == 0 else SCALE)[...]
            m = m * lax.rsqrt(jnp.mean(m * m, axis=-1, keepdims=True) + EPS)
            MIX[gi, i * 256 : (i + 1) * 256, 0:512] = m.astype(BF16)

    def attend(gi, r):
        sink = jnp.exp((sinks_in if gi == 0 else SINK)[...])
        left = lax.broadcasted_iota(jnp.int32, (1, 128), 1) < 64
        es = jnp.concatenate(
            [
                jnp.broadcast_to(
                    jnp.where(left, sink[:, 2 * j : 2 * j + 1], sink[:, 2 * j + 1 : 2 * j + 2]),
                    (128, 128),
                )
                for j in range(4)
            ],
            axis=0,
        )

        def body(k, carry):
            slot = k
            rows = pl.ds(pl.multiple_of(k * 256 + r * 128, 128), 128)
            kv = KV[gi, slot, pl.ds(r * 128, 256), :].astype(F32)
            low = lax.broadcasted_iota(jnp.int32, (256, 128), 1) < 64
            ke = jnp.where(low, kv, 0.0)
            vo = jnp.where(low, 0.0, kv)
            ko = pltpu.roll(ke, 64, 1)
            ve = pltpu.roll(vo, 64, 1)
            q_here = (1 - slot) * x + slot * p
            missing = jnp.where((sp == 0) & (q_here == 0), 128, 0) if r == 0 else 0
            there = lax.broadcasted_iota(jnp.int32, (256, 128), 0) >= missing
            oe = jnp.where(low & there, 1.0, 0.0)
            oo = jnp.where(jnp.logical_not(low) & there, 1.0, 0.0)
            keys = jnp.concatenate([ke, ko], axis=0).astype(BF16)
            values = jnp.concatenate(
                [jnp.concatenate([ve, oe], axis=1), jnp.concatenate([vo, oo], axis=1)], axis=0
            ).astype(BF16)
            q = QB[gi, rows, :]
            q = jnp.concatenate([q[:, j * 128 : (j + 1) * 128] for j in range(4)], axis=0)
            sc = lax.dot_general(q, keys, (((1,), (1,)), ((), ())), preferred_element_type=F32)
            e = jnp.exp(sc + BIAS[gi]).astype(BF16)
            o = jnp.dot(e, values, preferred_element_type=F32)
            att = o[:, 0:128] / (o[:, 128:256] + es)
            parts = [att[j * 128 : (j + 1) * 128] for j in range(4)]
            sq = parts[0] * parts[0]
            for j in range(1, 4):
                sq += parts[j] * parts[j]
            r_ = lax.rsqrt(jnp.sum(sq, axis=-1, keepdims=True) * (1.0 / 512) + EPS)
            for j in range(4):
                MIX[gi, rows, 512 + j * 128 : 640 + j * 128] = (parts[j] * r_).astype(BF16)
            return carry

        lax.fori_loop(0, 2, body, 0)

    recv(d1)
    share1(0, s2, sib1)
    recv(sib1)
    matmul_slab(0, x, True)
    recv(tp_)
    scale_slab(p)
    matmul_slab(0, p)
    d1o = step_d1(1, c1o)
    c2a, c2b = group(W2.at[0, 0]), group(W2.at[0, 0])
    recv(b2)
    c2_send(0)
    x_w2 = group(shard2.at[0])
    send(W2.at[c, s, f, 0], ST2, dev_dx, x_w2, W2_SENT)
    l6.wait()
    half = pl.ds(c * 256, 256)
    x_pm = group(ST3)
    send(PM.at[0, half], ST3, dev_dx, x_pm, OTHER_SENT + 2)
    wait(two_slabs, ssem.at[TF_SENT])
    scale_slab(n)
    matmul_slab(0, n)
    recv(tf)
    scale_slab(x2)
    matmul_slab(0, x2)
    post(0)
    halo_send(0)
    recv(c1o[1])
    share1(1, sd, sib1o)
    share1(1, su, sib1o)
    recv(x_w2)
    f_w2 = group(shard2.at[0])
    send(ST2, W2.at[c, s, f, 1], dev_dx, f_w2, W2_SENT)
    matmul_planes(1, c, (s, sd, su), True)
    recv(sib1o)
    recv(f_w2)
    a2o = step_a2(1)
    recv(x_pm)
    f_pm = group(ST3)
    send(ST3, PM.at[1, half], dev_dx, f_pm, OTHER_SENT + 3)
    matmul_planes(1, cs, (ss_, ssd, ssu))
    halo_relay(0)
    attend(0, 1)
    recv(d1o)
    sib1o_far = group(W1.at[0, 0, 0])
    share1(1, s2, sib1o_far)
    matmul_planes(1, c, (s2,))
    recv(sib1o_far)
    matmul_planes(1, cs, (ss2,))
    b2o = step_b2(1, a2o)
    post(1)
    halo_send(1)

    recv(sc_c, sk_c)
    attend(1, 1)
    halo_relay(1)
    recv(f_pm)
    sib_pm = group(ST3)
    send(PM.at[1, half], PM.at[1, half], dev_sib, sib_pm, OTHER_SENT + 4)
    recv(b2o)
    c2_send(1)
    sib2_own = group(W2.at[0, 0])
    send2(W2.at[c, s], dev_sib, sib2_own)
    halo_wait(0)
    attend(0, 0)
    pool(0, x)
    halo_wait(1)
    attend(1, 0)
    recv(sib_pm)
    pool(1, x2)

    def unit(u, cc, s_, fs):
        rhs = []
        for g in range(2):
            rhs.append(jnp.concatenate([W2[cc, s_, fs[0], g], W2[cc, s_, fs[1], g]], axis=1))
        o = jnp.dot(MIX[0], rhs[0], preferred_element_type=F32)
        o += jnp.dot(MIX[1], rhs[1], preferred_element_type=F32)
        ob = o.astype(BF16)
        for e in range(2):
            idx = 2 * u + e
            OWNB[idx] = ob[0:256, e * 128 : (e + 1) * 128]
            SENDB[idx] = ob[256:512, e * 128 : (e + 1) * 128]
            pltpu.make_async_remote_copy(
                src_ref=SENDB.at[idx], dst_ref=RECVB.at[idx], send_sem=osend, recv_sem=orecv.at[u],
                device_id=dev_p, device_id_type=MESH,
            ).start()

    def total(u, cc, s_, fs):
        wait(RECVB.at[pl.ds(2 * u, 2)], orecv.at[u])
        for e in range(2):
            idx = 2 * u + e
            col = pl.ds(pl.multiple_of(sp_of(cc, fs[e], s_) * 128, 128), 128)
            OWNB[idx] = (OWNB[idx].astype(F32) + RECVB[idx].astype(F32)).astype(BF16)
            pltpu.make_async_copy(OWNB.at[idx], out.at[:, col], oloc).start()

    def pair(stage, mine, sA, kA, sB, kB, act=unit):
        cc = c if mine else cs

        def body(t, carry):
            k = kA + t * (kB - kA)
            act(stage * 4 + (0 if mine else 2) + t, cc, sA + t * (sB - sA), (2 * k, 2 * k + 1))
            return carry

        lax.fori_loop(0, 2, body, 0)

    def far_unit(u, cc, s_, k, act):
        def body(t, carry):
            act(u, cc, s_, (t, 2 + t))
            return carry

        lax.fori_loop(k, k + 1, body, 0)

    pair(0, True, s, 0, s, 1)
    recv(sib2_own)
    pair(0, False, ss_, 0, ss_, 1)
    recv(c2a)
    u0, d0 = half_plane(sd, 0), half_plane(su, 1)
    d2 = [group(W2.at[0, 0, pl.ds(0, 2)]) for _ in range(2)]
    for k in range(2):
        send2(u0.at[k], dev_su, d2[k])
        send2(d0.at[k], dev_sd, d2[k])
    sib2_a = group(W2.at[0, 0])
    send2(u0, dev_sib, sib2_a)
    send2(d0, dev_sib, sib2_a)
    pair(1, True, sd, 0, su, 1)
    recv(sib2_a)
    pair(1, False, ssd, 0, ssu, 1)
    recv(c2b)
    sib2_b = group(W2.at[0, 0])
    send2(half_plane(sd, 1), dev_sib, sib2_b)
    send2(half_plane(su, 0), dev_sib, sib2_b)
    pair(2, True, sd, 1, su, 0)
    pair(0, True, s, 0, s, 1, total)
    pair(0, False, ss_, 0, ss_, 1, total)
    recv(sib2_b)
    pair(2, False, ssd, 1, ssu, 0)

    for k in range(2):
        recv(d2[k])
        sib2_c = group(W2.at[0, 0, pl.ds(0, 2)])
        send2(W2.at[c, s2, k], dev_sib, sib2_c)
        send2(W2.at[c, s2, 2 + k], dev_sib, sib2_c)
        far_unit(12 + 2 * k, c, s2, k, unit)
        recv(sib2_c)
        far_unit(13 + 2 * k, cs, ss2, k, unit)
        if k == 0:
            pair(1, True, sd, 0, su, 1, total)
            pair(1, False, ssd, 0, ssu, 1, total)

    wait(W1, ssem.at[W1_SENT])
    wait(W2, ssem.at[W2_SENT])
    wait(TOK.at[0], ssem.at[TOK_SENT])
    for k, whole in enumerate((SCALE, SINK, ST3, ST3, ST3)):
        wait(whole, ssem.at[OTHER_SENT + k])
    for gi in range(2):
        halo_sent(gi)
        relay_sent(gi)
    wait(SENDB, osend)
    pair(2, True, sd, 1, su, 0, total)
    pair(2, False, ssd, 1, ssu, 0, total)
    for k in range(2):
        far_unit(12 + 2 * k, c, s2, k, total)
        far_unit(13 + 2 * k, cs, ss2, k, total)
    wait(OWNB, oloc)
    assert len(groups) == N_GROUPS, len(groups)


def local_program(
    tokens, norm_gain, w_pool_in, w_query, w_key, w_value, pool_map, pool_scale,
    q_gain, k_gain, sinks, w_out,
):
    any_ = pl.BlockSpec(memory_space=pl.ANY)
    vmem = pl.BlockSpec(memory_space=pltpu.VMEM)
    dma = pltpu.SemaphoreType.DMA
    return pl.pallas_call(
        kernel,
        out_shape=jax.ShapeDtypeStruct((256, 4096), BF16),
        in_specs=[any_] * 7 + [vmem] * 5,
        out_specs=any_,
        scratch_shapes=[
            pltpu.VMEM((2, 2, 4, 4, 128, 1152), BF16),
            pltpu.VMEM((2, 4, 4, 2, 1024, 128), BF16),
            pltpu.VMEM((2, 4, 256, 1024), BF16),
            pltpu.VMEM((128, 1152), BF16),
            pltpu.VMEM((1024, 128), BF16),
            pltpu.VMEM((256, 512), BF16),
            pltpu.VMEM((2, 512, 512), BF16),
            pltpu.VMEM((1, 512), F32),
            pltpu.VMEM((1, 8), F32),
            pltpu.VMEM((128, 128), BF16),
            pltpu.VMEM((2, 2, 384, 128), BF16),
            pltpu.VMEM((2, 2, 272, 512), BF16),
            pltpu.VMEM((2, 512, 512), BF16),
            pltpu.VMEM((512, 1152), F32),
            pltpu.VMEM((2, 256, 128), F32),
            pltpu.VMEM((2, 512, 1024), BF16),
            pltpu.VMEM((2, 512, 512), F32),
            pltpu.VMEM((512, 512), BF16),
            pltpu.VMEM((32, 256, 128), BF16),
            pltpu.VMEM((32, 256, 128), BF16),
            pltpu.VMEM((32, 256, 128), BF16),
            pltpu.VMEM((2, 128, 128), BF16),
            pltpu.VMEM((2, 16, 512), BF16),
            dma((8,)),
            dma((9,)),
            dma((N_GROUPS,)),
            dma(()),
            dma((16,)),
            dma(()),
            dma((2, 2, 2)),
            dma((2, 2, 2)),
            dma((2, 2)),
            dma((2, 2)),
        ],
        compiler_params=pltpu.CompilerParams(
            collective_id=0, has_side_effects=True, vmem_limit_bytes=66_000_000
        ),
        name="mixer",
    )(
        tokens, w_pool_in, w_query, w_key.T, w_value.T, w_out, pool_map.reshape(512, 512),
        pool_scale.reshape(1, 512), sinks.reshape(1, 8), q_gain.reshape(1, 64),
        k_gain.reshape(1, 64), norm_gain.reshape(1, 4096),
    )


def solution(mesh):
    in_specs = (
        P("sp", "tp"), P(), P("sp", "tp"), P("sp", "tp"), P("sp", "tp"), P("sp", "tp"),
        P("tp", None, None), P("tp"), P(), P(), P("tp"), P("tp", "sp"),
    )
    out_specs = P(("sp", "tp"), None)
    return jax.shard_map(local_program, mesh=mesh, in_specs=in_specs, out_specs=out_specs, check_vma=False)
```

```python
import jax
import jax.numpy as jnp
from jax import lax
from jax.experimental import pallas as pl
from jax.experimental.pallas import tpu as pltpu
from jax.sharding import PartitionSpec as P

MESH = pl.DeviceIdType.MESH
F32 = jnp.float32
BF16 = jnp.bfloat16
EPS = 1e-6
N_GROUPS = 43
PIECES = 8


def mod4(v):
    return lax.rem(v, 4)


def kernel(
    tokens, wp, wq, wk_t, wv_t, wo, pmap, scale_in, sinks_in, q_in, k_in, gain_in,
    out,
    W1, W2, TOK, ST1, ST2, ST3, PM, SCALE, SINK, q_gain, k_gain, gain, KVT, KV, PB, QB, ACC, SS, MIX, BIAS, BLK, SENDB, OWNB, RECVB, RLK, RLP,
    lsem, ssem, rsem, osend, orecv, oloc, hsend, hrecv, rlsend, rlrecv,
):
    sp = lax.axis_index("sp")
    x = lax.axis_index("tp")
    c = lax.rem(sp, 2)
    y = mod4(lax.div(sp, 2))
    z = lax.div(sp, 8)
    f = y + c * (z - y)
    s = z + c * (y - z)
    par = lax.rem(x, 2)
    flip1 = x + 1 - 2 * par
    flip3 = 3 - x
    p = (1 - c) * flip1 + c * flip3
    n = (1 - c) * flip3 + c * flip1
    x2 = mod4(x + 2)
    dx = mod4(x + 1 + 2 * c)

    def sp_of(c_, f_, s_):
        y_ = (1 - c_) * f_ + c_ * s_
        z_ = (1 - c_) * s_ + c_ * f_
        return (z_ * 4 + y_) * 2 + c_

    fu, fd = mod4(f + 1), mod4(f + 3)
    su, sd, s2 = mod4(s + 1), mod4(s + 3), mod4(s + 2)
    dev_fu, dev_fd = (sp_of(c, fu, s), x), (sp_of(c, fd, s), x)
    dev_su, dev_sd = (sp_of(c, f, su), x), (sp_of(c, f, sd), x)
    dev_sib = (sp + 1 - 2 * c, x)
    dev_dx, dev_p, dev_n, dev_x2 = (sp, dx), (sp, p), (sp, n), (sp, x2)
    cs, ss_, sf_ = 1 - c, f, s
    ssu, ssd, ss2 = mod4(ss_ + 1), mod4(ss_ + 3), mod4(ss_ + 2)

    groups = []
    W1_SENT, W2_SENT, TOK_SENT, TF_SENT, OTHER_SENT = range(5)

    def group(whole):
        groups.append(whole)
        return len(groups) - 1

    def send(src, dst, dev, to, sent):
        pltpu.make_async_remote_copy(
            src_ref=src, dst_ref=dst, send_sem=ssem.at[sent], recv_sem=rsem.at[to],
            device_id=dev, device_id_type=MESH,
        ).start()

    def wait(whole, sem):
        pltpu.make_async_copy(whole, whole, sem).wait()

    def recv(*gs):
        for g in gs:
            wait(groups[g], rsem.at[g])

    def holder(q, c_):
        inner = lax.rem(lax.div(q + 1, 2), 2)
        even = lax.div(q, 2) * 2 + par
        odd = inner * (2 - par) + (1 - inner) * 3 * par
        return (1 - c_) * even + c_ * odd

    quarters = (x, p)

    def halo_to(i):
        q = quarters[i]
        qn = mod4(q + 1)
        spn = sp + lax.div(q + 1, 4)
        xn = holder(qn, lax.rem(spn, 2))
        here = (spn == sp) & (xn == x)
        away = jnp.logical_not(here) & (spn < 32)
        passed = away & (c == 1) & (q == 3)
        return qn, jnp.where(spn < 32, spn, 0), xn, here, away & jnp.logical_not(passed), passed

    def halo_from(i):
        q = quarters[i]
        first = (sp == 0) & (q == 0)
        back = jnp.where(q == 0, 1, 0)
        relayed = (back == 1) & (c == 0)
        spp = jnp.where(first, sp, sp - back - jnp.where(relayed, 1, 0))
        xp = holder(mod4(q + 3), lax.rem(sp - back + 2, 2))
        here = (back == 0) & (xp == x)
        return first, jnp.logical_not(first) & jnp.logical_not(here), spp, xp

    relay = (c == 0) & ((x == 0) | (x == 3)) & (sp < 30)
    relay_dev = (jnp.where(relay, sp + 2, 0), par)
    relay_slot = jnp.where(par == 0, 0, 1)

    barrier = pltpu.get_barrier_semaphore()

    def greet(dev):
        pl.semaphore_signal(barrier, inc=1, device_id=dev, device_id_type=MESH)

    for dev in (dev_fu, dev_fd, dev_su, dev_sd, dev_sib, dev_p, dev_n, dev_x2):
        greet(dev)
    @pl.when(relay)
    def _():
        greet(relay_dev)

    for i in range(2):
        _, spn, xn, _, away, _ = halo_to(i)

        @pl.when(away)
        def _():
            greet((spn, xn))

        _, apart, spp, xp = halo_from(i)

        @pl.when(apart)
        def _():
            greet((spp, xp))

    loc = []

    def local(src, dst):
        d = pltpu.make_async_copy(src, dst, lsem.at[len(loc)])
        d.start()
        loc.append(d)
        return d

    own1 = W1.at[0, c, s, f]
    l0 = local(wp, own1.at[:, pl.ds(0, 512)])
    l1 = local(wq, own1.at[:, pl.ds(512, 512)])
    l2 = local(wk_t, KVT.at[pl.ds(0, 64)])
    l7 = local(wv_t, KVT.at[pl.ds(64, 64)])
    l3 = local(wo, W2.at[c, s, f, 0])
    l4 = local(tokens.at[pl.ds(x * 256, 256)], TOK.at[0, x])
    l5 = local(tokens.at[pl.ds(p * 256, 256)], TOK.at[1, x])
    l6 = local(pmap, PM.at[0])
    small = [
        local(src, dst)
        for src, dst in (
            (scale_in, SCALE.at[0]), (sinks_in, SINK.at[0]), (q_in, q_gain), (k_in, k_gain), (gain_in, gain),
        )
    ]

    lane_i = lax.broadcasted_iota(jnp.int32, (512, 512), 1)
    row_i = lax.broadcasted_iota(jnp.int32, (512, 512), 0)
    l2.wait()
    l7.wait()
    W1[0, c, s, f, :, pl.ds(1024, 128)] = KVT[...].astype(F32).T.astype(BF16)
    BLK[...] = jnp.where(
        lax.shift_right_logical(lane_i, 6) == lax.shift_right_logical(row_i, 6), 1.0, 0.0
    ).astype(BF16)
    SS[...] = jnp.zeros_like(SS)
    peers = 8 + jnp.where(relay, 1, 0)
    for i in range(2):
        peers += jnp.where(halo_to(i)[4], 1, 0) + jnp.where(halo_from(i)[1], 1, 0)
    pl.semaphore_wait(barrier, peers)

    l0.wait()
    l1.wait()
    l3.wait()
    shard1, shard2 = W1.at[0, 0, 0, 0], W2.at[0, 0, 0]

    def send1(piece, dev, to):
        send(piece, piece, dev, to, W1_SENT)

    def send2(piece, dev, to):
        send(piece, piece, dev, to, W2_SENT)

    def step_a1(g):
        piece = W1.at[g, c, s, f]
        to = group(shard1), group(shard1)
        for k in range(2):
            send1(piece.at[pl.ds(64 * k, 64)], dev_fu, to[k])
            send1(piece.at[pl.ds(64 - 64 * k, 64)], dev_fd, to[k])
        return to

    def step_b1(g, a):
        recv(a[0])
        to = group(shard1)
        send1(W1.at[g, c, s, fd, pl.ds(0, 64)], dev_fu, to)
        send1(W1.at[g, c, s, fu, pl.ds(64, 64)], dev_fd, to)
        return to

    def step_c1(g, a, b, shared):
        recv(a[1], b)
        plane = W1.at[g, c, s]
        to = group(W1.at[0, 0, 0]), group(W1.at[0, 0, 0])
        for k in range(2):
            send1(plane.at[pl.ds(2 * k, 2)], dev_su, to[k])
            send1(plane.at[pl.ds(2 - 2 * k, 2)], dev_sd, to[k])
        send1(plane, dev_sib, shared)
        return to

    def step_d1(g, cc):
        recv(cc[0])
        to = group(W1.at[0, 0, 0])
        send1(W1.at[g, c, sd, pl.ds(0, 2)], dev_su, to)
        send1(W1.at[g, c, su, pl.ds(2, 2)], dev_sd, to)
        return to

    def share1(g, s_, to):
        send1(W1.at[g, c, s_], dev_sib, to)

    def step_a2(g):
        to = group(shard2)
        for dev in (dev_fu, dev_fd):
            send2(W2.at[c, s, f, g], dev, to)
        return to

    def step_b2(g, a):
        recv(a)
        to = group(shard2.at[0])
        send2(W2.at[c, s, fd, g, pl.ds(0, 512)], dev_fu, to)
        send2(W2.at[c, s, fu, g, pl.ds(512, 512)], dev_fd, to)
        return to

    x_w1 = [group(shard1.at[pl.ds(0, 64)]) for _ in range(2)]
    for k in range(2):
        part = pl.ds(64 * k, 64)
        send(own1.at[part], ST1.at[part], dev_dx, x_w1[k], W1_SENT)
    a1 = step_a1(0)
    a2 = step_a2(0)
    key_i = jnp.bitwise_and(lane_i, 255)
    dist = 128 + jnp.bitwise_and(row_i, 127) - key_i
    band = (dist >= 0) & (dist < 128)
    head_in = 2 * lax.shift_right_logical(row_i, 7) + lax.shift_right_logical(lane_i, 8) + 1
    for gi, g in ((0, x), (1, x2)):
        slope = jnp.exp2(-0.25 * (g * 8 + head_in).astype(F32))
        BIAS[gi] = jnp.where(band, -slope * dist.astype(F32), -1e30)

    f_w1 = group(shard1)
    for k in range(2):
        recv(x_w1[k])
        part = pl.ds(64 * k, 64)
        send(ST1.at[part], W1.at[1, c, s, f, part], dev_dx, f_w1, W1_SENT)
        if k == 0:
            b1 = step_b1(0, a1)
    two_slabs = TOK.at[0, pl.ds(0, 2)]
    tn = group(two_slabs)
    send(tokens.at[pl.ds(n * 256, 256)], TOK.at[0, x], dev_n, tn, TOK_SENT)
    send(tokens.at[pl.ds(x2 * 256, 256)], TOK.at[1, x], dev_n, tn, TOK_SENT)
    sc_c, sk_c = group(SCALE.at[1]), group(SINK.at[1])
    send(scale_in, SCALE.at[1], dev_x2, sc_c, OTHER_SENT)
    send(sinks_in, SINK.at[1], dev_x2, sk_c, OTHER_SENT + 1)

    b2 = step_b2(0, a2)
    sib1 = group(W1.at[0, 0])
    c1a, c1b = step_c1(0, a1, b1, sib1)
    recv(f_w1)
    a1o = step_a1(1)

    def scale_slab(j):
        g = gain[:, pl.ds(pl.multiple_of(j * 1024, 1024), 1024)]

        def body(k, carry):
            slot, r = lax.div(k, 4), pl.ds(lax.rem(k, 4) * 64, 64)
            t = TOK[slot, j, r, :].astype(F32)
            sq = t * t
            tot = sq[:, 0:128]
            for m in range(1, 8):
                tot += sq[:, m * 128 : (m + 1) * 128]
            SS[slot, r, :] += tot
            TOK[slot, j, r, :] = (t * g).astype(BF16)
            return carry

        lax.fori_loop(0, 8, body, 0)

    for d in (l4, l5, *small):
        d.wait()
    scale_slab(x)
    b1o = step_b1(1, a1o)
    tp_ = group(two_slabs)
    send(tokens.at[pl.ds(p * 256, 256)], TOK.at[0, x], dev_p, tp_, TOK_SENT)
    send(tokens.at[pl.ds(x * 256, 256)], TOK.at[1, x], dev_p, tp_, TOK_SENT)
    recv(tn)
    tf = group(two_slabs)
    send(TOK.at[0, n], TOK.at[1, n], dev_p, tf, TF_SENT)
    send(TOK.at[1, n], TOK.at[0, n], dev_p, tf, TF_SENT)
    d1 = step_d1(0, (c1a, c1b))
    sib1o = group(W1.at[0, 0, pl.ds(0, 3)])
    c1o = step_c1(1, a1o, b1o, sib1o)
    recv(c1b)
    share1(0, sd, sib1)
    share1(0, su, sib1)

    def half_plane(s_, k):
        return W2.at[c, s_, pl.ds(2 * k, 2)]

    def c2_send(g):
        to = c2a, c2b
        for k in range(2):
            send2(W2.at[c, s, pl.ds(2 * k, 2), g], dev_su, to[k])
            send2(W2.at[c, s, pl.ds(2 - 2 * k, 2), g], dev_sd, to[k])

    def matmul(lhs, rhs, first):
        o = jnp.dot(lhs, rhs, preferred_element_type=F32)
        if first:
            ACC[...] = o
        else:
            ACC[...] += o

    def matmul_slab(gi, jz, first=False):
        def body(t, carry):
            parts = []
            for yy in range(4):
                parts.append(W1[gi, 0, jz, yy])
                parts.append(W1[gi, 1, yy, jz])
            matmul(TOK[:, jz].reshape(512, 1024), jnp.concatenate(parts, axis=0), first)
            return carry

        lax.fori_loop(0, 1, body, 0)

    def matmul_planes(gi, cc, planes, first=False):
        def body(t, carry):
            lhs, rhs = [], []
            for s_ in planes:
                for k in range(4):
                    rhs.append(W1[gi, cc, s_, k])
                    off = ((1 - cc) * k + cc * s_) * 256 + cc * 128
                    col = pl.ds(pl.multiple_of(off, 128), 128)
                    lhs.append(TOK[:, (1 - cc) * s_ + cc * k, :, col].reshape(512, 128))
            matmul(jnp.concatenate(lhs, axis=1), jnp.concatenate(rhs, axis=0), first)
            return carry

        lax.fori_loop(0, 1, body, 0)

    def post(gi):
        def body(k, carry):
            slot, r = lax.div(k, 2), lax.rem(k, 2)
            rows = pl.ds(pl.multiple_of(k * 128, 128), 128)
            tot = jnp.sum(SS[slot, pl.ds(r * 128, 128), :], axis=-1, keepdims=True)
            a = ACC[rows, :] * lax.rsqrt(tot * (1.0 / 4096) + EPS)
            PB[gi, slot, pl.ds(pl.multiple_of(16 + r * 128, 16), 128), :] = a[:, 0:512].astype(BF16)
            qf = a[:, 512:1024].astype(BF16).astype(F32)
            sq = qf * qf
            hi = sq.astype(BF16)
            lo = (sq - hi.astype(F32)).astype(BF16)
            ssq = jnp.dot(hi, BLK[...], preferred_element_type=F32) + jnp.dot(
                lo, BLK[...], preferred_element_type=F32
            )
            qg = jnp.concatenate([q_gain[...]] * 8, axis=1) * 0.125
            QB[gi, rows, :] = (qf * lax.rsqrt(ssq * (1.0 / 64) + EPS) * qg).astype(BF16)
            kv = a[:, 1024:1152].astype(BF16).astype(F32)
            is_key = lax.broadcasted_iota(jnp.int32, (128, 128), 1) < 64
            ksq = jnp.sum(jnp.where(is_key, kv * kv, 0.0), axis=-1, keepdims=True)
            kn = kv * lax.rsqrt(ksq * (1.0 / 64) + EPS) * jnp.concatenate([k_gain[...]] * 2, axis=1)
            KV[gi, slot, pl.ds(pl.multiple_of(128 + r * 128, 128), 128), :] = jnp.where(
                is_key, kn, kv
            ).astype(BF16)
            return carry

        lax.fori_loop(0, 4, body, 0)

    def halo_next(gi, i):
        qn, spn, xn, here, away, passed = halo_to(i)
        slot = jnp.where(xn == qn, 0, 1)
        gn = jnp.where(xn == x, gi, 1 - gi)
        tails = (KV.at[gi, i, pl.ds(256, 128)], PB.at[gi, i, pl.ds(256, 16)])
        copies = [
            pltpu.make_async_remote_copy(
                src_ref=src, dst_ref=dst, send_sem=hsend.at[gi, i, k], recv_sem=hrecv.at[gn, slot, k],
                device_id=(spn, xn), device_id_type=MESH,
            )
            for k, (src, dst) in enumerate(
                zip(tails, (KV.at[gn, slot, pl.ds(0, 128)], PB.at[gn, slot, pl.ds(0, 16)]))
            )
        ]
        passes = [
            pltpu.make_async_remote_copy(
                src_ref=src, dst_ref=dst, send_sem=hsend.at[gi, i, k], recv_sem=rlrecv.at[gi, k],
                device_id=dev_sib, device_id_type=MESH,
            )
            for k, (src, dst) in enumerate(zip(tails, (RLK.at[gi], RLP.at[gi])))
        ]
        return here, away, copies, passed, passes

    def halo_send(gi):
        for i in range(2):
            here, away, copies, passed, passes = halo_next(gi, i)

            @pl.when(passed)
            def _():
                for d in passes:
                    d.start()

            @pl.when(away)
            def _():
                for d in copies:
                    d.start()

            @pl.when(here)
            def _():
                KV[gi, 1 - i, pl.ds(0, 128), :] = KV[gi, i, pl.ds(256, 128), :]
                PB[gi, 1 - i, pl.ds(0, 16), :] = PB[gi, i, pl.ds(256, 16), :]

    def halo_sent(gi):
        for i in range(2):
            _, away, copies, passed, passes = halo_next(gi, i)

            @pl.when(passed)
            def _():
                for d in passes:
                    d.wait_send()

            @pl.when(away)
            def _():
                for d in copies:
                    d.wait_send()

    def relay_copies(gi):
        gn = jnp.where(par == x, gi, 1 - gi)
        return [
            pltpu.make_async_remote_copy(
                src_ref=src, dst_ref=dst, send_sem=rlsend.at[gi, k],
                recv_sem=hrecv.at[gn, relay_slot, k], device_id=relay_dev, device_id_type=MESH,
            )
            for k, (src, dst) in enumerate(
                (
                    (RLK.at[gi], KV.at[gn, relay_slot, pl.ds(0, 128)]),
                    (RLP.at[gi], PB.at[gn, relay_slot, pl.ds(0, 16)]),
                )
            )
        ]

    def halo_relay(gi):
        @pl.when(relay)
        def _():
            for k, dst in enumerate((RLK.at[gi], RLP.at[gi])):
                pltpu.make_async_copy(dst, dst, rlrecv.at[gi, k]).wait()
            for d in relay_copies(gi):
                d.start()

    def relay_sent(gi):
        @pl.when(relay)
        def _():
            for d in relay_copies(gi):
                d.wait_send()

    def halo_wait(gi):
        for i in range(2):
            first, apart, _, _ = halo_from(i)

            @pl.when(first)
            def _():
                KV[gi, i, pl.ds(0, 128), :] = jnp.zeros((128, 128), BF16)
                PB[gi, i, pl.ds(0, 16), :] = jnp.zeros((16, 512), BF16)

            @pl.when(apart)
            def _():
                for k, dst in enumerate((KV.at[gi, i, pl.ds(0, 128)], PB.at[gi, i, pl.ds(0, 16)])):
                    pltpu.make_async_copy(dst, dst, hrecv.at[gi, i, k]).wait()

    def pool(gi, g):
        span = lax.shift_left(jnp.int32(2), g)
        for i in range(2):
            pf = PB[gi, i].astype(F32)
            t2 = pf + pltpu.roll(pf, 1, 0)
            t4 = t2 + pltpu.roll(t2, 2, 0)
            t8 = t4 + pltpu.roll(t4, 4, 0)
            t16 = t8 + pltpu.roll(t8, 8, 0)
            run = jnp.where(g == 0, t2, jnp.where(g == 1, t4, jnp.where(g == 2, t8, t16)))[16:]
            pos = sp * 1024 + quarters[i] * 256 + lax.broadcasted_iota(jnp.int32, (256, 1), 0)
            count = jnp.minimum(pos + 1, span).astype(F32)
            diff = (run * (1.0 / count) - pf[16:]).astype(BF16)
            m = jnp.dot(diff, PM[gi], preferred_element_type=F32)
            m = m * SCALE[gi]
            m = m * lax.rsqrt(jnp.mean(m * m, axis=-1, keepdims=True) + EPS)
            MIX[gi, i * 256 : (i + 1) * 256, 0:512] = m.astype(BF16)

    def attend(gi, r):
        sink = jnp.exp(SINK[gi])
        left = lax.broadcasted_iota(jnp.int32, (1, 128), 1) < 64
        es = jnp.concatenate(
            [
                jnp.broadcast_to(
                    jnp.where(left, sink[:, 2 * j : 2 * j + 1], sink[:, 2 * j + 1 : 2 * j + 2]),
                    (128, 128),
                )
                for j in range(4)
            ],
            axis=0,
        )

        def body(k, carry):
            slot = k
            rows = pl.ds(pl.multiple_of(k * 256 + r * 128, 128), 128)
            kv = KV[gi, slot, pl.ds(r * 128, 256), :].astype(F32)
            low = lax.broadcasted_iota(jnp.int32, (256, 128), 1) < 64
            ke = jnp.where(low, kv, 0.0)
            vo = jnp.where(low, 0.0, kv)
            ko = pltpu.roll(ke, 64, 1)
            ve = pltpu.roll(vo, 64, 1)
            q_here = (1 - slot) * x + slot * p
            missing = jnp.where((sp == 0) & (q_here == 0), 128, 0) if r == 0 else 0
            there = lax.broadcasted_iota(jnp.int32, (256, 128), 0) >= missing
            oe = jnp.where(low & there, 1.0, 0.0)
            oo = jnp.where(jnp.logical_not(low) & there, 1.0, 0.0)
            keys = jnp.concatenate([ke, ko], axis=0).astype(BF16)
            values = jnp.concatenate(
                [jnp.concatenate([ve, oe], axis=1), jnp.concatenate([vo, oo], axis=1)], axis=0
            ).astype(BF16)
            q = QB[gi, rows, :]
            q = jnp.concatenate([q[:, j * 128 : (j + 1) * 128] for j in range(4)], axis=0)
            sc = lax.dot_general(q, keys, (((1,), (1,)), ((), ())), preferred_element_type=F32)
            e = jnp.exp(sc + BIAS[gi]).astype(BF16)
            o = jnp.dot(e, values, preferred_element_type=F32)
            att = o[:, 0:128] / (o[:, 128:256] + es)
            parts = [att[j * 128 : (j + 1) * 128] for j in range(4)]
            sq = parts[0] * parts[0]
            for j in range(1, 4):
                sq += parts[j] * parts[j]
            r_ = lax.rsqrt(jnp.sum(sq, axis=-1, keepdims=True) * (1.0 / 512) + EPS)
            for j in range(4):
                MIX[gi, rows, 512 + j * 128 : 640 + j * 128] = (parts[j] * r_).astype(BF16)
            return carry

        lax.fori_loop(0, 2, body, 0)

    recv(d1)
    share1(0, s2, sib1)
    recv(sib1)
    matmul_slab(0, x, True)
    recv(tp_)
    scale_slab(p)
    matmul_slab(0, p)
    d1o = step_d1(1, c1o)
    c2a, c2b = group(W2.at[0, 0]), group(W2.at[0, 0])
    recv(b2)
    c2_send(0)
    x_w2 = group(shard2.at[0])
    send(W2.at[c, s, f, 0], ST2, dev_dx, x_w2, W2_SENT)
    l6.wait()
    half = pl.ds(c * 256, 256)
    x_pm = group(ST3)
    send(PM.at[0, half], ST3, dev_dx, x_pm, OTHER_SENT + 2)
    wait(two_slabs, ssem.at[TF_SENT])
    scale_slab(n)
    matmul_slab(0, n)
    recv(tf)
    scale_slab(x2)
    matmul_slab(0, x2)
    post(0)
    halo_send(0)
    recv(c1o[1])
    share1(1, sd, sib1o)
    share1(1, su, sib1o)
    recv(x_w2)
    f_w2 = group(shard2.at[0])
    send(ST2, W2.at[c, s, f, 1], dev_dx, f_w2, W2_SENT)
    matmul_planes(1, c, (s, sd, su), True)
    recv(sib1o)
    recv(f_w2)
    a2o = step_a2(1)
    recv(x_pm)
    f_pm = group(ST3)
    send(ST3, PM.at[1, half], dev_dx, f_pm, OTHER_SENT + 3)
    matmul_planes(1, cs, (ss_, ssd, ssu))
    halo_relay(0)
    attend(0, 1)
    recv(d1o)
    sib1o_far = group(W1.at[0, 0, 0])
    share1(1, s2, sib1o_far)
    matmul_planes(1, c, (s2,))
    recv(sib1o_far)
    matmul_planes(1, cs, (ss2,))
    b2o = step_b2(1, a2o)
    post(1)
    halo_send(1)

    recv(sc_c, sk_c)
    attend(1, 1)
    halo_relay(1)
    recv(f_pm)
    sib_pm = group(ST3)
    send(PM.at[1, half], PM.at[1, half], dev_sib, sib_pm, OTHER_SENT + 4)
    recv(b2o)
    c2_send(1)
    sib2_own = group(W2.at[0, 0])
    send2(W2.at[c, s], dev_sib, sib2_own)
    halo_wait(0)
    attend(0, 0)
    pool(0, x)
    halo_wait(1)
    attend(1, 0)
    recv(sib_pm)
    pool(1, x2)

    def product(cc, s_, fs, g):
        rhs = jnp.concatenate([W2[cc, s_, fs[0], g], W2[cc, s_, fs[1], g]], axis=1)
        return jnp.dot(MIX[g], rhs, preferred_element_type=F32)

    def unit(u, cc, s_, fs):
        leave(u, product(cc, s_, fs, 0) + product(cc, s_, fs, 1))

    def part_unit(u, cc, s_, fs):
        ACC[:, (u - 14) * 256 : (u - 13) * 256] = product(cc, s_, fs, 0)

    def last_unit(u, cc, s_, fs):
        leave(u, ACC[:, (u - 14) * 256 : (u - 13) * 256] + product(cc, s_, fs, 1))

    def leave(u, o):
        ob = o.astype(BF16)
        for e in range(2):
            idx = 2 * u + e
            OWNB[idx] = ob[0:256, e * 128 : (e + 1) * 128]
            SENDB[idx] = ob[256:512, e * 128 : (e + 1) * 128]
            pltpu.make_async_remote_copy(
                src_ref=SENDB.at[idx], dst_ref=RECVB.at[idx], send_sem=osend, recv_sem=orecv.at[u],
                device_id=dev_p, device_id_type=MESH,
            ).start()

    def total(u, cc, s_, fs):
        wait(RECVB.at[pl.ds(2 * u, 2)], orecv.at[u])
        for e in range(2):
            idx = 2 * u + e
            col = pl.ds(pl.multiple_of(sp_of(cc, fs[e], s_) * 128, 128), 128)
            OWNB[idx] = (OWNB[idx].astype(F32) + RECVB[idx].astype(F32)).astype(BF16)
            pltpu.make_async_copy(OWNB.at[idx], out.at[:, col], oloc).start()

    def pair(stage, mine, sA, kA, sB, kB, act=unit):
        cc = c if mine else cs

        def body(t, carry):
            k = kA + t * (kB - kA)
            act(stage * 4 + (0 if mine else 2) + t, cc, sA + t * (sB - sA), (2 * k, 2 * k + 1))
            return carry

        lax.fori_loop(0, 2, body, 0)

    def far_unit(u, cc, s_, k, act):
        def body(t, carry):
            act(u, cc, s_, (t, 2 + t))
            return carry

        lax.fori_loop(k, k + 1, body, 0)

    pair(0, True, s, 0, s, 1)
    recv(sib2_own)
    pair(0, False, ss_, 0, ss_, 1)
    recv(c2a)
    u0, d0 = half_plane(sd, 0), half_plane(su, 1)
    d2 = [group(W2.at[0, 0, pl.ds(0, 2)]), group(shard2), group(shard2)]
    send2(u0.at[0], dev_su, d2[0])
    send2(d0.at[0], dev_sd, d2[0])
    for g in range(2):
        send2(u0.at[1, g], dev_su, d2[1 + g])
        send2(d0.at[1, g], dev_sd, d2[1 + g])
    sib2_a = group(W2.at[0, 0])
    send2(u0, dev_sib, sib2_a)
    send2(d0, dev_sib, sib2_a)
    pair(1, True, sd, 0, su, 1)
    recv(sib2_a)
    pair(1, False, ssd, 0, ssu, 1)
    recv(c2b)
    sib2_b = group(W2.at[0, 0])
    send2(half_plane(sd, 1), dev_sib, sib2_b)
    send2(half_plane(su, 0), dev_sib, sib2_b)
    pair(2, True, sd, 1, su, 0)
    pair(0, True, s, 0, s, 1, total)
    pair(0, False, ss_, 0, ss_, 1, total)
    recv(sib2_b)
    pair(2, False, ssd, 1, ssu, 0)

    recv(d2[0])
    sib2_c = group(W2.at[0, 0, pl.ds(0, 2)])
    send2(W2.at[c, s2, 0], dev_sib, sib2_c)
    send2(W2.at[c, s2, 2], dev_sib, sib2_c)
    far_unit(12, c, s2, 0, unit)
    recv(sib2_c)
    far_unit(13, cs, ss2, 0, unit)
    pair(1, True, sd, 0, su, 1, total)
    pair(1, False, ssd, 0, ssu, 1, total)

    sib2_d = [group(shard2), group(shard2)]
    for g in range(2):
        recv(d2[1 + g])
        send2(W2.at[c, s2, 1, g], dev_sib, sib2_d[g])
        send2(W2.at[c, s2, 3, g], dev_sib, sib2_d[g])
        far_unit(14, c, s2, 1, (part_unit, last_unit)[g])
    for g in range(2):
        recv(sib2_d[g])
        far_unit(15, cs, ss2, 1, (part_unit, last_unit)[g])

    wait(W1, ssem.at[W1_SENT])
    wait(W2, ssem.at[W2_SENT])
    wait(TOK.at[0], ssem.at[TOK_SENT])
    for k, whole in enumerate((SCALE.at[1], SINK.at[1], ST3, ST3, ST3)):
        wait(whole, ssem.at[OTHER_SENT + k])
    for gi in range(2):
        halo_sent(gi)
        relay_sent(gi)
    wait(SENDB, osend)
    pair(2, True, sd, 1, su, 0, total)
    pair(2, False, ssd, 1, ssu, 0, total)
    for k in range(2):
        far_unit(12 + 2 * k, c, s2, k, total)
        far_unit(13 + 2 * k, cs, ss2, k, total)
    wait(OWNB, oloc)
    assert len(groups) == N_GROUPS, len(groups)


def hand_over(src, out, held, in_sem, out_sem):
    rows = 256 // PIECES
    parts = [pl.ds(k * rows, rows) for k in range(PIECES)]
    ins = [pltpu.make_async_copy(src.at[r], held.at[r], in_sem.at[k]) for k, r in enumerate(parts)]
    outs = [pltpu.make_async_copy(held.at[r], out.at[r], out_sem.at[k]) for k, r in enumerate(parts)]
    for d in ins:
        d.start()
    for d, o in zip(ins, outs):
        d.wait()
        o.start()
    for o in outs:
        o.wait()


def local_program(
    tokens, norm_gain, w_pool_in, w_query, w_key, w_value, pool_map, pool_scale,
    q_gain, k_gain, sinks, w_out,
):
    any_ = pl.BlockSpec(memory_space=pl.ANY)
    dma = pltpu.SemaphoreType.DMA
    summed = pl.pallas_call(
        kernel,
        out_shape=jax.ShapeDtypeStruct((256, 4096), BF16),
        in_specs=[any_] * 12,
        out_specs=any_,
        scratch_shapes=[
            pltpu.VMEM((2, 2, 4, 4, 128, 1152), BF16),
            pltpu.VMEM((2, 4, 4, 2, 1024, 128), BF16),
            pltpu.VMEM((2, 4, 256, 1024), BF16),
            pltpu.VMEM((128, 1152), BF16),
            pltpu.VMEM((1024, 128), BF16),
            pltpu.VMEM((256, 512), BF16),
            pltpu.VMEM((2, 512, 512), BF16),
            pltpu.VMEM((2, 1, 512), F32),
            pltpu.VMEM((2, 1, 8), F32),
            pltpu.VMEM((1, 64), F32),
            pltpu.VMEM((1, 64), F32),
            pltpu.VMEM((1, 4096), F32),
            pltpu.VMEM((128, 128), BF16),
            pltpu.VMEM((2, 2, 384, 128), BF16),
            pltpu.VMEM((2, 2, 272, 512), BF16),
            pltpu.VMEM((2, 512, 512), BF16),
            pltpu.VMEM((512, 1152), F32),
            pltpu.VMEM((2, 256, 128), F32),
            pltpu.VMEM((2, 512, 1024), BF16),
            pltpu.VMEM((2, 512, 512), F32),
            pltpu.VMEM((512, 512), BF16),
            pltpu.VMEM((32, 256, 128), BF16),
            pltpu.VMEM((32, 256, 128), BF16),
            pltpu.VMEM((32, 256, 128), BF16),
            pltpu.VMEM((2, 128, 128), BF16),
            pltpu.VMEM((2, 16, 512), BF16),
            dma((13,)),
            dma((9,)),
            dma((N_GROUPS,)),
            dma(()),
            dma((16,)),
            dma(()),
            dma((2, 2, 2)),
            dma((2, 2, 2)),
            dma((2, 2)),
            dma((2, 2)),
        ],
        compiler_params=pltpu.CompilerParams(
            collective_id=0, has_side_effects=True, vmem_limit_bytes=66_000_000
        ),
        name="mixer",
    )(
        tokens, w_pool_in, w_query, w_key.T, w_value.T, w_out, pool_map.reshape(512, 512),
        pool_scale.reshape(1, 512), sinks.reshape(1, 8), q_gain.reshape(1, 64),
        k_gain.reshape(1, 64), norm_gain.reshape(1, 4096),
    )
    return pl.pallas_call(
        hand_over,
        out_shape=jax.ShapeDtypeStruct((256, 4096), BF16),
        in_specs=[any_],
        out_specs=any_,
        scratch_shapes=[pltpu.VMEM((256, 4096), BF16), dma((PIECES,)), dma((PIECES,))],
        name="hand_over",
    )(summed)


def solution(mesh):
    in_specs = (
        P("sp", "tp"), P(), P("sp", "tp"), P("sp", "tp"), P("sp", "tp"), P("sp", "tp"),
        P("tp", None, None), P("tp"), P(), P(), P("tp"), P("tp", "sp"),
    )
    out_specs = P(("sp", "tp"), None)
    return jax.shard_map(local_program, mesh=mesh, in_specs=in_specs, out_specs=out_specs, check_vma=False)
```

```python
import jax
import jax.numpy as jnp
from jax import lax
from jax.experimental import pallas as pl
from jax.experimental.pallas import tpu as pltpu
from jax.sharding import PartitionSpec as P

MESH = pl.DeviceIdType.MESH
F32 = jnp.float32
BF16 = jnp.bfloat16
EPS = 1e-6
N_GROUPS = 45
PIECES = 8


def mod4(v):
    return lax.rem(v, 4)


def kernel(
    tokens, wp, wq, wk_t, wv_t, wo, pmap, scale_in, sinks_in, q_in, k_in, gain_in,
    out,
    W1, W2, TOK, ST1, ST2, ST3, PM, SCALE, SINK, q_gain, k_gain, gain, KVT, KV, PB, QB, ACC, SS, MIX, BIAS, BLK, SENDB, OWNB, RECVB, RLK, RLP,
    lsem, ssem, rsem, osend, orecv, oloc, hsend, hrecv, rlsend, rlrecv,
):
    sp = lax.axis_index("sp")
    x = lax.axis_index("tp")
    c = lax.rem(sp, 2)
    y = mod4(lax.div(sp, 2))
    z = lax.div(sp, 8)
    f = y + c * (z - y)
    s = z + c * (y - z)
    par = lax.rem(x, 2)
    flip1 = x + 1 - 2 * par
    flip3 = 3 - x
    p = (1 - c) * flip1 + c * flip3
    n = (1 - c) * flip3 + c * flip1
    x2 = mod4(x + 2)
    dx = mod4(x + 1 + 2 * c)

    def sp_of(c_, f_, s_):
        y_ = (1 - c_) * f_ + c_ * s_
        z_ = (1 - c_) * s_ + c_ * f_
        return (z_ * 4 + y_) * 2 + c_

    fu, fd = mod4(f + 1), mod4(f + 3)
    su, sd, s2 = mod4(s + 1), mod4(s + 3), mod4(s + 2)
    dev_fu, dev_fd = (sp_of(c, fu, s), x), (sp_of(c, fd, s), x)
    dev_su, dev_sd = (sp_of(c, f, su), x), (sp_of(c, f, sd), x)
    dev_sib = (sp + 1 - 2 * c, x)
    dev_dx, dev_p, dev_n, dev_x2 = (sp, dx), (sp, p), (sp, n), (sp, x2)
    cs, ss_, sf_ = 1 - c, f, s
    ssu, ssd, ss2 = mod4(ss_ + 1), mod4(ss_ + 3), mod4(ss_ + 2)

    groups = []
    W1_SENT, W2_SENT, TOK_SENT, TF_SENT, OTHER_SENT = range(5)

    def group(whole):
        groups.append(whole)
        return len(groups) - 1

    def send(src, dst, dev, to, sent):
        pltpu.make_async_remote_copy(
            src_ref=src, dst_ref=dst, send_sem=ssem.at[sent], recv_sem=rsem.at[to],
            device_id=dev, device_id_type=MESH,
        ).start()

    def wait(whole, sem):
        pltpu.make_async_copy(whole, whole, sem).wait()

    def recv(*gs):
        for g in gs:
            wait(groups[g], rsem.at[g])

    def holder(q, c_):
        inner = lax.rem(lax.div(q + 1, 2), 2)
        even = lax.div(q, 2) * 2 + par
        odd = inner * (2 - par) + (1 - inner) * 3 * par
        return (1 - c_) * even + c_ * odd

    quarters = (x, p)

    def halo_to(i):
        q = quarters[i]
        qn = mod4(q + 1)
        spn = sp + lax.div(q + 1, 4)
        xn = holder(qn, lax.rem(spn, 2))
        here = (spn == sp) & (xn == x)
        away = jnp.logical_not(here) & (spn < 32)
        passed = away & (c == 1) & (q == 3)
        return qn, jnp.where(spn < 32, spn, 0), xn, here, away & jnp.logical_not(passed), passed

    def halo_from(i):
        q = quarters[i]
        first = (sp == 0) & (q == 0)
        back = jnp.where(q == 0, 1, 0)
        relayed = (back == 1) & (c == 0)
        spp = jnp.where(first, sp, sp - back - jnp.where(relayed, 1, 0))
        xp = holder(mod4(q + 3), lax.rem(sp - back + 2, 2))
        here = (back == 0) & (xp == x)
        return first, jnp.logical_not(first) & jnp.logical_not(here), spp, xp

    relay = (c == 0) & ((x == 0) | (x == 3)) & (sp < 30)
    relay_dev = (jnp.where(relay, sp + 2, 0), par)
    relay_slot = jnp.where(par == 0, 0, 1)

    barrier = pltpu.get_barrier_semaphore()

    def greet(dev):
        pl.semaphore_signal(barrier, inc=1, device_id=dev, device_id_type=MESH)

    for dev in (dev_fu, dev_fd, dev_su, dev_sd, dev_sib, dev_p, dev_n, dev_x2):
        greet(dev)
    @pl.when(relay)
    def _():
        greet(relay_dev)

    for i in range(2):
        _, spn, xn, _, away, _ = halo_to(i)

        @pl.when(away)
        def _():
            greet((spn, xn))

        _, apart, spp, xp = halo_from(i)

        @pl.when(apart)
        def _():
            greet((spp, xp))

    loc = []

    def local(src, dst):
        d = pltpu.make_async_copy(src, dst, lsem.at[len(loc)])
        d.start()
        loc.append(d)
        return d

    own1 = W1.at[0, c, s, f]
    l0 = local(wp, own1.at[:, pl.ds(0, 512)])
    l1 = local(wq, own1.at[:, pl.ds(512, 512)])
    l2 = local(wk_t, KVT.at[pl.ds(0, 64)])
    l7 = local(wv_t, KVT.at[pl.ds(64, 64)])
    l3 = local(wo, W2.at[c, s, f, 0])
    l4 = local(tokens.at[pl.ds(x * 256, 256)], TOK.at[0, x])
    l5 = local(tokens.at[pl.ds(p * 256, 256)], TOK.at[1, x])
    l6 = local(pmap, PM.at[0])
    small = [
        local(src, dst)
        for src, dst in (
            (scale_in, SCALE.at[0]), (sinks_in, SINK.at[0]), (q_in, q_gain), (k_in, k_gain), (gain_in, gain),
        )
    ]

    lane_i = lax.broadcasted_iota(jnp.int32, (512, 512), 1)
    row_i = lax.broadcasted_iota(jnp.int32, (512, 512), 0)
    l2.wait()
    l7.wait()
    W1[0, c, s, f, :, pl.ds(1024, 128)] = KVT[...].astype(F32).T.astype(BF16)
    BLK[...] = jnp.where(
        lax.shift_right_logical(lane_i, 6) == lax.shift_right_logical(row_i, 6), 1.0, 0.0
    ).astype(BF16)
    SS[...] = jnp.zeros_like(SS)
    peers = 8 + jnp.where(relay, 1, 0)
    for i in range(2):
        peers += jnp.where(halo_to(i)[4], 1, 0) + jnp.where(halo_from(i)[1], 1, 0)
    pl.semaphore_wait(barrier, peers)

    l0.wait()
    l1.wait()
    l3.wait()
    shard1, shard2 = W1.at[0, 0, 0, 0], W2.at[0, 0, 0]

    def send1(piece, dev, to):
        send(piece, piece, dev, to, W1_SENT)

    def send2(piece, dev, to):
        send(piece, piece, dev, to, W2_SENT)

    def step_a1(g):
        piece = W1.at[g, c, s, f]
        to = group(shard1), group(shard1)
        for k in range(2):
            send1(piece.at[pl.ds(64 * k, 64)], dev_fu, to[k])
            send1(piece.at[pl.ds(64 - 64 * k, 64)], dev_fd, to[k])
        return to

    def step_b1(g, a):
        recv(a[0])
        to = group(shard1)
        send1(W1.at[g, c, s, fd, pl.ds(0, 64)], dev_fu, to)
        send1(W1.at[g, c, s, fu, pl.ds(64, 64)], dev_fd, to)
        return to

    def step_c1(g, a, b, shared):
        recv(a[1], b)
        plane = W1.at[g, c, s]
        to = group(W1.at[0, 0, 0]), group(W1.at[0, 0, 0])
        for k in range(2):
            send1(plane.at[pl.ds(2 * k, 2)], dev_su, to[k])
            send1(plane.at[pl.ds(2 - 2 * k, 2)], dev_sd, to[k])
        send1(plane, dev_sib, shared)
        return to

    def step_d1(g, cc):
        recv(cc[0])
        to = group(W1.at[0, 0, 0])
        send1(W1.at[g, c, sd, pl.ds(0, 2)], dev_su, to)
        send1(W1.at[g, c, su, pl.ds(2, 2)], dev_sd, to)
        return to

    def share1(g, s_, to):
        send1(W1.at[g, c, s_], dev_sib, to)

    def step_a2(g):
        to = group(shard2.at[0]), group(shard2.at[0])
        for k in range(2):
            send2(W2.at[c, s, f, g, pl.ds(512 * k, 512)], dev_fu, to[k])
            send2(W2.at[c, s, f, g, pl.ds(512 - 512 * k, 512)], dev_fd, to[k])
        return to

    def step_b2(g, a):
        recv(a[0])
        to = group(shard2.at[0])
        send2(W2.at[c, s, fd, g, pl.ds(0, 512)], dev_fu, to)
        send2(W2.at[c, s, fu, g, pl.ds(512, 512)], dev_fd, to)
        return to

    x_w1 = [group(shard1.at[pl.ds(0, 64)]) for _ in range(2)]
    for k in range(2):
        part = pl.ds(64 * k, 64)
        send(own1.at[part], ST1.at[part], dev_dx, x_w1[k], W1_SENT)
    a1 = step_a1(0)
    a2 = step_a2(0)
    key_i = jnp.bitwise_and(lane_i, 255)
    dist = 128 + jnp.bitwise_and(row_i, 127) - key_i
    band = (dist >= 0) & (dist < 128)
    head_in = 2 * lax.shift_right_logical(row_i, 7) + lax.shift_right_logical(lane_i, 8) + 1
    for gi, g in ((0, x), (1, x2)):
        slope = jnp.exp2(-0.25 * (g * 8 + head_in).astype(F32))
        BIAS[gi] = jnp.where(band, -slope * dist.astype(F32), -1e30)

    f_w1 = group(shard1)
    for k in range(2):
        recv(x_w1[k])
        part = pl.ds(64 * k, 64)
        send(ST1.at[part], W1.at[1, c, s, f, part], dev_dx, f_w1, W1_SENT)
        if k == 0:
            b1 = step_b1(0, a1)
    two_slabs = TOK.at[0, pl.ds(0, 2)]
    tn = group(two_slabs)
    send(tokens.at[pl.ds(n * 256, 256)], TOK.at[0, x], dev_n, tn, TOK_SENT)
    send(tokens.at[pl.ds(x2 * 256, 256)], TOK.at[1, x], dev_n, tn, TOK_SENT)
    sc_c, sk_c = group(SCALE.at[1]), group(SINK.at[1])
    send(scale_in, SCALE.at[1], dev_x2, sc_c, OTHER_SENT)
    send(sinks_in, SINK.at[1], dev_x2, sk_c, OTHER_SENT + 1)

    b2 = step_b2(0, a2)
    sib1 = group(W1.at[0, 0])
    c1a, c1b = step_c1(0, a1, b1, sib1)
    recv(f_w1)
    a1o = step_a1(1)

    def scale_slab(j):
        g = gain[:, pl.ds(pl.multiple_of(j * 1024, 1024), 1024)]

        def body(k, carry):
            slot, r = lax.div(k, 4), pl.ds(lax.rem(k, 4) * 64, 64)
            t = TOK[slot, j, r, :].astype(F32)
            sq = t * t
            tot = sq[:, 0:128]
            for m in range(1, 8):
                tot += sq[:, m * 128 : (m + 1) * 128]
            SS[slot, r, :] += tot
            TOK[slot, j, r, :] = (t * g).astype(BF16)
            return carry

        lax.fori_loop(0, 8, body, 0)

    for d in (l4, l5, *small):
        d.wait()
    scale_slab(x)
    b1o = step_b1(1, a1o)
    tp_ = group(two_slabs)
    send(tokens.at[pl.ds(p * 256, 256)], TOK.at[0, x], dev_p, tp_, TOK_SENT)
    send(tokens.at[pl.ds(x * 256, 256)], TOK.at[1, x], dev_p, tp_, TOK_SENT)
    recv(tn)
    tf = group(two_slabs)
    send(TOK.at[0, n], TOK.at[1, n], dev_p, tf, TF_SENT)
    send(TOK.at[1, n], TOK.at[0, n], dev_p, tf, TF_SENT)
    d1 = step_d1(0, (c1a, c1b))
    sib1o = group(W1.at[0, 0, pl.ds(0, 3)])
    c1o = step_c1(1, a1o, b1o, sib1o)
    recv(c1b)
    share1(0, sd, sib1)
    share1(0, su, sib1)

    def half_plane(s_, k):
        return W2.at[c, s_, pl.ds(2 * k, 2)]

    def c2_send(g):
        to = c2a, c2b
        for k in range(2):
            send2(W2.at[c, s, pl.ds(2 * k, 2), g], dev_su, to[k])
            send2(W2.at[c, s, pl.ds(2 - 2 * k, 2), g], dev_sd, to[k])

    def matmul(lhs, rhs, first):
        o = jnp.dot(lhs, rhs, preferred_element_type=F32)
        if first:
            ACC[...] = o
        else:
            ACC[...] += o

    def matmul_slab(gi, jz, first=False):
        def body(t, carry):
            parts = []
            for yy in range(4):
                parts.append(W1[gi, 0, jz, yy])
                parts.append(W1[gi, 1, yy, jz])
            matmul(TOK[:, jz].reshape(512, 1024), jnp.concatenate(parts, axis=0), first)
            return carry

        lax.fori_loop(0, 1, body, 0)

    def matmul_planes(gi, cc, planes, first=False):
        def body(t, carry):
            lhs, rhs = [], []
            for s_ in planes:
                for k in range(4):
                    rhs.append(W1[gi, cc, s_, k])
                    off = ((1 - cc) * k + cc * s_) * 256 + cc * 128
                    col = pl.ds(pl.multiple_of(off, 128), 128)
                    lhs.append(TOK[:, (1 - cc) * s_ + cc * k, :, col].reshape(512, 128))
            matmul(jnp.concatenate(lhs, axis=1), jnp.concatenate(rhs, axis=0), first)
            return carry

        lax.fori_loop(0, 1, body, 0)

    def post(gi):
        def body(k, carry):
            slot, r = lax.div(k, 2), lax.rem(k, 2)
            rows = pl.ds(pl.multiple_of(k * 128, 128), 128)
            tot = jnp.sum(SS[slot, pl.ds(r * 128, 128), :], axis=-1, keepdims=True)
            a = ACC[rows, :] * lax.rsqrt(tot * (1.0 / 4096) + EPS)
            PB[gi, slot, pl.ds(pl.multiple_of(16 + r * 128, 16), 128), :] = a[:, 0:512].astype(BF16)
            qf = a[:, 512:1024].astype(BF16).astype(F32)
            sq = qf * qf
            hi = sq.astype(BF16)
            lo = (sq - hi.astype(F32)).astype(BF16)
            ssq = jnp.dot(hi, BLK[...], preferred_element_type=F32) + jnp.dot(
                lo, BLK[...], preferred_element_type=F32
            )
            qg = jnp.concatenate([q_gain[...]] * 8, axis=1) * 0.125
            QB[gi, rows, :] = (qf * lax.rsqrt(ssq * (1.0 / 64) + EPS) * qg).astype(BF16)
            kv = a[:, 1024:1152].astype(BF16).astype(F32)
            is_key = lax.broadcasted_iota(jnp.int32, (128, 128), 1) < 64
            ksq = jnp.sum(jnp.where(is_key, kv * kv, 0.0), axis=-1, keepdims=True)
            kn = kv * lax.rsqrt(ksq * (1.0 / 64) + EPS) * jnp.concatenate([k_gain[...]] * 2, axis=1)
            KV[gi, slot, pl.ds(pl.multiple_of(128 + r * 128, 128), 128), :] = jnp.where(
                is_key, kn, kv
            ).astype(BF16)
            return carry

        lax.fori_loop(0, 4, body, 0)

    def halo_next(gi, i):
        qn, spn, xn, here, away, passed = halo_to(i)
        slot = jnp.where(xn == qn, 0, 1)
        gn = jnp.where(xn == x, gi, 1 - gi)
        tails = (KV.at[gi, i, pl.ds(256, 128)], PB.at[gi, i, pl.ds(256, 16)])
        copies = [
            pltpu.make_async_remote_copy(
                src_ref=src, dst_ref=dst, send_sem=hsend.at[gi, i, k], recv_sem=hrecv.at[gn, slot, k],
                device_id=(spn, xn), device_id_type=MESH,
            )
            for k, (src, dst) in enumerate(
                zip(tails, (KV.at[gn, slot, pl.ds(0, 128)], PB.at[gn, slot, pl.ds(0, 16)]))
            )
        ]
        passes = [
            pltpu.make_async_remote_copy(
                src_ref=src, dst_ref=dst, send_sem=hsend.at[gi, i, k], recv_sem=rlrecv.at[gi, k],
                device_id=dev_sib, device_id_type=MESH,
            )
            for k, (src, dst) in enumerate(zip(tails, (RLK.at[gi], RLP.at[gi])))
        ]
        return here, away, copies, passed, passes

    def halo_send(gi):
        for i in range(2):
            here, away, copies, passed, passes = halo_next(gi, i)

            @pl.when(passed)
            def _():
                for d in passes:
                    d.start()

            @pl.when(away)
            def _():
                for d in copies:
                    d.start()

            @pl.when(here)
            def _():
                KV[gi, 1 - i, pl.ds(0, 128), :] = KV[gi, i, pl.ds(256, 128), :]
                PB[gi, 1 - i, pl.ds(0, 16), :] = PB[gi, i, pl.ds(256, 16), :]

    def halo_sent(gi):
        for i in range(2):
            _, away, copies, passed, passes = halo_next(gi, i)

            @pl.when(passed)
            def _():
                for d in passes:
                    d.wait_send()

            @pl.when(away)
            def _():
                for d in copies:
                    d.wait_send()

    def relay_copies(gi):
        gn = jnp.where(par == x, gi, 1 - gi)
        return [
            pltpu.make_async_remote_copy(
                src_ref=src, dst_ref=dst, send_sem=rlsend.at[gi, k],
                recv_sem=hrecv.at[gn, relay_slot, k], device_id=relay_dev, device_id_type=MESH,
            )
            for k, (src, dst) in enumerate(
                (
                    (RLK.at[gi], KV.at[gn, relay_slot, pl.ds(0, 128)]),
                    (RLP.at[gi], PB.at[gn, relay_slot, pl.ds(0, 16)]),
                )
            )
        ]

    def halo_relay(gi):
        @pl.when(relay)
        def _():
            for k, dst in enumerate((RLK.at[gi], RLP.at[gi])):
                pltpu.make_async_copy(dst, dst, rlrecv.at[gi, k]).wait()
            for d in relay_copies(gi):
                d.start()

    def relay_sent(gi):
        @pl.when(relay)
        def _():
            for d in relay_copies(gi):
                d.wait_send()

    def halo_wait(gi):
        for i in range(2):
            first, apart, _, _ = halo_from(i)

            @pl.when(first)
            def _():
                KV[gi, i, pl.ds(0, 128), :] = jnp.zeros((128, 128), BF16)
                PB[gi, i, pl.ds(0, 16), :] = jnp.zeros((16, 512), BF16)

            @pl.when(apart)
            def _():
                for k, dst in enumerate((KV.at[gi, i, pl.ds(0, 128)], PB.at[gi, i, pl.ds(0, 16)])):
                    pltpu.make_async_copy(dst, dst, hrecv.at[gi, i, k]).wait()

    def pool(gi, g):
        span = lax.shift_left(jnp.int32(2), g)
        for i in range(2):
            pf = PB[gi, i].astype(F32)
            t2 = pf + pltpu.roll(pf, 1, 0)
            t4 = t2 + pltpu.roll(t2, 2, 0)
            t8 = t4 + pltpu.roll(t4, 4, 0)
            t16 = t8 + pltpu.roll(t8, 8, 0)
            run = jnp.where(g == 0, t2, jnp.where(g == 1, t4, jnp.where(g == 2, t8, t16)))[16:]
            pos = sp * 1024 + quarters[i] * 256 + lax.broadcasted_iota(jnp.int32, (256, 1), 0)
            count = jnp.minimum(pos + 1, span).astype(F32)
            diff = (run * (1.0 / count) - pf[16:]).astype(BF16)
            m = jnp.dot(diff, PM[gi], preferred_element_type=F32)
            m = m * SCALE[gi]
            m = m * lax.rsqrt(jnp.mean(m * m, axis=-1, keepdims=True) + EPS)
            MIX[gi, i * 256 : (i + 1) * 256, 0:512] = m.astype(BF16)

    def attend(gi, r):
        sink = jnp.exp(SINK[gi])
        left = lax.broadcasted_iota(jnp.int32, (1, 128), 1) < 64
        es = jnp.concatenate(
            [
                jnp.broadcast_to(
                    jnp.where(left, sink[:, 2 * j : 2 * j + 1], sink[:, 2 * j + 1 : 2 * j + 2]),
                    (128, 128),
                )
                for j in range(4)
            ],
            axis=0,
        )

        def body(k, carry):
            slot = k
            rows = pl.ds(pl.multiple_of(k * 256 + r * 128, 128), 128)
            kv = KV[gi, slot, pl.ds(r * 128, 256), :].astype(F32)
            low = lax.broadcasted_iota(jnp.int32, (256, 128), 1) < 64
            ke = jnp.where(low, kv, 0.0)
            vo = jnp.where(low, 0.0, kv)
            ko = pltpu.roll(ke, 64, 1)
            ve = pltpu.roll(vo, 64, 1)
            q_here = (1 - slot) * x + slot * p
            missing = jnp.where((sp == 0) & (q_here == 0), 128, 0) if r == 0 else 0
            there = lax.broadcasted_iota(jnp.int32, (256, 128), 0) >= missing
            oe = jnp.where(low & there, 1.0, 0.0)
            oo = jnp.where(jnp.logical_not(low) & there, 1.0, 0.0)
            keys = jnp.concatenate([ke, ko], axis=0).astype(BF16)
            values = jnp.concatenate(
                [jnp.concatenate([ve, oe], axis=1), jnp.concatenate([vo, oo], axis=1)], axis=0
            ).astype(BF16)
            q = QB[gi, rows, :]
            q = jnp.concatenate([q[:, j * 128 : (j + 1) * 128] for j in range(4)], axis=0)
            sc = lax.dot_general(q, keys, (((1,), (1,)), ((), ())), preferred_element_type=F32)
            e = jnp.exp(sc + BIAS[gi]).astype(BF16)
            o = jnp.dot(e, values, preferred_element_type=F32)
            att = o[:, 0:128] / (o[:, 128:256] + es)
            parts = [att[j * 128 : (j + 1) * 128] for j in range(4)]
            sq = parts[0] * parts[0]
            for j in range(1, 4):
                sq += parts[j] * parts[j]
            r_ = lax.rsqrt(jnp.sum(sq, axis=-1, keepdims=True) * (1.0 / 512) + EPS)
            for j in range(4):
                MIX[gi, rows, 512 + j * 128 : 640 + j * 128] = (parts[j] * r_).astype(BF16)
            return carry

        lax.fori_loop(0, 2, body, 0)

    recv(d1)
    share1(0, s2, sib1)
    recv(sib1)
    matmul_slab(0, x, True)
    recv(tp_)
    scale_slab(p)
    matmul_slab(0, p)
    d1o = step_d1(1, c1o)
    c2a, c2b = group(W2.at[0, 0]), group(W2.at[0, 0])
    recv(a2[1], b2)
    c2_send(0)
    x_w2 = group(shard2.at[0])
    send(W2.at[c, s, f, 0], ST2, dev_dx, x_w2, W2_SENT)
    l6.wait()
    half = pl.ds(c * 256, 256)
    x_pm = group(ST3)
    send(PM.at[0, half], ST3, dev_dx, x_pm, OTHER_SENT + 2)
    wait(two_slabs, ssem.at[TF_SENT])
    scale_slab(n)
    matmul_slab(0, n)
    recv(tf)
    scale_slab(x2)
    matmul_slab(0, x2)
    post(0)
    halo_send(0)
    recv(c1o[1])
    share1(1, sd, sib1o)
    share1(1, su, sib1o)
    recv(x_w2)
    f_w2 = group(shard2.at[0])
    send(ST2, W2.at[c, s, f, 1], dev_dx, f_w2, W2_SENT)
    matmul_planes(1, c, (s, sd, su), True)
    recv(sib1o)
    recv(f_w2)
    a2o = step_a2(1)
    recv(x_pm)
    f_pm = group(ST3)
    send(ST3, PM.at[1, half], dev_dx, f_pm, OTHER_SENT + 3)
    matmul_planes(1, cs, (ss_, ssd, ssu))
    halo_relay(0)
    attend(0, 1)
    recv(d1o)
    sib1o_far = group(W1.at[0, 0, 0])
    share1(1, s2, sib1o_far)
    matmul_planes(1, c, (s2,))
    b2o = step_b2(1, a2o)
    recv(sib1o_far)
    matmul_planes(1, cs, (ss2,))
    post(1)
    halo_send(1)

    recv(sc_c, sk_c)
    attend(1, 1)
    halo_relay(1)
    recv(f_pm)
    sib_pm = group(ST3)
    send(PM.at[1, half], PM.at[1, half], dev_sib, sib_pm, OTHER_SENT + 4)
    recv(a2o[1], b2o)
    c2_send(1)
    sib2_own = group(W2.at[0, 0])
    send2(W2.at[c, s], dev_sib, sib2_own)
    halo_wait(0)
    attend(0, 0)
    pool(0, x)
    halo_wait(1)
    attend(1, 0)
    recv(sib_pm)
    pool(1, x2)

    def product(cc, s_, fs, g):
        rhs = jnp.concatenate([W2[cc, s_, fs[0], g], W2[cc, s_, fs[1], g]], axis=1)
        return jnp.dot(MIX[g], rhs, preferred_element_type=F32)

    def unit(u, cc, s_, fs):
        leave(u, product(cc, s_, fs, 0) + product(cc, s_, fs, 1))

    def leave(u, o):
        ob = o.astype(BF16)
        for e in range(2):
            idx = 2 * u + e
            OWNB[idx] = ob[0:256, e * 128 : (e + 1) * 128]
            SENDB[idx] = ob[256:512, e * 128 : (e + 1) * 128]
            pltpu.make_async_remote_copy(
                src_ref=SENDB.at[idx], dst_ref=RECVB.at[idx], send_sem=osend, recv_sem=orecv.at[u],
                device_id=dev_p, device_id_type=MESH,
            ).start()

    def total(u, cc, s_, fs):
        wait(RECVB.at[pl.ds(2 * u, 2)], orecv.at[u])
        for e in range(2):
            idx = 2 * u + e
            col = pl.ds(pl.multiple_of(sp_of(cc, fs[e], s_) * 128, 128), 128)
            OWNB[idx] = (OWNB[idx].astype(F32) + RECVB[idx].astype(F32)).astype(BF16)
            pltpu.make_async_copy(OWNB.at[idx], out.at[:, col], oloc).start()

    def pair(stage, mine, sA, kA, sB, kB, act=unit):
        cc = c if mine else cs

        def body(t, carry):
            k = kA + t * (kB - kA)
            act(stage * 4 + (0 if mine else 2) + t, cc, sA + t * (sB - sA), (2 * k, 2 * k + 1))
            return carry

        lax.fori_loop(0, 2, body, 0)

    def far_unit(u, cc, s_, k, act):
        def body(t, carry):
            act(u, cc, s_, (t, 2 + t))
            return carry

        lax.fori_loop(k, k + 1, body, 0)

    pair(0, True, s, 0, s, 1)
    recv(sib2_own)
    pair(0, False, ss_, 0, ss_, 1)
    recv(c2a)
    u0, d0 = half_plane(sd, 0), half_plane(su, 1)
    last = [group(shard2) for _ in range(4)]
    d2 = [group(W2.at[0, 0, pl.ds(0, 2)]), last[0], last[1]]
    send2(u0.at[0], dev_su, d2[0])
    send2(d0.at[0], dev_sd, d2[0])
    for g in range(2):
        send2(u0.at[1, g], dev_su, d2[1 + g])
        send2(d0.at[1, g], dev_sd, d2[1 + g])
    sib2_a = group(W2.at[0, 0])
    send2(u0, dev_sib, sib2_a)
    send2(d0, dev_sib, sib2_a)
    pair(1, True, sd, 0, su, 1)
    recv(sib2_a)
    pair(1, False, ssd, 0, ssu, 1)
    recv(c2b)
    sib2_b = group(W2.at[0, 0])
    send2(half_plane(sd, 1), dev_sib, sib2_b)
    send2(half_plane(su, 0), dev_sib, sib2_b)
    pair(2, True, sd, 1, su, 0)
    pair(0, True, s, 0, s, 1, total)
    pair(0, False, ss_, 0, ss_, 1, total)
    recv(sib2_b)
    pair(2, False, ssd, 1, ssu, 0)

    recv(d2[0])
    sib2_c = group(W2.at[0, 0, pl.ds(0, 2)])
    send2(W2.at[c, s2, 0], dev_sib, sib2_c)
    send2(W2.at[c, s2, 2], dev_sib, sib2_c)
    far_unit(12, c, s2, 0, unit)
    recv(sib2_c)
    far_unit(13, cs, ss2, 0, unit)
    pair(1, True, sd, 0, su, 1, total)
    pair(1, False, ssd, 0, ssu, 1, total)

    def last_step(t, carry):
        g, other = lax.rem(t, 2), lax.div(t, 2)
        wait(shard2, rsem.at[last[0] + t])

        @pl.when(t < 2)
        def _():
            for k in (1, 3):
                send2(W2.at[c, s2, k, g], dev_sib, last[2] + t)

        cc, s_ = c + other * (cs - c), s2 + other * (ss2 - s2)
        rhs = jnp.concatenate([W2[cc, s_, k, g] for k in (1, 3)], axis=1)
        o = jnp.dot(MIX[g], rhs, preferred_element_type=F32)
        o = jnp.where(g == 0, o, ACC[:, 0:256] + o)
        ACC[:, 0:256] = o

        @pl.when(g == 1)
        def _():
            leave(14 + other, ACC[:, 0:256])

        return carry

    lax.fori_loop(0, 4, last_step, 0)

    wait(W1, ssem.at[W1_SENT])
    wait(W2, ssem.at[W2_SENT])
    wait(TOK.at[0], ssem.at[TOK_SENT])
    for k, whole in enumerate((SCALE.at[1], SINK.at[1], ST3, ST3, ST3)):
        wait(whole, ssem.at[OTHER_SENT + k])
    for gi in range(2):
        halo_sent(gi)
        relay_sent(gi)
    wait(SENDB, osend)
    pair(2, True, sd, 1, su, 0, total)
    pair(2, False, ssd, 1, ssu, 0, total)
    for k in range(2):
        far_unit(12 + 2 * k, c, s2, k, total)
        far_unit(13 + 2 * k, cs, ss2, k, total)
    wait(OWNB, oloc)
    assert len(groups) == N_GROUPS, len(groups)


def hand_over(src, out, held, in_sem, out_sem):
    rows = 256 // PIECES
    parts = [pl.ds(k * rows, rows) for k in range(PIECES)]
    ins = [pltpu.make_async_copy(src.at[r], held.at[r], in_sem.at[k]) for k, r in enumerate(parts)]
    outs = [pltpu.make_async_copy(held.at[r], out.at[r], out_sem.at[k]) for k, r in enumerate(parts)]
    for d in ins:
        d.start()
    for d, o in zip(ins, outs):
        d.wait()
        o.start()
    for o in outs:
        o.wait()


def local_program(
    tokens, norm_gain, w_pool_in, w_query, w_key, w_value, pool_map, pool_scale,
    q_gain, k_gain, sinks, w_out,
):
    any_ = pl.BlockSpec(memory_space=pl.ANY)
    dma = pltpu.SemaphoreType.DMA
    summed = pl.pallas_call(
        kernel,
        out_shape=jax.ShapeDtypeStruct((256, 4096), BF16),
        in_specs=[any_] * 12,
        out_specs=any_,
        scratch_shapes=[
            pltpu.VMEM((2, 2, 4, 4, 128, 1152), BF16),
            pltpu.VMEM((2, 4, 4, 2, 1024, 128), BF16),
            pltpu.VMEM((2, 4, 256, 1024), BF16),
            pltpu.VMEM((128, 1152), BF16),
            pltpu.VMEM((1024, 128), BF16),
            pltpu.VMEM((256, 512), BF16),
            pltpu.VMEM((2, 512, 512), BF16),
            pltpu.VMEM((2, 1, 512), F32),
            pltpu.VMEM((2, 1, 8), F32),
            pltpu.VMEM((1, 64), F32),
            pltpu.VMEM((1, 64), F32),
            pltpu.VMEM((1, 4096), F32),
            pltpu.VMEM((128, 128), BF16),
            pltpu.VMEM((2, 2, 384, 128), BF16),
            pltpu.VMEM((2, 2, 272, 512), BF16),
            pltpu.VMEM((2, 512, 512), BF16),
            pltpu.VMEM((512, 1152), F32),
            pltpu.VMEM((2, 256, 128), F32),
            pltpu.VMEM((2, 512, 1024), BF16),
            pltpu.VMEM((2, 512, 512), F32),
            pltpu.VMEM((512, 512), BF16),
            pltpu.VMEM((32, 256, 128), BF16),
            pltpu.VMEM((32, 256, 128), BF16),
            pltpu.VMEM((32, 256, 128), BF16),
            pltpu.VMEM((2, 128, 128), BF16),
            pltpu.VMEM((2, 16, 512), BF16),
            dma((13,)),
            dma((9,)),
            dma((N_GROUPS,)),
            dma(()),
            dma((16,)),
            dma(()),
            dma((2, 2, 2)),
            dma((2, 2, 2)),
            dma((2, 2)),
            dma((2, 2)),
        ],
        compiler_params=pltpu.CompilerParams(
            collective_id=0, has_side_effects=True, vmem_limit_bytes=66_000_000
        ),
        name="mixer",
    )(
        tokens, w_pool_in, w_query, w_key.T, w_value.T, w_out, pool_map.reshape(512, 512),
        pool_scale.reshape(1, 512), sinks.reshape(1, 8), q_gain.reshape(1, 64),
        k_gain.reshape(1, 64), norm_gain.reshape(1, 4096),
    )
    return pl.pallas_call(
        hand_over,
        out_shape=jax.ShapeDtypeStruct((256, 4096), BF16),
        in_specs=[any_],
        out_specs=any_,
        scratch_shapes=[pltpu.VMEM((256, 4096), BF16), dma((PIECES,)), dma((PIECES,))],
        name="hand_over",
    )(summed)


def solution(mesh):
    in_specs = (
        P("sp", "tp"), P(), P("sp", "tp"), P("sp", "tp"), P("sp", "tp"), P("sp", "tp"),
        P("tp", None, None), P("tp"), P(), P(), P("tp"), P("tp", "sp"),
    )
    out_specs = P(("sp", "tp"), None)
    return jax.shard_map(local_program, mesh=mesh, in_specs=in_specs, out_specs=out_specs, check_vma=False)
```

```python
import jax
import jax.numpy as jnp
from jax import lax
from jax.experimental import pallas as pl
from jax.experimental.pallas import tpu as pltpu
from jax.sharding import PartitionSpec as P

MESH = pl.DeviceIdType.MESH
F32 = jnp.float32
BF16 = jnp.bfloat16
EPS = 1e-6
N_GROUPS = 45
PIECES = 8


def mod4(v):
    return lax.rem(v, 4)


def kernel(
    tokens, wp, wq, wk_t, wv_t, wo, pmap, scale_in, sinks_in, q_in, k_in, gain_in,
    out,
    W1, W2, TOK, ST1, ST2, ST3, PM, SCALE, SINK, q_gain, k_gain, gain, KVT, KV, PB, QB, ACC, SS, MIX, BIAS, BLK, SENDB, OWNB, RECVB, RLK, RLP,
    lsem, ssem, rsem, osend, orecv, oloc, hsend, hrecv, rlsend, rlrecv,
):
    sp = lax.axis_index("sp")
    x = lax.axis_index("tp")
    c = lax.rem(sp, 2)
    y = mod4(lax.div(sp, 2))
    z = lax.div(sp, 8)
    f = y + c * (z - y)
    s = z + c * (y - z)
    par = lax.rem(x, 2)
    flip1 = x + 1 - 2 * par
    flip3 = 3 - x
    p = (1 - c) * flip1 + c * flip3
    n = (1 - c) * flip3 + c * flip1
    x2 = mod4(x + 2)
    dx = mod4(x + 1 + 2 * c)

    def sp_of(c_, f_, s_):
        y_ = (1 - c_) * f_ + c_ * s_
        z_ = (1 - c_) * s_ + c_ * f_
        return (z_ * 4 + y_) * 2 + c_

    fu, fd = mod4(f + 1), mod4(f + 3)
    su, sd, s2 = mod4(s + 1), mod4(s + 3), mod4(s + 2)
    dev_fu, dev_fd = (sp_of(c, fu, s), x), (sp_of(c, fd, s), x)
    dev_su, dev_sd = (sp_of(c, f, su), x), (sp_of(c, f, sd), x)
    dev_sib = (sp + 1 - 2 * c, x)
    dev_dx, dev_p, dev_n, dev_x2 = (sp, dx), (sp, p), (sp, n), (sp, x2)
    cs, ss_, sf_ = 1 - c, f, s
    ssu, ssd, ss2 = mod4(ss_ + 1), mod4(ss_ + 3), mod4(ss_ + 2)

    groups = []
    W1_SENT, W2_SENT, TOK_SENT, TF_SENT, OTHER_SENT = range(5)

    def group(whole):
        groups.append(whole)
        return len(groups) - 1

    def send(src, dst, dev, to, sent):
        pltpu.make_async_remote_copy(
            src_ref=src, dst_ref=dst, send_sem=ssem.at[sent], recv_sem=rsem.at[to],
            device_id=dev, device_id_type=MESH,
        ).start()

    def wait(whole, sem):
        pltpu.make_async_copy(whole, whole, sem).wait()

    def recv(*gs):
        for g in gs:
            wait(groups[g], rsem.at[g])

    def holder(q, c_):
        inner = lax.rem(lax.div(q + 1, 2), 2)
        even = lax.div(q, 2) * 2 + par
        odd = inner * (2 - par) + (1 - inner) * 3 * par
        return (1 - c_) * even + c_ * odd

    quarters = (x, p)

    def halo_to(i):
        q = quarters[i]
        qn = mod4(q + 1)
        spn = sp + lax.div(q + 1, 4)
        xn = holder(qn, lax.rem(spn, 2))
        here = (spn == sp) & (xn == x)
        away = jnp.logical_not(here) & (spn < 32)
        passed = away & (c == 1) & (q == 3)
        return qn, jnp.where(spn < 32, spn, 0), xn, here, away & jnp.logical_not(passed), passed

    def halo_from(i):
        q = quarters[i]
        first = (sp == 0) & (q == 0)
        back = jnp.where(q == 0, 1, 0)
        relayed = (back == 1) & (c == 0)
        spp = jnp.where(first, sp, sp - back - jnp.where(relayed, 1, 0))
        xp = holder(mod4(q + 3), lax.rem(sp - back + 2, 2))
        here = (back == 0) & (xp == x)
        return first, jnp.logical_not(first) & jnp.logical_not(here), spp, xp

    relay = (c == 0) & ((x == 0) | (x == 3)) & (sp < 30)
    relay_dev = (jnp.where(relay, sp + 2, 0), par)
    relay_slot = jnp.where(par == 0, 0, 1)

    barrier = pltpu.get_barrier_semaphore()

    def greet(dev):
        pl.semaphore_signal(barrier, inc=1, device_id=dev, device_id_type=MESH)

    @pl.when(relay)
    def _():
        greet(relay_dev)

    for i in range(2):
        _, spn, xn, _, away, _ = halo_to(i)

        @pl.when(away)
        def _():
            greet((spn, xn))

        _, apart, spp, xp = halo_from(i)

        @pl.when(apart)
        def _():
            greet((spp, xp))

    for dev in (dev_x2, dev_su, dev_sd, dev_fu, dev_fd, dev_p, dev_n, dev_sib):
        greet(dev)

    loc = []

    def local(src, dst):
        d = pltpu.make_async_copy(src, dst, lsem.at[len(loc)])
        d.start()
        loc.append(d)
        return d

    own1 = W1.at[0, c, s, f]
    l0 = local(wp, own1.at[:, pl.ds(0, 512)])
    l1 = local(wq, own1.at[:, pl.ds(512, 512)])
    l2 = local(wk_t, KVT.at[pl.ds(0, 64)])
    l7 = local(wv_t, KVT.at[pl.ds(64, 64)])
    l3 = local(wo, W2.at[c, s, f, 0])
    l4 = local(tokens.at[pl.ds(x * 256, 256)], TOK.at[0, x])
    l5 = local(tokens.at[pl.ds(p * 256, 256)], TOK.at[1, x])
    l6 = local(pmap, PM.at[0])
    small = [
        local(src, dst)
        for src, dst in (
            (scale_in, SCALE.at[0]), (sinks_in, SINK.at[0]), (q_in, q_gain), (k_in, k_gain), (gain_in, gain),
        )
    ]

    lane_i = lax.broadcasted_iota(jnp.int32, (512, 512), 1)
    row_i = lax.broadcasted_iota(jnp.int32, (512, 512), 0)
    l2.wait()
    l7.wait()
    W1[0, c, s, f, :, pl.ds(1024, 128)] = KVT[...].astype(F32).T.astype(BF16)
    BLK[...] = jnp.where(
        lax.shift_right_logical(lane_i, 6) == lax.shift_right_logical(row_i, 6), 1.0, 0.0
    ).astype(BF16)
    SS[...] = jnp.zeros_like(SS)
    peers = 8 + jnp.where(relay, 1, 0)
    for i in range(2):
        peers += jnp.where(halo_to(i)[4], 1, 0) + jnp.where(halo_from(i)[1], 1, 0)
    pl.semaphore_wait(barrier, peers)

    l0.wait()
    l1.wait()
    l3.wait()
    shard1, shard2 = W1.at[0, 0, 0, 0], W2.at[0, 0, 0]

    def send1(piece, dev, to):
        send(piece, piece, dev, to, W1_SENT)

    def send2(piece, dev, to):
        send(piece, piece, dev, to, W2_SENT)

    def step_a1(g):
        piece = W1.at[g, c, s, f]
        to = group(shard1), group(shard1)
        for k in range(2):
            send1(piece.at[pl.ds(64 * k, 64)], dev_fu, to[k])
            send1(piece.at[pl.ds(64 - 64 * k, 64)], dev_fd, to[k])
        return to

    def step_b1(g, a):
        recv(a[0])
        to = group(shard1)
        send1(W1.at[g, c, s, fd, pl.ds(0, 64)], dev_fu, to)
        send1(W1.at[g, c, s, fu, pl.ds(64, 64)], dev_fd, to)
        return to

    def step_c1(g, a, b, shared):
        recv(a[1], b)
        plane = W1.at[g, c, s]
        to = group(W1.at[0, 0, 0]), group(W1.at[0, 0, 0])
        for k in range(2):
            send1(plane.at[pl.ds(2 * k, 2)], dev_su, to[k])
            send1(plane.at[pl.ds(2 - 2 * k, 2)], dev_sd, to[k])
        send1(plane, dev_sib, shared)
        return to

    def step_d1(g, cc):
        recv(cc[0])
        to = group(W1.at[0, 0, 0])
        send1(W1.at[g, c, sd, pl.ds(0, 2)], dev_su, to)
        send1(W1.at[g, c, su, pl.ds(2, 2)], dev_sd, to)
        return to

    def share1(g, s_, to):
        send1(W1.at[g, c, s_], dev_sib, to)

    def step_a2(g):
        to = group(shard2.at[0]), group(shard2.at[0])
        for k in range(2):
            send2(W2.at[c, s, f, g, pl.ds(512 * k, 512)], dev_fu, to[k])
            send2(W2.at[c, s, f, g, pl.ds(512 - 512 * k, 512)], dev_fd, to[k])
        return to

    def step_b2(g, a):
        recv(a[0])
        to = group(shard2.at[0])
        send2(W2.at[c, s, fd, g, pl.ds(0, 512)], dev_fu, to)
        send2(W2.at[c, s, fu, g, pl.ds(512, 512)], dev_fd, to)
        return to

    x_w1 = [group(shard1.at[pl.ds(0, 64)]) for _ in range(2)]
    for k in range(2):
        part = pl.ds(64 * k, 64)
        send(own1.at[part], ST1.at[part], dev_dx, x_w1[k], W1_SENT)
    a1 = step_a1(0)
    a2 = step_a2(0)
    key_i = jnp.bitwise_and(lane_i, 255)
    dist = 128 + jnp.bitwise_and(row_i, 127) - key_i
    band = (dist >= 0) & (dist < 128)
    head_in = 2 * lax.shift_right_logical(row_i, 7) + lax.shift_right_logical(lane_i, 8) + 1
    for gi, g in ((0, x), (1, x2)):
        slope = jnp.exp2(-0.25 * (g * 8 + head_in).astype(F32))
        BIAS[gi] = jnp.where(band, -slope * dist.astype(F32), -1e30)

    f_w1 = group(shard1)
    for k in range(2):
        recv(x_w1[k])
        part = pl.ds(64 * k, 64)
        send(ST1.at[part], W1.at[1, c, s, f, part], dev_dx, f_w1, W1_SENT)
        if k == 0:
            b1 = step_b1(0, a1)
    two_slabs = TOK.at[0, pl.ds(0, 2)]
    tn = group(two_slabs)
    send(tokens.at[pl.ds(n * 256, 256)], TOK.at[0, x], dev_n, tn, TOK_SENT)
    send(tokens.at[pl.ds(x2 * 256, 256)], TOK.at[1, x], dev_n, tn, TOK_SENT)
    sc_c, sk_c = group(SCALE.at[1]), group(SINK.at[1])
    send(scale_in, SCALE.at[1], dev_x2, sc_c, OTHER_SENT)
    send(sinks_in, SINK.at[1], dev_x2, sk_c, OTHER_SENT + 1)

    b2 = step_b2(0, a2)
    sib1 = group(W1.at[0, 0])
    c1a, c1b = step_c1(0, a1, b1, sib1)
    recv(f_w1)
    a1o = step_a1(1)

    def scale_slab(j):
        g = gain[:, pl.ds(pl.multiple_of(j * 1024, 1024), 1024)]

        def body(k, carry):
            slot, r = lax.div(k, 4), pl.ds(lax.rem(k, 4) * 64, 64)
            t = TOK[slot, j, r, :].astype(F32)
            sq = t * t
            tot = sq[:, 0:128]
            for m in range(1, 8):
                tot += sq[:, m * 128 : (m + 1) * 128]
            SS[slot, r, :] += tot
            TOK[slot, j, r, :] = (t * g).astype(BF16)
            return carry

        lax.fori_loop(0, 8, body, 0)

    for d in (l4, l5, *small):
        d.wait()
    scale_slab(x)
    b1o = step_b1(1, a1o)
    tp_ = group(two_slabs)
    send(tokens.at[pl.ds(p * 256, 256)], TOK.at[0, x], dev_p, tp_, TOK_SENT)
    send(tokens.at[pl.ds(x * 256, 256)], TOK.at[1, x], dev_p, tp_, TOK_SENT)
    recv(tn)
    tf = group(two_slabs)
    send(TOK.at[0, n], TOK.at[1, n], dev_p, tf, TF_SENT)
    send(TOK.at[1, n], TOK.at[0, n], dev_p, tf, TF_SENT)
    d1 = step_d1(0, (c1a, c1b))
    sib1o = group(W1.at[0, 0, pl.ds(0, 3)])
    c1o = step_c1(1, a1o, b1o, sib1o)
    recv(c1b)
    share1(0, sd, sib1)
    share1(0, su, sib1)

    def half_plane(s_, k):
        return W2.at[c, s_, pl.ds(2 * k, 2)]

    def c2_send(g):
        to = c2a, c2b
        for k in range(2):
            send2(W2.at[c, s, pl.ds(2 * k, 2), g], dev_su, to[k])
            send2(W2.at[c, s, pl.ds(2 - 2 * k, 2), g], dev_sd, to[k])

    def matmul(lhs, rhs, first):
        o = jnp.dot(lhs, rhs, preferred_element_type=F32)
        if first:
            ACC[...] = o
        else:
            ACC[...] += o

    def matmul_slab(gi, jz, first=False):
        def body(t, carry):
            parts = []
            for yy in range(4):
                parts.append(W1[gi, 0, jz, yy])
                parts.append(W1[gi, 1, yy, jz])
            matmul(TOK[:, jz].reshape(512, 1024), jnp.concatenate(parts, axis=0), first)
            return carry

        lax.fori_loop(0, 1, body, 0)

    def matmul_planes(gi, cc, planes, first=False):
        def body(t, carry):
            lhs, rhs = [], []
            for s_ in planes:
                for k in range(4):
                    rhs.append(W1[gi, cc, s_, k])
                    off = ((1 - cc) * k + cc * s_) * 256 + cc * 128
                    col = pl.ds(pl.multiple_of(off, 128), 128)
                    lhs.append(TOK[:, (1 - cc) * s_ + cc * k, :, col].reshape(512, 128))
            matmul(jnp.concatenate(lhs, axis=1), jnp.concatenate(rhs, axis=0), first)
            return carry

        lax.fori_loop(0, 1, body, 0)

    def post(gi):
        def body(k, carry):
            slot, r = lax.div(k, 2), lax.rem(k, 2)
            rows = pl.ds(pl.multiple_of(k * 128, 128), 128)
            tot = jnp.sum(SS[slot, pl.ds(r * 128, 128), :], axis=-1, keepdims=True)
            a = ACC[rows, :] * lax.rsqrt(tot * (1.0 / 4096) + EPS)
            PB[gi, slot, pl.ds(pl.multiple_of(16 + r * 128, 16), 128), :] = a[:, 0:512].astype(BF16)
            qf = a[:, 512:1024].astype(BF16).astype(F32)
            sq = qf * qf
            hi = sq.astype(BF16)
            lo = (sq - hi.astype(F32)).astype(BF16)
            ssq = jnp.dot(hi, BLK[...], preferred_element_type=F32) + jnp.dot(
                lo, BLK[...], preferred_element_type=F32
            )
            qg = jnp.concatenate([q_gain[...]] * 8, axis=1) * 0.125
            QB[gi, rows, :] = (qf * lax.rsqrt(ssq * (1.0 / 64) + EPS) * qg).astype(BF16)
            kv = a[:, 1024:1152].astype(BF16).astype(F32)
            is_key = lax.broadcasted_iota(jnp.int32, (128, 128), 1) < 64
            ksq = jnp.sum(jnp.where(is_key, kv * kv, 0.0), axis=-1, keepdims=True)
            kn = kv * lax.rsqrt(ksq * (1.0 / 64) + EPS) * jnp.concatenate([k_gain[...]] * 2, axis=1)
            KV[gi, slot, pl.ds(pl.multiple_of(128 + r * 128, 128), 128), :] = jnp.where(
                is_key, kn, kv
            ).astype(BF16)
            return carry

        lax.fori_loop(0, 4, body, 0)

    def halo_next(gi, i):
        qn, spn, xn, here, away, passed = halo_to(i)
        slot = jnp.where(xn == qn, 0, 1)
        gn = jnp.where(xn == x, gi, 1 - gi)
        tails = (KV.at[gi, i, pl.ds(256, 128)], PB.at[gi, i, pl.ds(256, 16)])
        copies = [
            pltpu.make_async_remote_copy(
                src_ref=src, dst_ref=dst, send_sem=hsend.at[gi, i, k], recv_sem=hrecv.at[gn, slot, k],
                device_id=(spn, xn), device_id_type=MESH,
            )
            for k, (src, dst) in enumerate(
                zip(tails, (KV.at[gn, slot, pl.ds(0, 128)], PB.at[gn, slot, pl.ds(0, 16)]))
            )
        ]
        passes = [
            pltpu.make_async_remote_copy(
                src_ref=src, dst_ref=dst, send_sem=hsend.at[gi, i, k], recv_sem=rlrecv.at[gi, k],
                device_id=dev_sib, device_id_type=MESH,
            )
            for k, (src, dst) in enumerate(zip(tails, (RLK.at[gi], RLP.at[gi])))
        ]
        return here, away, copies, passed, passes

    def halo_send(gi):
        for i in range(2):
            here, away, copies, passed, passes = halo_next(gi, i)

            @pl.when(passed)
            def _():
                for d in passes:
                    d.start()

            @pl.when(away)
            def _():
                for d in copies:
                    d.start()

            @pl.when(here)
            def _():
                KV[gi, 1 - i, pl.ds(0, 128), :] = KV[gi, i, pl.ds(256, 128), :]
                PB[gi, 1 - i, pl.ds(0, 16), :] = PB[gi, i, pl.ds(256, 16), :]

    def halo_sent(gi):
        for i in range(2):
            _, away, copies, passed, passes = halo_next(gi, i)

            @pl.when(passed)
            def _():
                for d in passes:
                    d.wait_send()

            @pl.when(away)
            def _():
                for d in copies:
                    d.wait_send()

    def relay_copies(gi):
        gn = jnp.where(par == x, gi, 1 - gi)
        return [
            pltpu.make_async_remote_copy(
                src_ref=src, dst_ref=dst, send_sem=rlsend.at[gi, k],
                recv_sem=hrecv.at[gn, relay_slot, k], device_id=relay_dev, device_id_type=MESH,
            )
            for k, (src, dst) in enumerate(
                (
                    (RLK.at[gi], KV.at[gn, relay_slot, pl.ds(0, 128)]),
                    (RLP.at[gi], PB.at[gn, relay_slot, pl.ds(0, 16)]),
                )
            )
        ]

    def halo_relay(gi):
        @pl.when(relay)
        def _():
            for k, dst in enumerate((RLK.at[gi], RLP.at[gi])):
                pltpu.make_async_copy(dst, dst, rlrecv.at[gi, k]).wait()
            for d in relay_copies(gi):
                d.start()

    def relay_sent(gi):
        @pl.when(relay)
        def _():
            for d in relay_copies(gi):
                d.wait_send()

    def halo_wait(gi):
        for i in range(2):
            first, apart, _, _ = halo_from(i)

            @pl.when(first)
            def _():
                KV[gi, i, pl.ds(0, 128), :] = jnp.zeros((128, 128), BF16)
                PB[gi, i, pl.ds(0, 16), :] = jnp.zeros((16, 512), BF16)

            @pl.when(apart)
            def _():
                for k, dst in enumerate((KV.at[gi, i, pl.ds(0, 128)], PB.at[gi, i, pl.ds(0, 16)])):
                    pltpu.make_async_copy(dst, dst, hrecv.at[gi, i, k]).wait()

    def pool(gi, g):
        span = lax.shift_left(jnp.int32(2), g)
        for i in range(2):
            pf = PB[gi, i].astype(F32)
            t2 = pf + pltpu.roll(pf, 1, 0)
            t4 = t2 + pltpu.roll(t2, 2, 0)
            t8 = t4 + pltpu.roll(t4, 4, 0)
            t16 = t8 + pltpu.roll(t8, 8, 0)
            run = jnp.where(g == 0, t2, jnp.where(g == 1, t4, jnp.where(g == 2, t8, t16)))[16:]
            pos = sp * 1024 + quarters[i] * 256 + lax.broadcasted_iota(jnp.int32, (256, 1), 0)
            count = jnp.minimum(pos + 1, span).astype(F32)
            diff = (run * (1.0 / count) - pf[16:]).astype(BF16)
            m = jnp.dot(diff, PM[gi], preferred_element_type=F32)
            m = m * SCALE[gi]
            m = m * lax.rsqrt(jnp.mean(m * m, axis=-1, keepdims=True) + EPS)
            MIX[gi, i * 256 : (i + 1) * 256, 0:512] = m.astype(BF16)

    def attend(gi, r):
        sink = jnp.exp(SINK[gi])
        left = lax.broadcasted_iota(jnp.int32, (1, 128), 1) < 64
        es = jnp.concatenate(
            [
                jnp.broadcast_to(
                    jnp.where(left, sink[:, 2 * j : 2 * j + 1], sink[:, 2 * j + 1 : 2 * j + 2]),
                    (128, 128),
                )
                for j in range(4)
            ],
            axis=0,
        )

        def body(k, carry):
            slot = k
            rows = pl.ds(pl.multiple_of(k * 256 + r * 128, 128), 128)
            kv = KV[gi, slot, pl.ds(r * 128, 256), :].astype(F32)
            low = lax.broadcasted_iota(jnp.int32, (256, 128), 1) < 64
            ke = jnp.where(low, kv, 0.0)
            vo = jnp.where(low, 0.0, kv)
            ko = pltpu.roll(ke, 64, 1)
            ve = pltpu.roll(vo, 64, 1)
            q_here = (1 - slot) * x + slot * p
            missing = jnp.where((sp == 0) & (q_here == 0), 128, 0) if r == 0 else 0
            there = lax.broadcasted_iota(jnp.int32, (256, 128), 0) >= missing
            oe = jnp.where(low & there, 1.0, 0.0)
            oo = jnp.where(jnp.logical_not(low) & there, 1.0, 0.0)
            keys = jnp.concatenate([ke, ko], axis=0).astype(BF16)
            values = jnp.concatenate(
                [jnp.concatenate([ve, oe], axis=1), jnp.concatenate([vo, oo], axis=1)], axis=0
            ).astype(BF16)
            q = QB[gi, rows, :]
            q = jnp.concatenate([q[:, j * 128 : (j + 1) * 128] for j in range(4)], axis=0)
            sc = lax.dot_general(q, keys, (((1,), (1,)), ((), ())), preferred_element_type=F32)
            e = jnp.exp(sc + BIAS[gi]).astype(BF16)
            o = jnp.dot(e, values, preferred_element_type=F32)
            att = o[:, 0:128] / (o[:, 128:256] + es)
            parts = [att[j * 128 : (j + 1) * 128] for j in range(4)]
            sq = parts[0] * parts[0]
            for j in range(1, 4):
                sq += parts[j] * parts[j]
            r_ = lax.rsqrt(jnp.sum(sq, axis=-1, keepdims=True) * (1.0 / 512) + EPS)
            for j in range(4):
                MIX[gi, rows, 512 + j * 128 : 640 + j * 128] = (parts[j] * r_).astype(BF16)
            return carry

        lax.fori_loop(0, 2, body, 0)

    recv(d1)
    share1(0, s2, sib1)
    recv(sib1)
    matmul_slab(0, x, True)
    recv(tp_)
    scale_slab(p)
    x_w2 = group(shard2.at[0])
    send(W2.at[c, s, f, 0], ST2, dev_dx, x_w2, W2_SENT)
    matmul_slab(0, p)
    d1o = step_d1(1, c1o)
    c2a, c2b = group(W2.at[0, 0]), group(W2.at[0, 0])
    recv(a2[1], b2)
    c2_send(0)
    l6.wait()
    half = pl.ds(c * 256, 256)
    x_pm = group(ST3)
    send(PM.at[0, half], ST3, dev_dx, x_pm, OTHER_SENT + 2)
    wait(two_slabs, ssem.at[TF_SENT])
    scale_slab(n)
    matmul_slab(0, n)
    recv(tf)
    scale_slab(x2)
    matmul_slab(0, x2)
    recv(x_w2)
    f_w2 = group(shard2.at[0])
    send(ST2, W2.at[c, s, f, 1], dev_dx, f_w2, W2_SENT)
    post(0)
    halo_send(0)
    recv(c1o[1])
    share1(1, sd, sib1o)
    share1(1, su, sib1o)
    matmul_planes(1, c, (s, sd, su), True)
    recv(sib1o)
    recv(f_w2)
    a2o = step_a2(1)
    recv(x_pm)
    f_pm = group(ST3)
    send(ST3, PM.at[1, half], dev_dx, f_pm, OTHER_SENT + 3)
    matmul_planes(1, cs, (ss_, ssd, ssu))
    halo_relay(0)
    attend(0, 1)
    recv(d1o)
    sib1o_far = group(W1.at[0, 0, 0])
    share1(1, s2, sib1o_far)
    matmul_planes(1, c, (s2,))
    b2o = step_b2(1, a2o)
    recv(sib1o_far)
    matmul_planes(1, cs, (ss2,))
    post(1)
    halo_send(1)

    recv(sc_c, sk_c)
    attend(1, 1)
    halo_relay(1)
    recv(f_pm)
    sib_pm = group(ST3)
    send(PM.at[1, half], PM.at[1, half], dev_sib, sib_pm, OTHER_SENT + 4)
    recv(a2o[1], b2o)
    c2_send(1)
    sib2_own = group(W2.at[0, 0])
    send2(W2.at[c, s], dev_sib, sib2_own)
    halo_wait(0)
    attend(0, 0)
    pool(0, x)
    halo_wait(1)
    attend(1, 0)
    recv(sib_pm)
    pool(1, x2)

    def product(cc, s_, fs, g):
        rhs = jnp.concatenate([W2[cc, s_, fs[0], g], W2[cc, s_, fs[1], g]], axis=1)
        return jnp.dot(MIX[g], rhs, preferred_element_type=F32)

    def unit(u, cc, s_, fs):
        leave(u, product(cc, s_, fs, 0) + product(cc, s_, fs, 1))

    def leave(u, o):
        ob = o.astype(BF16)
        for e in range(2):
            idx = 2 * u + e
            OWNB[idx] = ob[0:256, e * 128 : (e + 1) * 128]
            SENDB[idx] = ob[256:512, e * 128 : (e + 1) * 128]
            pltpu.make_async_remote_copy(
                src_ref=SENDB.at[idx], dst_ref=RECVB.at[idx], send_sem=osend, recv_sem=orecv.at[u],
                device_id=dev_p, device_id_type=MESH,
            ).start()

    def total(u, cc, s_, fs):
        wait(RECVB.at[pl.ds(2 * u, 2)], orecv.at[u])
        for e in range(2):
            idx = 2 * u + e
            col = pl.ds(pl.multiple_of(sp_of(cc, fs[e], s_) * 128, 128), 128)
            OWNB[idx] = (OWNB[idx].astype(F32) + RECVB[idx].astype(F32)).astype(BF16)
            pltpu.make_async_copy(OWNB.at[idx], out.at[:, col], oloc).start()

    def pair(stage, mine, sA, kA, sB, kB, act=unit):
        cc = c if mine else cs

        def body(t, carry):
            k = kA + t * (kB - kA)
            act(stage * 4 + (0 if mine else 2) + t, cc, sA + t * (sB - sA), (2 * k, 2 * k + 1))
            return carry

        lax.fori_loop(0, 2, body, 0)

    def far_unit(u, cc, s_, k, act):
        def body(t, carry):
            act(u, cc, s_, (t, 2 + t))
            return carry

        lax.fori_loop(k, k + 1, body, 0)

    pair(0, True, s, 0, s, 1)
    recv(sib2_own)
    pair(0, False, ss_, 0, ss_, 1)
    recv(c2a)
    u0, d0 = half_plane(sd, 0), half_plane(su, 1)
    last = [group(shard2) for _ in range(4)]
    d2 = [group(W2.at[0, 0, pl.ds(0, 2)]), last[0], last[1]]
    send2(u0.at[0], dev_su, d2[0])
    send2(d0.at[0], dev_sd, d2[0])
    for g in range(2):
        send2(u0.at[1, g], dev_su, d2[1 + g])
        send2(d0.at[1, g], dev_sd, d2[1 + g])
    sib2_a = group(W2.at[0, 0])
    send2(u0, dev_sib, sib2_a)
    send2(d0, dev_sib, sib2_a)
    pair(1, True, sd, 0, su, 1)
    recv(sib2_a)
    pair(1, False, ssd, 0, ssu, 1)
    recv(c2b)
    sib2_b = group(W2.at[0, 0])
    send2(half_plane(sd, 1), dev_sib, sib2_b)
    send2(half_plane(su, 0), dev_sib, sib2_b)
    pair(2, True, sd, 1, su, 0)
    pair(0, True, s, 0, s, 1, total)
    pair(0, False, ss_, 0, ss_, 1, total)
    recv(sib2_b)
    pair(2, False, ssd, 1, ssu, 0)

    recv(d2[0])
    sib2_c = group(W2.at[0, 0, pl.ds(0, 2)])
    send2(W2.at[c, s2, 0], dev_sib, sib2_c)
    send2(W2.at[c, s2, 2], dev_sib, sib2_c)
    far_unit(12, c, s2, 0, unit)
    recv(sib2_c)
    far_unit(13, cs, ss2, 0, unit)
    pair(1, True, sd, 0, su, 1, total)
    pair(1, False, ssd, 0, ssu, 1, total)

    def last_step(t, carry):
        g, other = lax.rem(t, 2), lax.div(t, 2)
        wait(shard2, rsem.at[last[0] + t])

        @pl.when(t < 2)
        def _():
            for k in (1, 3):
                send2(W2.at[c, s2, k, g], dev_sib, last[2] + t)

        cc, s_ = c + other * (cs - c), s2 + other * (ss2 - s2)
        rhs = jnp.concatenate([W2[cc, s_, k, g] for k in (1, 3)], axis=1)
        o = jnp.dot(MIX[g], rhs, preferred_element_type=F32)
        o = jnp.where(g == 0, o, ACC[:, 0:256] + o)
        ACC[:, 0:256] = o

        @pl.when(g == 1)
        def _():
            leave(14 + other, ACC[:, 0:256])

        return carry

    lax.fori_loop(0, 4, last_step, 0)

    wait(W1, ssem.at[W1_SENT])
    wait(W2, ssem.at[W2_SENT])
    wait(TOK.at[0], ssem.at[TOK_SENT])
    for k, whole in enumerate((SCALE.at[1], SINK.at[1], ST3, ST3, ST3)):
        wait(whole, ssem.at[OTHER_SENT + k])
    for gi in range(2):
        halo_sent(gi)
        relay_sent(gi)
    wait(SENDB, osend)
    pair(2, True, sd, 1, su, 0, total)
    pair(2, False, ssd, 1, ssu, 0, total)
    for k in range(2):
        far_unit(12 + 2 * k, c, s2, k, total)
        far_unit(13 + 2 * k, cs, ss2, k, total)
    wait(OWNB, oloc)
    assert len(groups) == N_GROUPS, len(groups)


def hand_over(src, out, held, in_sem, out_sem):
    rows = 256 // PIECES
    parts = [pl.ds(k * rows, rows) for k in range(PIECES)]
    ins = [pltpu.make_async_copy(src.at[r], held.at[r], in_sem.at[k]) for k, r in enumerate(parts)]
    outs = [pltpu.make_async_copy(held.at[r], out.at[r], out_sem.at[k]) for k, r in enumerate(parts)]
    for d in ins:
        d.start()
    for d, o in zip(ins, outs):
        d.wait()
        o.start()
    for o in outs:
        o.wait()


def local_program(
    tokens, norm_gain, w_pool_in, w_query, w_key, w_value, pool_map, pool_scale,
    q_gain, k_gain, sinks, w_out,
):
    any_ = pl.BlockSpec(memory_space=pl.ANY)
    dma = pltpu.SemaphoreType.DMA
    summed = pl.pallas_call(
        kernel,
        out_shape=jax.ShapeDtypeStruct((256, 4096), BF16),
        in_specs=[any_] * 12,
        out_specs=any_,
        scratch_shapes=[
            pltpu.VMEM((2, 2, 4, 4, 128, 1152), BF16),
            pltpu.VMEM((2, 4, 4, 2, 1024, 128), BF16),
            pltpu.VMEM((2, 4, 256, 1024), BF16),
            pltpu.VMEM((128, 1152), BF16),
            pltpu.VMEM((1024, 128), BF16),
            pltpu.VMEM((256, 512), BF16),
            pltpu.VMEM((2, 512, 512), BF16),
            pltpu.VMEM((2, 1, 512), F32),
            pltpu.VMEM((2, 1, 8), F32),
            pltpu.VMEM((1, 64), F32),
            pltpu.VMEM((1, 64), F32),
            pltpu.VMEM((1, 4096), F32),
            pltpu.VMEM((128, 128), BF16),
            pltpu.VMEM((2, 2, 384, 128), BF16),
            pltpu.VMEM((2, 2, 272, 512), BF16),
            pltpu.VMEM((2, 512, 512), BF16),
            pltpu.VMEM((512, 1152), F32),
            pltpu.VMEM((2, 256, 128), F32),
            pltpu.VMEM((2, 512, 1024), BF16),
            pltpu.VMEM((2, 512, 512), F32),
            pltpu.VMEM((512, 512), BF16),
            pltpu.VMEM((32, 256, 128), BF16),
            pltpu.VMEM((32, 256, 128), BF16),
            pltpu.VMEM((32, 256, 128), BF16),
            pltpu.VMEM((2, 128, 128), BF16),
            pltpu.VMEM((2, 16, 512), BF16),
            dma((13,)),
            dma((9,)),
            dma((N_GROUPS,)),
            dma(()),
            dma((16,)),
            dma(()),
            dma((2, 2, 2)),
            dma((2, 2, 2)),
            dma((2, 2)),
            dma((2, 2)),
        ],
        compiler_params=pltpu.CompilerParams(
            collective_id=0, has_side_effects=True, vmem_limit_bytes=66_000_000
        ),
        name="mixer",
    )(
        tokens, w_pool_in, w_query, w_key.T, w_value.T, w_out, pool_map.reshape(512, 512),
        pool_scale.reshape(1, 512), sinks.reshape(1, 8), q_gain.reshape(1, 64),
        k_gain.reshape(1, 64), norm_gain.reshape(1, 4096),
    )
    return pl.pallas_call(
        hand_over,
        out_shape=jax.ShapeDtypeStruct((256, 4096), BF16),
        in_specs=[any_],
        out_specs=any_,
        scratch_shapes=[pltpu.VMEM((256, 4096), BF16), dma((PIECES,)), dma((PIECES,))],
        name="hand_over",
    )(summed)


def solution(mesh):
    in_specs = (
        P("sp", "tp"), P(), P("sp", "tp"), P("sp", "tp"), P("sp", "tp"), P("sp", "tp"),
        P("tp", None, None), P("tp"), P(), P(), P("tp"), P("tp", "sp"),
    )
    out_specs = P(("sp", "tp"), None)
    return jax.shard_map(local_program, mesh=mesh, in_specs=in_specs, out_specs=out_specs, check_vma=False)
```

```python
import jax
import jax.numpy as jnp
from jax import lax
from jax.experimental import pallas as pl
from jax.experimental.pallas import tpu as pltpu
from jax.sharding import PartitionSpec as P

MESH = pl.DeviceIdType.MESH
F32 = jnp.float32
BF16 = jnp.bfloat16
EPS = 1e-6
N_GROUPS = 45
PIECES = 8


def mod4(v):
    return lax.rem(v, 4)


def kernel(
    tokens, wp, wq, wk_t, wv_t, wo, pmap, scale_in, sinks_in, q_in, k_in, gain_in,
    out,
    W1, W2, TOK, ST1, ST2, ST3, PM, SCALE, SINK, q_gain, k_gain, gain, KVT, KV, PB, QB, ACC, SS, MIX, BIAS, BLK, SENDB, OWNB, RECVB, RLK, RLP,
    lsem, ssem, rsem, osend, orecv, oloc, hsend, hrecv, rlsend, rlrecv,
):
    sp = lax.axis_index("sp")
    x = lax.axis_index("tp")
    c = lax.rem(sp, 2)
    y = mod4(lax.div(sp, 2))
    z = lax.div(sp, 8)
    f = y + c * (z - y)
    s = z + c * (y - z)
    par = lax.rem(x, 2)
    flip1 = x + 1 - 2 * par
    flip3 = 3 - x
    p = (1 - c) * flip1 + c * flip3
    n = (1 - c) * flip3 + c * flip1
    x2 = mod4(x + 2)
    dx = mod4(x + 1 + 2 * c)

    def sp_of(c_, f_, s_):
        y_ = (1 - c_) * f_ + c_ * s_
        z_ = (1 - c_) * s_ + c_ * f_
        return (z_ * 4 + y_) * 2 + c_

    fu, fd = mod4(f + 1), mod4(f + 3)
    su, sd, s2 = mod4(s + 1), mod4(s + 3), mod4(s + 2)
    dev_fu, dev_fd = (sp_of(c, fu, s), x), (sp_of(c, fd, s), x)
    dev_su, dev_sd = (sp_of(c, f, su), x), (sp_of(c, f, sd), x)
    dev_sib = (sp + 1 - 2 * c, x)
    dev_dx, dev_p, dev_n, dev_x2 = (sp, dx), (sp, p), (sp, n), (sp, x2)
    cs, ss_, sf_ = 1 - c, f, s
    ssu, ssd, ss2 = mod4(ss_ + 1), mod4(ss_ + 3), mod4(ss_ + 2)

    groups = []
    W1_SENT, W2_SENT, TOK_SENT, TF_SENT, OTHER_SENT = range(5)

    def group(whole):
        groups.append(whole)
        return len(groups) - 1

    def send(src, dst, dev, to, sent):
        pltpu.make_async_remote_copy(
            src_ref=src, dst_ref=dst, send_sem=ssem.at[sent], recv_sem=rsem.at[to],
            device_id=dev, device_id_type=MESH,
        ).start()

    def wait(whole, sem):
        pltpu.make_async_copy(whole, whole, sem).wait()

    def recv(*gs):
        for g in gs:
            wait(groups[g], rsem.at[g])

    def holder(q, c_):
        inner = lax.rem(lax.div(q + 1, 2), 2)
        even = lax.div(q, 2) * 2 + par
        odd = inner * (2 - par) + (1 - inner) * 3 * par
        return (1 - c_) * even + c_ * odd

    quarters = (x, p)

    def halo_to(i):
        q = quarters[i]
        qn = mod4(q + 1)
        spn = sp + lax.div(q + 1, 4)
        xn = holder(qn, lax.rem(spn, 2))
        here = (spn == sp) & (xn == x)
        away = jnp.logical_not(here) & (spn < 32)
        passed = away & (c == 1) & (q == 3)
        return qn, jnp.where(spn < 32, spn, 0), xn, here, away & jnp.logical_not(passed), passed

    def halo_from(i):
        q = quarters[i]
        first = (sp == 0) & (q == 0)
        back = jnp.where(q == 0, 1, 0)
        relayed = (back == 1) & (c == 0)
        spp = jnp.where(first, sp, sp - back - jnp.where(relayed, 1, 0))
        xp = holder(mod4(q + 3), lax.rem(sp - back + 2, 2))
        here = (back == 0) & (xp == x)
        return first, jnp.logical_not(first) & jnp.logical_not(here), spp, xp

    relay = (c == 0) & ((x == 0) | (x == 3)) & (sp < 30)
    relay_dev = (jnp.where(relay, sp + 2, 0), par)
    relay_slot = jnp.where(par == 0, 0, 1)

    barrier = pltpu.get_barrier_semaphore()

    def greet(dev):
        pl.semaphore_signal(barrier, inc=1, device_id=dev, device_id_type=MESH)

    @pl.when(relay)
    def _():
        greet(relay_dev)

    for i in range(2):
        _, spn, xn, _, away, _ = halo_to(i)

        @pl.when(away)
        def _():
            greet((spn, xn))

        _, apart, spp, xp = halo_from(i)

        @pl.when(apart)
        def _():
            greet((spp, xp))

    for dev in (dev_x2, dev_su, dev_sd, dev_fu, dev_fd, dev_p, dev_n, dev_sib):
        greet(dev)

    loc = []

    def local(src, dst):
        d = pltpu.make_async_copy(src, dst, lsem.at[len(loc)])
        d.start()
        loc.append(d)
        return d

    own1 = W1.at[0, c, s, f]
    l0 = local(wp, own1.at[:, pl.ds(0, 512)])
    l1 = local(wq, own1.at[:, pl.ds(512, 512)])
    l2 = local(wk_t, KVT.at[pl.ds(0, 64)])
    l7 = local(wv_t, KVT.at[pl.ds(64, 64)])
    l3 = local(wo, W2.at[c, s, f, 0])
    l4 = local(tokens.at[pl.ds(x * 256, 256)], TOK.at[0, x])
    l5 = local(tokens.at[pl.ds(p * 256, 256)], TOK.at[1, x])
    l6 = local(pmap, PM.at[0])
    small = [
        local(src, dst)
        for src, dst in (
            (scale_in, SCALE.at[0]), (sinks_in, SINK.at[0]), (q_in, q_gain), (k_in, k_gain), (gain_in, gain),
        )
    ]

    lane_i = lax.broadcasted_iota(jnp.int32, (512, 512), 1)
    row_i = lax.broadcasted_iota(jnp.int32, (512, 512), 0)
    l2.wait()
    l7.wait()
    W1[0, c, s, f, :, pl.ds(1024, 128)] = KVT[...].astype(F32).T.astype(BF16)
    BLK[...] = jnp.where(
        lax.shift_right_logical(lane_i, 6) == lax.shift_right_logical(row_i, 6), 1.0, 0.0
    ).astype(BF16)
    SS[...] = jnp.zeros_like(SS)
    peers = 8 + jnp.where(relay, 1, 0)
    for i in range(2):
        peers += jnp.where(halo_to(i)[4], 1, 0) + jnp.where(halo_from(i)[1], 1, 0)
    pl.semaphore_wait(barrier, peers)

    l0.wait()
    l1.wait()
    l3.wait()
    shard1, shard2 = W1.at[0, 0, 0, 0], W2.at[0, 0, 0]

    def send1(piece, dev, to):
        send(piece, piece, dev, to, W1_SENT)

    def send2(piece, dev, to):
        send(piece, piece, dev, to, W2_SENT)

    def step_a1(g):
        piece = W1.at[g, c, s, f]
        to = group(shard1), group(shard1)
        for k in range(2):
            send1(piece.at[pl.ds(64 * k, 64)], dev_fu, to[k])
            send1(piece.at[pl.ds(64 - 64 * k, 64)], dev_fd, to[k])
        return to

    def step_b1(g, a):
        recv(a[0])
        to = group(shard1)
        send1(W1.at[g, c, s, fd, pl.ds(0, 64)], dev_fu, to)
        send1(W1.at[g, c, s, fu, pl.ds(64, 64)], dev_fd, to)
        return to

    def step_c1(g, a, b, shared):
        recv(a[1], b)
        plane = W1.at[g, c, s]
        to = group(W1.at[0, 0, 0]), group(W1.at[0, 0, 0])
        for k in range(2):
            send1(plane.at[pl.ds(2 * k, 2)], dev_su, to[k])
            send1(plane.at[pl.ds(2 - 2 * k, 2)], dev_sd, to[k])
        send1(plane, dev_sib, shared)
        return to

    def step_d1(g, cc):
        recv(cc[0])
        to = group(W1.at[0, 0, 0])
        send1(W1.at[g, c, sd, pl.ds(0, 2)], dev_su, to)
        send1(W1.at[g, c, su, pl.ds(2, 2)], dev_sd, to)
        return to

    def share1(g, s_, to):
        send1(W1.at[g, c, s_], dev_sib, to)

    def step_a2(g):
        to = group(shard2.at[0]), group(shard2.at[0])
        for k in range(2):
            send2(W2.at[c, s, f, g, pl.ds(512 * k, 512)], dev_fu, to[k])
            send2(W2.at[c, s, f, g, pl.ds(512 - 512 * k, 512)], dev_fd, to[k])
        return to

    def step_b2(g, a):
        recv(a[0])
        to = group(shard2.at[0])
        send2(W2.at[c, s, fd, g, pl.ds(0, 512)], dev_fu, to)
        send2(W2.at[c, s, fu, g, pl.ds(512, 512)], dev_fd, to)
        return to

    x_w1 = [group(shard1.at[pl.ds(0, 64)]) for _ in range(2)]
    for k in range(2):
        part = pl.ds(64 * k, 64)
        send(own1.at[part], ST1.at[part], dev_dx, x_w1[k], W1_SENT)
    a1 = step_a1(0)
    a2 = step_a2(0)
    key_i = jnp.bitwise_and(lane_i, 255)
    dist = 128 + jnp.bitwise_and(row_i, 127) - key_i
    band = (dist >= 0) & (dist < 128)
    head_in = 2 * lax.shift_right_logical(row_i, 7) + lax.shift_right_logical(lane_i, 8) + 1
    for gi, g in ((0, x), (1, x2)):
        slope = jnp.exp2(-0.25 * (g * 8 + head_in).astype(F32))
        BIAS[gi] = jnp.where(band, -slope * dist.astype(F32), -1e30)

    f_w1 = group(shard1)
    for k in range(2):
        recv(x_w1[k])
        part = pl.ds(64 * k, 64)
        send(ST1.at[part], W1.at[1, c, s, f, part], dev_dx, f_w1, W1_SENT)
        if k == 0:
            b1 = step_b1(0, a1)
    two_slabs = TOK.at[0, pl.ds(0, 2)]
    tn = group(two_slabs)
    send(tokens.at[pl.ds(n * 256, 256)], TOK.at[0, x], dev_n, tn, TOK_SENT)
    send(tokens.at[pl.ds(x2 * 256, 256)], TOK.at[1, x], dev_n, tn, TOK_SENT)
    sc_c, sk_c = group(SCALE.at[1]), group(SINK.at[1])
    send(scale_in, SCALE.at[1], dev_x2, sc_c, OTHER_SENT)
    send(sinks_in, SINK.at[1], dev_x2, sk_c, OTHER_SENT + 1)

    b2 = step_b2(0, a2)
    sib1 = group(W1.at[0, 0])
    c1a, c1b = step_c1(0, a1, b1, sib1)
    recv(f_w1)
    a1o = step_a1(1)

    def scale_slab(j):
        g = gain[:, pl.ds(pl.multiple_of(j * 1024, 1024), 1024)]

        def body(k, carry):
            slot, r = lax.div(k, 4), pl.ds(lax.rem(k, 4) * 64, 64)
            t = TOK[slot, j, r, :].astype(F32)
            sq = t * t
            tot = sq[:, 0:128]
            for m in range(1, 8):
                tot += sq[:, m * 128 : (m + 1) * 128]
            SS[slot, r, :] += tot
            TOK[slot, j, r, :] = (t * g).astype(BF16)
            return carry

        lax.fori_loop(0, 8, body, 0)

    for d in (l4, l5, *small):
        d.wait()
    scale_slab(x)
    b1o = step_b1(1, a1o)
    tp_ = group(two_slabs)
    send(tokens.at[pl.ds(p * 256, 256)], TOK.at[0, x], dev_p, tp_, TOK_SENT)
    send(tokens.at[pl.ds(x * 256, 256)], TOK.at[1, x], dev_p, tp_, TOK_SENT)
    recv(tn)
    tf = group(two_slabs)
    send(TOK.at[0, n], TOK.at[1, n], dev_p, tf, TF_SENT)
    send(TOK.at[1, n], TOK.at[0, n], dev_p, tf, TF_SENT)
    d1 = step_d1(0, (c1a, c1b))
    sib1o = group(W1.at[0, 0, pl.ds(0, 3)])
    c1o = step_c1(1, a1o, b1o, sib1o)
    recv(c1b)
    share1(0, sd, sib1)
    share1(0, su, sib1)

    def half_plane(s_, k):
        return W2.at[c, s_, pl.ds(2 * k, 2)]

    def c2_send(g):
        to = c2a, c2b
        for k in range(2):
            send2(W2.at[c, s, pl.ds(2 * k, 2), g], dev_su, to[k])
            send2(W2.at[c, s, pl.ds(2 - 2 * k, 2), g], dev_sd, to[k])

    def matmul(lhs, rhs, first):
        o = jnp.dot(lhs, rhs, preferred_element_type=F32)
        if first:
            ACC[...] = o
        else:
            ACC[...] += o

    def matmul_slab(gi, jz, first=False):
        def body(t, carry):
            parts = []
            for yy in range(4):
                parts.append(W1[gi, 0, jz, yy])
                parts.append(W1[gi, 1, yy, jz])
            matmul(TOK[:, jz].reshape(512, 1024), jnp.concatenate(parts, axis=0), first)
            return carry

        lax.fori_loop(0, 1, body, 0)

    def matmul_planes(gi, cc, planes, first=False):
        def body(t, carry):
            lhs, rhs = [], []
            for s_ in planes:
                for k in range(4):
                    rhs.append(W1[gi, cc, s_, k])
                    off = ((1 - cc) * k + cc * s_) * 256 + cc * 128
                    col = pl.ds(pl.multiple_of(off, 128), 128)
                    lhs.append(TOK[:, (1 - cc) * s_ + cc * k, :, col].reshape(512, 128))
            matmul(jnp.concatenate(lhs, axis=1), jnp.concatenate(rhs, axis=0), first)
            return carry

        lax.fori_loop(0, 1, body, 0)

    def post(gi):
        def body(k, carry):
            slot, r = lax.div(k, 2), lax.rem(k, 2)
            rows = pl.ds(pl.multiple_of(k * 128, 128), 128)
            tot = jnp.sum(SS[slot, pl.ds(r * 128, 128), :], axis=-1, keepdims=True)
            a = ACC[rows, :] * lax.rsqrt(tot * (1.0 / 4096) + EPS)
            PB[gi, slot, pl.ds(pl.multiple_of(16 + r * 128, 16), 128), :] = a[:, 0:512].astype(BF16)
            qf = a[:, 512:1024].astype(BF16).astype(F32)
            sq = qf * qf
            hi = sq.astype(BF16)
            lo = (sq - hi.astype(F32)).astype(BF16)
            ssq = jnp.dot(hi, BLK[...], preferred_element_type=F32) + jnp.dot(
                lo, BLK[...], preferred_element_type=F32
            )
            qg = jnp.concatenate([q_gain[...]] * 8, axis=1) * 0.125
            QB[gi, rows, :] = (qf * lax.rsqrt(ssq * (1.0 / 64) + EPS) * qg).astype(BF16)
            kv = a[:, 1024:1152].astype(BF16).astype(F32)
            is_key = lax.broadcasted_iota(jnp.int32, (128, 128), 1) < 64
            ksq = jnp.sum(jnp.where(is_key, kv * kv, 0.0), axis=-1, keepdims=True)
            kn = kv * lax.rsqrt(ksq * (1.0 / 64) + EPS) * jnp.concatenate([k_gain[...]] * 2, axis=1)
            KV[gi, slot, pl.ds(pl.multiple_of(128 + r * 128, 128), 128), :] = jnp.where(
                is_key, kn, kv
            ).astype(BF16)
            return carry

        lax.fori_loop(0, 4, body, 0)

    def halo_next(gi, i):
        qn, spn, xn, here, away, passed = halo_to(i)
        slot = jnp.where(xn == qn, 0, 1)
        gn = jnp.where(xn == x, gi, 1 - gi)
        tails = (KV.at[gi, i, pl.ds(256, 128)], PB.at[gi, i, pl.ds(256, 16)])
        copies = [
            pltpu.make_async_remote_copy(
                src_ref=src, dst_ref=dst, send_sem=hsend.at[gi, i, k], recv_sem=hrecv.at[gn, slot, k],
                device_id=(spn, xn), device_id_type=MESH,
            )
            for k, (src, dst) in enumerate(
                zip(tails, (KV.at[gn, slot, pl.ds(0, 128)], PB.at[gn, slot, pl.ds(0, 16)]))
            )
        ]
        passes = [
            pltpu.make_async_remote_copy(
                src_ref=src, dst_ref=dst, send_sem=hsend.at[gi, i, k], recv_sem=rlrecv.at[gi, k],
                device_id=dev_sib, device_id_type=MESH,
            )
            for k, (src, dst) in enumerate(zip(tails, (RLK.at[gi], RLP.at[gi])))
        ]
        return here, away, copies, passed, passes

    def halo_send(gi):
        for i in range(2):
            here, away, copies, passed, passes = halo_next(gi, i)

            @pl.when(passed)
            def _():
                for d in passes:
                    d.start()

            @pl.when(away)
            def _():
                for d in copies:
                    d.start()

            @pl.when(here)
            def _():
                KV[gi, 1 - i, pl.ds(0, 128), :] = KV[gi, i, pl.ds(256, 128), :]
                PB[gi, 1 - i, pl.ds(0, 16), :] = PB[gi, i, pl.ds(256, 16), :]

    def halo_sent(gi):
        for i in range(2):
            _, away, copies, passed, passes = halo_next(gi, i)

            @pl.when(passed)
            def _():
                for d in passes:
                    d.wait_send()

            @pl.when(away)
            def _():
                for d in copies:
                    d.wait_send()

    def relay_copies(gi):
        gn = jnp.where(par == x, gi, 1 - gi)
        return [
            pltpu.make_async_remote_copy(
                src_ref=src, dst_ref=dst, send_sem=rlsend.at[gi, k],
                recv_sem=hrecv.at[gn, relay_slot, k], device_id=relay_dev, device_id_type=MESH,
            )
            for k, (src, dst) in enumerate(
                (
                    (RLK.at[gi], KV.at[gn, relay_slot, pl.ds(0, 128)]),
                    (RLP.at[gi], PB.at[gn, relay_slot, pl.ds(0, 16)]),
                )
            )
        ]

    def halo_relay(gi):
        @pl.when(relay)
        def _():
            for k, dst in enumerate((RLK.at[gi], RLP.at[gi])):
                pltpu.make_async_copy(dst, dst, rlrecv.at[gi, k]).wait()
            for d in relay_copies(gi):
                d.start()

    def relay_sent(gi):
        @pl.when(relay)
        def _():
            for d in relay_copies(gi):
                d.wait_send()

    def halo_wait(gi):
        for i in range(2):
            first, apart, _, _ = halo_from(i)

            @pl.when(first)
            def _():
                KV[gi, i, pl.ds(0, 128), :] = jnp.zeros((128, 128), BF16)
                PB[gi, i, pl.ds(0, 16), :] = jnp.zeros((16, 512), BF16)

            @pl.when(apart)
            def _():
                for k, dst in enumerate((KV.at[gi, i, pl.ds(0, 128)], PB.at[gi, i, pl.ds(0, 16)])):
                    pltpu.make_async_copy(dst, dst, hrecv.at[gi, i, k]).wait()

    def pool(gi, g):
        span = lax.shift_left(jnp.int32(2), g)
        for i in range(2):
            pf = PB[gi, i].astype(F32)
            t2 = pf + pltpu.roll(pf, 1, 0)
            t4 = t2 + pltpu.roll(t2, 2, 0)
            t8 = t4 + pltpu.roll(t4, 4, 0)
            t16 = t8 + pltpu.roll(t8, 8, 0)
            run = jnp.where(g == 0, t2, jnp.where(g == 1, t4, jnp.where(g == 2, t8, t16)))[16:]
            pos = sp * 1024 + quarters[i] * 256 + lax.broadcasted_iota(jnp.int32, (256, 1), 0)
            count = jnp.minimum(pos + 1, span).astype(F32)
            diff = (run * (1.0 / count) - pf[16:]).astype(BF16)
            m = jnp.dot(diff, PM[gi], preferred_element_type=F32)
            m = m * SCALE[gi]
            m = m * lax.rsqrt(jnp.mean(m * m, axis=-1, keepdims=True) + EPS)
            MIX[gi, i * 256 : (i + 1) * 256, 0:512] = m.astype(BF16)

    def attend(gi, r):
        sink = jnp.exp(SINK[gi])
        left = lax.broadcasted_iota(jnp.int32, (1, 128), 1) < 64
        es = jnp.concatenate(
            [
                jnp.broadcast_to(
                    jnp.where(left, sink[:, 2 * j : 2 * j + 1], sink[:, 2 * j + 1 : 2 * j + 2]),
                    (128, 128),
                )
                for j in range(4)
            ],
            axis=0,
        )

        def body(k, carry):
            slot = k
            rows = pl.ds(pl.multiple_of(k * 256 + r * 128, 128), 128)
            kv = KV[gi, slot, pl.ds(r * 128, 256), :].astype(F32)
            low = lax.broadcasted_iota(jnp.int32, (256, 128), 1) < 64
            ke = jnp.where(low, kv, 0.0)
            vo = jnp.where(low, 0.0, kv)
            ko = pltpu.roll(ke, 64, 1)
            ve = pltpu.roll(vo, 64, 1)
            q_here = (1 - slot) * x + slot * p
            missing = jnp.where((sp == 0) & (q_here == 0), 128, 0) if r == 0 else 0
            there = lax.broadcasted_iota(jnp.int32, (256, 128), 0) >= missing
            oe = jnp.where(low & there, 1.0, 0.0)
            oo = jnp.where(jnp.logical_not(low) & there, 1.0, 0.0)
            keys = jnp.concatenate([ke, ko], axis=0).astype(BF16)
            values = jnp.concatenate(
                [jnp.concatenate([ve, oe], axis=1), jnp.concatenate([vo, oo], axis=1)], axis=0
            ).astype(BF16)
            q = QB[gi, rows, :]
            q = jnp.concatenate([q[:, j * 128 : (j + 1) * 128] for j in range(4)], axis=0)
            sc = lax.dot_general(q, keys, (((1,), (1,)), ((), ())), preferred_element_type=F32)
            e = jnp.exp(sc + BIAS[gi]).astype(BF16)
            o = jnp.dot(e, values, preferred_element_type=F32)
            att = o[:, 0:128] / (o[:, 128:256] + es)
            parts = [att[j * 128 : (j + 1) * 128] for j in range(4)]
            sq = parts[0] * parts[0]
            for j in range(1, 4):
                sq += parts[j] * parts[j]
            r_ = lax.rsqrt(jnp.sum(sq, axis=-1, keepdims=True) * (1.0 / 512) + EPS)
            for j in range(4):
                MIX[gi, rows, 512 + j * 128 : 640 + j * 128] = (parts[j] * r_).astype(BF16)
            return carry

        lax.fori_loop(0, 2, body, 0)

    recv(d1)
    share1(0, s2, sib1)
    recv(sib1)
    matmul_slab(0, x, True)
    recv(tp_)
    scale_slab(p)
    x_w2 = group(shard2.at[0])
    send(W2.at[c, s, f, 0], ST2, dev_dx, x_w2, W2_SENT)
    matmul_slab(0, p)
    d1o = step_d1(1, c1o)
    c2a, c2b = group(W2.at[0, 0]), group(W2.at[0, 0])
    recv(a2[1], b2)
    c2_send(0)
    l6.wait()
    half = pl.ds(c * 256, 256)
    x_pm = group(ST3)
    send(PM.at[0, half], ST3, dev_dx, x_pm, OTHER_SENT + 2)
    wait(two_slabs, ssem.at[TF_SENT])
    scale_slab(n)
    matmul_slab(0, n)
    recv(tf)
    scale_slab(x2)
    matmul_slab(0, x2)
    recv(x_w2)
    f_w2 = group(shard2.at[0])
    send(ST2, W2.at[c, s, f, 1], dev_dx, f_w2, W2_SENT)
    post(0)
    halo_send(0)
    recv(c1o[1])
    share1(1, sd, sib1o)
    share1(1, su, sib1o)
    matmul_planes(1, c, (s, sd, su), True)
    recv(sib1o)
    recv(f_w2)
    a2o = step_a2(1)
    recv(x_pm)
    f_pm = group(ST3)
    send(ST3, PM.at[1, half], dev_dx, f_pm, OTHER_SENT + 3)
    matmul_planes(1, cs, (ss_, ssd, ssu))
    halo_relay(0)
    attend(0, 1)
    recv(d1o)
    sib1o_far = group(W1.at[0, 0, 0])
    share1(1, s2, sib1o_far)
    matmul_planes(1, c, (s2,))
    b2o = step_b2(1, a2o)
    recv(sib1o_far)
    matmul_planes(1, cs, (ss2,))
    post(1)
    halo_send(1)

    recv(sc_c, sk_c)
    attend(1, 1)
    halo_relay(1)
    recv(f_pm)
    sib_pm = group(ST3)
    send(PM.at[1, half], PM.at[1, half], dev_sib, sib_pm, OTHER_SENT + 4)
    recv(a2o[1], b2o)
    c2_send(1)
    sib2_own = group(W2.at[0, 0])
    send2(W2.at[c, s], dev_sib, sib2_own)
    halo_wait(0)
    attend(0, 0)
    pool(0, x)
    halo_wait(1)
    attend(1, 0)
    recv(sib_pm)
    pool(1, x2)

    def product(cc, s_, fs, g):
        rhs = jnp.concatenate([W2[cc, s_, fs[0], g], W2[cc, s_, fs[1], g]], axis=1)
        return jnp.dot(MIX[g], rhs, preferred_element_type=F32)

    def unit(u, cc, s_, fs):
        leave(u, product(cc, s_, fs, 0) + product(cc, s_, fs, 1))

    def leave(u, o):
        ob = o.astype(BF16)
        for e in range(2):
            idx = 2 * u + e
            OWNB[idx] = ob[0:256, e * 128 : (e + 1) * 128]
            SENDB[idx] = ob[256:512, e * 128 : (e + 1) * 128]
            pltpu.make_async_remote_copy(
                src_ref=SENDB.at[idx], dst_ref=RECVB.at[idx], send_sem=osend, recv_sem=orecv.at[u],
                device_id=dev_p, device_id_type=MESH,
            ).start()

    def total(u, cc, s_, fs):
        wait(RECVB.at[pl.ds(2 * u, 2)], orecv.at[u])
        for e in range(2):
            idx = 2 * u + e
            col = pl.ds(pl.multiple_of(sp_of(cc, fs[e], s_) * 128, 128), 128)
            OWNB[idx] = (OWNB[idx].astype(F32) + RECVB[idx].astype(F32)).astype(BF16)
            pltpu.make_async_copy(OWNB.at[idx], out.at[:, col], oloc).start()

    def pair(stage, mine, sA, kA, sB, kB, act=unit):
        cc = c if mine else cs

        def body(t, carry):
            k = kA + t * (kB - kA)
            act(stage * 4 + (0 if mine else 2) + t, cc, sA + t * (sB - sA), (2 * k, 2 * k + 1))
            return carry

        lax.fori_loop(0, 2, body, 0)

    def far_unit(u, cc, s_, k, act):
        def body(t, carry):
            act(u, cc, s_, (t, 2 + t))
            return carry

        lax.fori_loop(k, k + 1, body, 0)

    pair(0, True, s, 0, s, 1)
    recv(sib2_own)
    pair(0, False, ss_, 0, ss_, 1)
    recv(c2a)
    u0, d0 = half_plane(sd, 0), half_plane(su, 1)
    last = [group(shard2) for _ in range(4)]
    d2 = [group(W2.at[0, 0, pl.ds(0, 2)]), last[0], last[1]]
    send2(u0.at[0], dev_su, d2[0])
    send2(d0.at[0], dev_sd, d2[0])
    for g in range(2):
        send2(u0.at[1, g], dev_su, d2[1 + g])
        send2(d0.at[1, g], dev_sd, d2[1 + g])
    sib2_a = group(W2.at[0, 0])
    send2(u0, dev_sib, sib2_a)
    send2(d0, dev_sib, sib2_a)
    pair(1, True, sd, 0, su, 1)
    recv(sib2_a)
    pair(1, False, ssd, 0, ssu, 1)
    recv(c2b)
    sib2_b = group(W2.at[0, 0])
    send2(half_plane(sd, 1), dev_sib, sib2_b)
    send2(half_plane(su, 0), dev_sib, sib2_b)
    pair(2, True, sd, 1, su, 0)
    pair(0, True, s, 0, s, 1, total)
    pair(0, False, ss_, 0, ss_, 1, total)
    recv(sib2_b)
    pair(2, False, ssd, 1, ssu, 0)

    recv(d2[0])
    sib2_c = group(W2.at[0, 0, pl.ds(0, 2)])
    send2(W2.at[c, s2, 0], dev_sib, sib2_c)
    send2(W2.at[c, s2, 2], dev_sib, sib2_c)
    far_unit(12, c, s2, 0, unit)
    recv(sib2_c)
    far_unit(13, cs, ss2, 0, unit)

    def last_step(t, carry):
        g, other = lax.rem(t, 2), lax.div(t, 2)
        wait(shard2, rsem.at[last[0] + t])

        @pl.when(t < 2)
        def _():
            for k in (1, 3):
                send2(W2.at[c, s2, k, g], dev_sib, last[2] + t)

        cc, s_ = c + other * (cs - c), s2 + other * (ss2 - s2)
        rhs = jnp.concatenate([W2[cc, s_, k, g] for k in (1, 3)], axis=1)
        o = jnp.dot(MIX[g], rhs, preferred_element_type=F32)
        o = jnp.where(g == 0, o, ACC[:, 0:256] + o)
        ACC[:, 0:256] = o

        @pl.when(g == 1)
        def _():
            leave(14 + other, ACC[:, 0:256])

        return carry

    lax.fori_loop(0, 4, last_step, 0)
    pair(1, True, sd, 0, su, 1, total)
    pair(1, False, ssd, 0, ssu, 1, total)

    wait(W1, ssem.at[W1_SENT])
    wait(W2, ssem.at[W2_SENT])
    wait(TOK.at[0], ssem.at[TOK_SENT])
    for k, whole in enumerate((SCALE.at[1], SINK.at[1], ST3, ST3, ST3)):
        wait(whole, ssem.at[OTHER_SENT + k])
    for gi in range(2):
        halo_sent(gi)
        relay_sent(gi)
    wait(SENDB, osend)
    pair(2, True, sd, 1, su, 0, total)
    pair(2, False, ssd, 1, ssu, 0, total)
    for k in range(2):
        far_unit(12 + 2 * k, c, s2, k, total)
        far_unit(13 + 2 * k, cs, ss2, k, total)
    wait(OWNB, oloc)
    assert len(groups) == N_GROUPS, len(groups)


def hand_over(src, out, held, in_sem, out_sem):
    rows = 256 // PIECES
    parts = [pl.ds(k * rows, rows) for k in range(PIECES)]
    ins = [pltpu.make_async_copy(src.at[r], held.at[r], in_sem.at[k]) for k, r in enumerate(parts)]
    outs = [pltpu.make_async_copy(held.at[r], out.at[r], out_sem.at[k]) for k, r in enumerate(parts)]
    for d in ins:
        d.start()
    for d, o in zip(ins, outs):
        d.wait()
        o.start()
    for o in outs:
        o.wait()


def local_program(
    tokens, norm_gain, w_pool_in, w_query, w_key, w_value, pool_map, pool_scale,
    q_gain, k_gain, sinks, w_out,
):
    any_ = pl.BlockSpec(memory_space=pl.ANY)
    dma = pltpu.SemaphoreType.DMA
    summed = pl.pallas_call(
        kernel,
        out_shape=jax.ShapeDtypeStruct((256, 4096), BF16),
        in_specs=[any_] * 12,
        out_specs=any_,
        scratch_shapes=[
            pltpu.VMEM((2, 2, 4, 4, 128, 1152), BF16),
            pltpu.VMEM((2, 4, 4, 2, 1024, 128), BF16),
            pltpu.VMEM((2, 4, 256, 1024), BF16),
            pltpu.VMEM((128, 1152), BF16),
            pltpu.VMEM((1024, 128), BF16),
            pltpu.VMEM((256, 512), BF16),
            pltpu.VMEM((2, 512, 512), BF16),
            pltpu.VMEM((2, 1, 512), F32),
            pltpu.VMEM((2, 1, 8), F32),
            pltpu.VMEM((1, 64), F32),
            pltpu.VMEM((1, 64), F32),
            pltpu.VMEM((1, 4096), F32),
            pltpu.VMEM((128, 128), BF16),
            pltpu.VMEM((2, 2, 384, 128), BF16),
            pltpu.VMEM((2, 2, 272, 512), BF16),
            pltpu.VMEM((2, 512, 512), BF16),
            pltpu.VMEM((512, 1152), F32),
            pltpu.VMEM((2, 256, 128), F32),
            pltpu.VMEM((2, 512, 1024), BF16),
            pltpu.VMEM((2, 512, 512), F32),
            pltpu.VMEM((512, 512), BF16),
            pltpu.VMEM((32, 256, 128), BF16),
            pltpu.VMEM((32, 256, 128), BF16),
            pltpu.VMEM((32, 256, 128), BF16),
            pltpu.VMEM((2, 128, 128), BF16),
            pltpu.VMEM((2, 16, 512), BF16),
            dma((13,)),
            dma((9,)),
            dma((N_GROUPS,)),
            dma(()),
            dma((16,)),
            dma(()),
            dma((2, 2, 2)),
            dma((2, 2, 2)),
            dma((2, 2)),
            dma((2, 2)),
        ],
        compiler_params=pltpu.CompilerParams(
            collective_id=0, has_side_effects=True, vmem_limit_bytes=66_000_000
        ),
        name="mixer",
    )(
        tokens, w_pool_in, w_query, w_key.T, w_value.T, w_out, pool_map.reshape(512, 512),
        pool_scale.reshape(1, 512), sinks.reshape(1, 8), q_gain.reshape(1, 64),
        k_gain.reshape(1, 64), norm_gain.reshape(1, 4096),
    )
    return pl.pallas_call(
        hand_over,
        out_shape=jax.ShapeDtypeStruct((256, 4096), BF16),
        in_specs=[any_],
        out_specs=any_,
        scratch_shapes=[pltpu.VMEM((256, 4096), BF16), dma((PIECES,)), dma((PIECES,))],
        name="hand_over",
    )(summed)


def solution(mesh):
    in_specs = (
        P("sp", "tp"), P(), P("sp", "tp"), P("sp", "tp"), P("sp", "tp"), P("sp", "tp"),
        P("tp", None, None), P("tp"), P(), P(), P("tp"), P("tp", "sp"),
    )
    out_specs = P(("sp", "tp"), None)
    return jax.shard_map(local_program, mesh=mesh, in_specs=in_specs, out_specs=out_specs, check_vma=False)
```
